512 devices in a mesh: sp: 64 (over z, y), tp: 8 (over x, core).
Axes of the slice: x: 4, y: 8, z: 8, core: 2. Of those that a mesh axis runs over, the one named last changes fastest.
Arguments:
- hidden_in: bfloat16 [32768, 2048], P('sp'), may hold values from -64 to 64
- pre_gain: float32 [2048], replicated, may hold values from 0.1 to 1.9
- query_proj: bfloat16 [2048, 2048], P(None, 'tp'), may hold values from -2 to 2
- key_proj: bfloat16 [2048, 2048], P('sp', 'tp'), may hold values from -2 to 2
- value_proj: bfloat16 [2048, 2048], P('sp', 'tp'), may hold values from -0.125 to 0.125
- out_proj: bfloat16 [2048, 2048], P('tp'), may hold values from -0.125 to 0.125
- post_gain: float32 [2048], replicated, may hold values from 0.1 to 1.9
Outputs:
- layer_out: bfloat16 [32768, 2048], P(('sp', 'tp'))
- log_weight: float32 [32, 32768], P('tp', 'sp')
The draws below stay inside these ranges and needn't reach their ends.
All inputs are finite; a program needn't handle non-finite values.
Results may differ from the reference program's by a relative error of at most 0.018.
The reference program's roundings to bfloat16 on the way count: a program that leaves them out, or rounds other values in their place, can miss the bound.
Values may be sent and summed in bfloat16 or wider, within the bound.
A program may use at most 64 MiB of HBM per device.

```python
import jax
import jax.numpy as jnp
from jax import lax

D = 2048
HEADS = 32
HEAD_DIM = 64
SPAN = 128
TOKENS = 32768
N_TP = 8


def draw_hidden_in(key, part):
    noise_part = jax.random.normal(jax.random.fold_in(key, 3), (TOKENS, D), jnp.float32)
    return jnp.clip(noise_part, -64.0, 64.0).astype(jnp.bfloat16)


def shared_pair(key):
    fan_scale = D ** (-0.5)
    query_part = jax.random.normal(jax.random.fold_in(key, 22), (D, HEADS * HEAD_DIM), jnp.float32) * fan_scale
    key_part = jax.random.normal(jax.random.fold_in(key, 23), (D, HEADS * HEAD_DIM), jnp.float32) * fan_scale
    return (jnp.clip(query_part, -2.0, 2.0), jnp.clip(key_part, -2.0, 2.0))


def draw_query_proj(key, part):
    return shared_pair(key)[0].astype(jnp.bfloat16)


def draw_key_proj(key, part):
    return shared_pair(key)[1].astype(jnp.bfloat16)


def steps_of(key, dims, split, least, high):
    factor_of = 1.0
    for dim, parts in split:
        steps = jax.random.uniform(jax.random.fold_in(jax.random.fold_in(key, 6), dim), (parts,), jnp.float32, least / len(split), high / len(split))
        factor_of = factor_of * jnp.repeat(jnp.exp(steps), dims[dim] // parts).reshape((-1,) + (1,) * (len(dims) - 1 - dim))
    return factor_of


def noise(key, shape, deviation, most, shards=(), held_as=jnp.bfloat16):
    values = jax.random.normal(key, shape, jnp.float32) * deviation
    if len(shards) > 0:
        values = steps_of(key, shape, shards, -0.22, 0.18) * values
    return jnp.clip(values, min=-most, max=most).astype(held_as)


def setup_inputs(seed: int = 0) -> dict:
    splits = jax.random.split(jax.random.key(seed), 8)
    return {
        "hidden_in": draw_hidden_in(jax.random.fold_in(splits[7], 71), 0),
        "pre_gain": jnp.clip(1.0 + 0.18 * jax.random.normal(splits[1], (D,), jnp.float32), 0.1, 1.9),
        "query_proj": draw_query_proj(jax.random.fold_in(splits[7], 71), 0),
        "key_proj": draw_key_proj(jax.random.fold_in(splits[7], 71), 0),
        "value_proj": noise(splits[4], (D, HEADS * HEAD_DIM), D ** -0.5, 0.125, ((0, 64), (1, 8))),
        "out_proj": noise(splits[5], (HEADS * HEAD_DIM, D), (HEADS * HEAD_DIM) ** -0.5, 0.125, ((0, 8),)),
        "post_gain": jnp.clip(1.0 + 0.18 * jax.random.normal(splits[6], (D,), jnp.float32), 0.1, 1.9),
    }


EPS = 1e-06
ROPE_BASE = 10000.0
DILATIONS = (1, 4, 16)

def rotate(vectors, positions):
    half_dim = vectors.shape[-1] // 2
    frequency = ROPE_BASE ** (-(jnp.arange(half_dim, dtype=jnp.float32) * 2.0 / vectors.shape[-1]))
    angles = positions[:, None] * frequency[None, :]
    cos_part = jnp.cos(angles)[:, None, :]
    sin_part = jnp.sin(angles)[:, None, :]
    front_half = vectors[..., :half_dim]
    back_half = vectors[..., half_dim:]
    return jnp.concatenate([front_half * cos_part - back_half * sin_part, back_half * cos_part + front_half * sin_part], axis=-1)

def rms_scale(matrix, gain):
    return matrix * lax.rsqrt(lax.optimization_barrier(jnp.mean(matrix * matrix, axis=-1, keepdims=True)) + EPS) * gain

def residue_attention(queries, key_rows, values, dilation):
    seq_len, head_count, head_depth = queries.shape
    blocks = seq_len // (dilation * SPAN)
    block_shape = (blocks, SPAN, dilation, head_count, head_depth)
    query_blocks = queries.reshape(block_shape).astype(jnp.float32)
    key_blocks = key_rows.reshape(block_shape).astype(jnp.float32)
    value_blocks = values.reshape(block_shape).astype(jnp.float32)
    zero_block = jnp.zeros((1,) + block_shape[1:], jnp.float32)
    key_pairs = jnp.concatenate([jnp.concatenate([zero_block, key_blocks[:-1]], axis=0), key_blocks], axis=1)
    value_pairs = jnp.concatenate([jnp.concatenate([zero_block, value_blocks[:-1]], axis=0), value_blocks], axis=1)
    scores = jnp.einsum('bqrhe,bkrhe->brhqk', query_blocks, key_pairs) * head_depth ** (-0.5)
    query_idx = jnp.arange(SPAN, dtype=jnp.int32)[:, None]
    key_idx = jnp.arange(2 * SPAN, dtype=jnp.int32)[None, :]
    distance = query_idx + SPAN - key_idx
    in_band = (distance >= 0) & (distance <= SPAN)
    key_pos = (jnp.arange(blocks, dtype=jnp.int32)[:, None, None, None, None] * SPAN + jnp.arange(2 * SPAN, dtype=jnp.int32)[None, None, None, None, :] - SPAN) * dilation + jnp.arange(dilation, dtype=jnp.int32)[None, :, None, None, None]
    valid = in_band[None, None, None] & (key_pos >= 0)
    scores = jnp.where(valid, scores, -jnp.inf)
    row_max = lax.optimization_barrier(jnp.max(scores, axis=-1, keepdims=True))
    exp_scores = jnp.exp(scores - row_max)
    denominator = lax.optimization_barrier(jnp.sum(exp_scores, axis=-1, keepdims=True))
    levels = (row_max + jnp.log(denominator))[..., 0]
    shares = lax.optimization_barrier((exp_scores / denominator).astype(jnp.bfloat16))
    outcome = jnp.einsum('brhqk,bkrhe->bqrhe', shares.astype(jnp.float32), value_pairs)
    outcome = outcome.reshape(seq_len, head_count, head_depth)
    levels = levels.transpose(2, 0, 3, 1).reshape(head_count, seq_len)
    return (outcome, levels)

def blend(group_outs, group_levels):
    levels = jnp.stack(group_levels)
    row_max = lax.optimization_barrier(jnp.max(levels, axis=0))
    log_weight = row_max + jnp.log(lax.optimization_barrier(jnp.sum(jnp.exp(levels - row_max[None]), axis=0)))
    shares = jnp.exp(levels - log_weight[None])
    blended = lax.optimization_barrier(jnp.sum(shares.transpose(0, 2, 1)[..., None] * jnp.stack(group_outs), axis=0))
    return (blended, log_weight)

def reference(hidden_in, pre_gain, query_proj, key_proj, value_proj, out_proj, post_gain):
    normed = rms_scale(hidden_in.astype(jnp.float32), pre_gain).astype(jnp.bfloat16)
    positions = jnp.arange(TOKENS, dtype=jnp.int32).astype(jnp.float32)
    group_width = HEADS // N_TP * HEAD_DIM

    def split_cols(matrix):
        return matrix.reshape(D, N_TP, group_width).transpose(1, 0, 2)

    def one_group(summed, weights):
        w_query, w_key, w_value, w_out = weights
        queries = rotate(jnp.dot(normed, w_query, preferred_element_type=jnp.float32).reshape(TOKENS, -1, HEAD_DIM), positions).astype(jnp.bfloat16)
        key_rows = rotate(jnp.dot(normed, w_key, preferred_element_type=jnp.float32).reshape(TOKENS, -1, HEAD_DIM), positions).astype(jnp.bfloat16)
        values = jnp.dot(normed, w_value, preferred_element_type=jnp.float32).astype(jnp.bfloat16).reshape(TOKENS, -1, HEAD_DIM)
        group_outs = []
        group_levels = []
        for dilation in DILATIONS:
            outcome, levels = residue_attention(queries, key_rows, values, dilation)
            group_outs.append(outcome)
            group_levels.append(levels)
        blended, log_weight = blend(group_outs, group_levels)
        attended = blended.astype(jnp.bfloat16).reshape(TOKENS, group_width)
        partial_value = lax.optimization_barrier(jnp.dot(attended, w_out, preferred_element_type=jnp.float32).astype(jnp.bfloat16))
        return (summed + partial_value.astype(jnp.float32), log_weight)
    summed, log_weight = lax.scan(one_group, jnp.zeros((TOKENS, D), jnp.float32), (split_cols(query_proj), split_cols(key_proj), split_cols(value_proj), out_proj.reshape(N_TP, group_width, D)))
    layer_out = rms_scale(summed, post_gain).astype(jnp.bfloat16)
    return (layer_out, log_weight.reshape(HEADS, TOKENS))
```

```python
import functools
import math

import jax
import jax.numpy as jnp
import numpy as np
from jax import lax
from jax.experimental import pallas as pl
from jax.experimental.pallas import tpu as pltpu
from jax.sharding import PartitionSpec as P

HEAD_DIM = 64
SPAN = 128
EPS = 1e-06
ROPE_BASE = 10000.0
NY = 8
NZ = 8
NSP = NY * NZ
NTP = 8
NX = 4
ROWS = 512
D = 2048
WIDTH = 256
OUT_ROWS = 64
SLOTS = 5
NEG = -1e30
SCALE2 = math.log2(math.e) / 8.0
LN2 = math.log(2.0)
F32 = jnp.float32
BF16 = jnp.bfloat16
MESH = pl.DeviceIdType.MESH

NT = (((1,), (1,)), ((), ()))
NN = (((1,), (0,)), ((), ()))

R_WY = 0
R_WZ = R_WY + 2 * (NY - 1)
R_X = R_WZ + 2 * 2 * 2 * 4
R_H = R_X + 16
R_A = R_H + 2 * SLOTS
R_END = R_A + 2 * (NTP - 1)
N_SEND = 110


def dot(a, b, dims=NN):
    return lax.dot_general(a, b, dims, preferred_element_type=F32)


def token_of(row):
    return (row // 128) + ((row // 8) % 4) * 4 + (row % 8) * 16 + ((row // 32) % 4) * 128


def kernel(
    hid, gain, freq, wq, wk, wv, wo, post,
    out, lw_out,
    hid_v, np_v, wq_v, w_v, wo_v, kv, q_s, st_o, st_m, st_l, att_p, att_n, att_all, lw_s,
    cos_s, sin_s, bias_c, bias_n, perm, sum_s, lsem, ssem, rsem,
):
    sp = lax.axis_index("sp")
    tp = lax.axis_index("tp")
    z, y = sp // NY, sp % NY
    x, core = tp // 2, tp % 2
    sends = []

    def start(src, dst, ridx, dev):
        copy = pltpu.make_async_remote_copy(
            src_ref=src, dst_ref=dst, send_sem=ssem.at[len(sends)], recv_sem=rsem.at[ridx],
            device_id=dev, device_id_type=MESH,
        )
        copy.start()
        sends.append(copy)

    def arrived(dst, ridx):
        pltpu.make_async_remote_copy(
            src_ref=dst, dst_ref=dst, send_sem=ssem.at[0], recv_sem=rsem.at[ridx],
            device_id=((sp + 1) % NSP, tp), device_id_type=MESH,
        ).wait_recv()

    y_peer = [(z * NY + (y + d) % NY, tp) for d in range(NY)]
    z_up = (((z + 1) % NZ) * NY + y, tp)
    z_down = (((z + NZ - 1) % NZ) * NY + y, tp)
    ahead = ((sp + 1) % NSP, tp)
    behind = ((sp + NSP - 1) % NSP, tp)
    t_peer = [(sp, (tp + d) % NTP) for d in range(NTP)]
    x_right = (sp, (tp + 2) % NTP)
    x_left = (sp, (tp + NTP - 2) % NTP)
    sibling = (sp, x * 2 + (1 - core))

    wrow = pl.ds(pl.multiple_of(sp * 32, 32), 32)
    local = [
        pltpu.make_async_copy(wk.at[:, 0:128], w_v.at[0, wrow, 0:128], lsem.at[0]),
        pltpu.make_async_copy(wv.at[:, 0:128], w_v.at[0, wrow, 128:256], lsem.at[1]),
        pltpu.make_async_copy(wk.at[:, 128:256], w_v.at[1, wrow, 0:128], lsem.at[2]),
        pltpu.make_async_copy(wv.at[:, 128:256], w_v.at[1, wrow, 128:256], lsem.at[3]),
        pltpu.make_async_copy(wo, wo_v.at[tp], lsem.at[4]),
        pltpu.make_async_copy(hid, hid_v, lsem.at[5]),
        pltpu.make_async_copy(wq, wq_v, lsem.at[6]),
    ]
    for copy in local:
        copy.start()

    barrier = pltpu.get_barrier_semaphore()
    partners = y_peer[1:] + t_peer[1:] + [z_up, z_down, ahead, behind]
    for dev in partners:
        pl.semaphore_signal(barrier, inc=1, device_id=dev, device_id_type=MESH)
    pl.semaphore_wait(barrier, len(partners))

    def weights_y_send(p):
        local[2 * p].wait()
        local[2 * p + 1].wait()
        for d in range(1, NY):
            start(w_v.at[p, wrow], w_v.at[p, wrow], R_WY + p * (NY - 1) + d - 1, y_peer[d])

    def weights_y_wait(p):
        for d in range(1, NY):
            row = (z * NY + (y + NY - d) % NY) * 32
            arrived(w_v.at[p, pl.ds(pl.multiple_of(row, 32), 32)], R_WY + p * (NY - 1) + d - 1)

    def z_rows(zz, half):
        return pl.ds(pl.multiple_of(zz * 256 + half * 128, 128), 128)

    def z_sem(p, half, direction, hop):
        return R_WZ + ((p * 2 + half) * 2 + direction) * 4 + hop

    def z_hops(half, direction):
        return 4 if half == direction else 3

    def weights_z_send(p):
        for half in range(2):
            part = w_v.at[p, z_rows(z, half)]
            start(part, part, z_sem(p, half, 0, 0), z_up)
            start(part, part, z_sem(p, half, 1, 0), z_down)

    def weights_z_step(p, hop):
        for half in range(2):
            for direction in range(2):
                hops = z_hops(half, direction)
                if hop < hops:
                    zz = (z + NZ - 1 - hop) % NZ if direction == 0 else (z + 1 + hop) % NZ
                    part = w_v.at[p, z_rows(zz, half)]
                    arrived(part, z_sem(p, half, direction, hop))
                    if hop + 1 < hops:
                        start(part, part, z_sem(p, half, direction, hop + 1), z_up if direction == 0 else z_down)

    def wo_part(delta, part):
        group = wo_v.at[(tp + delta) % NTP]
        return group if part is None else group.at[pl.ds(part * 128, 128)]

    def wo_send():
        local[4].wait()
        start(wo_part(0, 0), wo_part(0, 0), R_X + 0, x_right)
        start(wo_part(0, 1), wo_part(0, 1), R_X + 1, x_left)
        start(wo_part(0, 1), wo_part(0, 1), R_X + 2, x_right)
        start(wo_part(0, 0), wo_part(0, 0), R_X + 3, x_left)
        start(wo_part(0, None), wo_part(0, None), R_X + 6, sibling)

    def wo_step(k):
        if k == 0:
            arrived(wo_part(6, 0), R_X + 0)
            start(wo_part(6, 0), wo_part(6, 0), R_X + 4, x_right)
            start(wo_part(6, 0), wo_part(6, 0), R_X + 7, sibling)
            arrived(wo_part(2, 1), R_X + 1)
            start(wo_part(2, 1), wo_part(2, 1), R_X + 5, x_left)
            start(wo_part(2, 1), wo_part(2, 1), R_X + 8, sibling)
        elif k == 1:
            arrived(wo_part(6, 1), R_X + 2)
            start(wo_part(6, 1), wo_part(6, 1), R_X + 9, sibling)
            arrived(wo_part(2, 0), R_X + 3)
            start(wo_part(2, 0), wo_part(2, 0), R_X + 10, sibling)
        else:
            arrived(wo_part(4, 0), R_X + 4)
            start(wo_part(4, 0), wo_part(4, 0), R_X + 11, sibling)
            arrived(wo_part(4, 1), R_X + 5)
            start(wo_part(4, 1), wo_part(4, 1), R_X + 12, sibling)

    def wo_sibling_wait():
        other = x * 2 + (1 - core)

        def part_of(delta, part):
            group = wo_v.at[(other + delta) % NTP]
            return group if part is None else group.at[pl.ds(part * 128, 128)]

        arrived(part_of(0, None), R_X + 6)
        arrived(part_of(6, 0), R_X + 7)
        arrived(part_of(2, 1), R_X + 8)
        arrived(part_of(6, 1), R_X + 9)
        arrived(part_of(2, 0), R_X + 10)
        arrived(part_of(4, 0), R_X + 11)
        arrived(part_of(4, 1), R_X + 12)

    def halo_send(p):
        start(kv.at[0, p], kv.at[1, p], R_H + p * SLOTS + 1, ahead)

    def halo_step(p, k):
        arrived(kv.at[k, p], R_H + p * SLOTS + k)
        if k < SLOTS - 1:
            start(kv.at[k, p], kv.at[k + 1, p], R_H + p * SLOTS + k + 1, ahead)

    lane = lax.broadcasted_iota(jnp.int32, (1, 128), 1)
    first_head = lane < 64
    first_half = (lane % 64) < 32

    def norm():
        local[5].wait()

        def step(i, _):
            rows = pl.ds(pl.multiple_of(i * 32, 32), 32)
            h = hid_v[rows, :].astype(F32)
            scale = lax.rsqrt(jnp.mean(h * h, axis=-1, keepdims=True) + EPS)
            hid_v[rows, :] = (h * scale * gain[...]).astype(BF16)
            return 0

        lax.fori_loop(0, ROWS // 32, step, 0)

    def permutation():
        token = token_of(lax.broadcasted_iota(jnp.int32, (ROWS, ROWS), 0))
        col = lax.broadcasted_iota(jnp.int32, (ROWS, ROWS), 1)
        perm[0] = (token == col).astype(F32).astype(BF16)
        row = lax.broadcasted_iota(jnp.int32, (ROWS, ROWS), 0)
        token_c = token_of(lax.broadcasted_iota(jnp.int32, (ROWS, ROWS), 1))
        perm[1] = (token_c == row).astype(F32).astype(BF16)

    def permute():
        def step(i, _):
            rows = pl.ds(pl.multiple_of(i * 128, 128), 128)
            for c in range(4):
                np_v[rows, c * 512 : (c + 1) * 512] = dot(perm[0, rows, :], hid_v[:, c * 512 : (c + 1) * 512]).astype(BF16)
            return 0

        lax.fori_loop(0, 4, step, 0)

    def tables():
        token = token_of(lax.broadcasted_iota(jnp.int32, (ROWS, 128), 0))
        angle = (sp * ROWS + token).astype(F32) * freq[...]
        cos_s[...] = jnp.cos(angle)
        sine = jnp.sin(angle)
        sin_s[...] = jnp.where(first_half, -sine, sine)

    def biases():
        row = lax.broadcasted_iota(jnp.int32, (128, 128), 0)
        col = lax.broadcasted_iota(jnp.int32, (128, 128), 1)

        def class_token(r):
            return (r // 32) * 128 + (r % 8) * 16 + ((r // 8) % 4) * 4

        for k in range(SLOTS):
            delta = class_token(row) - class_token(col) + ROWS * k
            near = (delta >= 0) & (delta <= 4 * SPAN)
            far = (delta >= 0) & (delta <= 16 * SPAN) & ((row // 8) % 4 == (col // 8) % 4)
            bias = jnp.where(near & far, 1.0, jnp.where(near | far, 0.0, NEG))
            bias_c[:, k * 128 : (k + 1) * 128] = jnp.where(sp >= k, bias, NEG)

        def near_token(r):
            return (r // 32) + (r % 8) * 16 + ((r // 8) % 4) * 4

        delta = near_token(row) - near_token(col)
        own = jnp.where((delta >= 0) & (delta <= SPAN), 0.0, NEG)
        delta = delta + 128
        prev = jnp.where((delta >= 0) & (delta <= SPAN), 0.0, NEG)
        bias_n[0, :, 0:128] = jnp.where(sp >= 1, prev, NEG)
        bias_n[1, :, 0:128] = prev
        bias_n[0, :, 128:256] = own
        bias_n[1, :, 128:256] = own

    def rotate(u, rows):
        swapped = jnp.where(first_half, pltpu.roll(u, 96, 1), pltpu.roll(u, 32, 1))
        return (u * cos_s[rows, :] + swapped * sin_s[rows, :]).astype(BF16)

    def queries():
        local[6].wait()

        def step(r, _):
            rows = pl.ds(pl.multiple_of(r * 128, 128), 128)
            q = dot(np_v[rows, :], wq_v[...])
            for p in range(2):
                turned = rotate(q[:, p * 128 : (p + 1) * 128], rows)
                zero = jnp.zeros_like(turned)
                q_s[p, r, 0:128, :] = jnp.where(first_head, turned, zero)
                q_s[p, r, 128:256, :] = jnp.where(first_head, zero, turned)
            return 0

        lax.fori_loop(0, 4, step, 0)

    def keys_values(p):
        def step(r, _):
            rows = pl.ds(pl.multiple_of(r * 128, 128), 128)
            both = dot(np_v[rows, :], w_v[p])
            kv[0, p, 0, rows, :] = rotate(both[:, 0:128], rows)
            kv[0, p, 1, rows, :] = both[:, 128:256].astype(BF16)
            return 0

        lax.fori_loop(0, 4, step, 0)

    def near(p, first, last):
        def step(b, _):
            slot = (3 - b) // 3
            before = (b + 3) % 4

            def part(r, base):
                return pl.ds(pl.multiple_of(base + r * 128, 32), 32)

            q = jnp.concatenate(
                [q_s[p, r, pl.ds(pl.multiple_of(h * 128 + b * 32, 32), 32), :] for h in range(2) for r in range(4)], axis=0
            )
            k, v = (
                jnp.concatenate(
                    [kv[slot, p, w, part(r, before * 32), :] for r in range(4)]
                    + [kv[0, p, w, part(r, b * 32), :] for r in range(4)],
                    axis=0,
                )
                for w in range(2)
            )
            bias = bias_n[jnp.minimum(b, 1)]
            s = dot(q, k, NT) * SCALE2 + jnp.concatenate([bias, bias], axis=0)
            m = jnp.max(s, axis=-1, keepdims=True)
            e = jnp.exp2(s - m)
            total = jnp.sum(e, axis=-1, keepdims=True)
            o = dot(e.astype(BF16), v)
            m = jnp.broadcast_to(m, o.shape)
            total = jnp.broadcast_to(total, o.shape)
            for h in range(2):
                for r in range(4):
                    at = pl.ds(pl.multiple_of(h * 128 + b * 32, 32), 32)
                    piece = slice(h * 128 + r * 32, h * 128 + r * 32 + 32)
                    st_o[p, r, at, :] = o[piece]
                    st_m[p, r, at, :] = m[piece]
                    st_l[p, r, at, :] = total[piece]
            return 0

        lax.fori_loop(first, last, step, 0)

    def far(p, slots):
        def step(r, _):
            rows = pl.ds(pl.multiple_of(r * 128, 128), 128)
            k, v = (
                jnp.concatenate([kv[s, p, w, rows, :] for s in slots], axis=0) if len(slots) > 1 else kv[slots[0], p, w, rows, :]
                for w in range(2)
            )
            bias = bias_c[:, slots[0] * 128 : (slots[-1] + 1) * 128]
            s = dot(q_s[p, r], k, NT) * SCALE2 + jnp.concatenate([bias, bias], axis=0)
            m_old = st_m[p, r]
            m = jnp.maximum(m_old, jnp.broadcast_to(jnp.max(s, axis=-1, keepdims=True), m_old.shape))
            wide = m if len(slots) == 1 else jnp.concatenate([m] * len(slots), axis=1)
            e = jnp.exp2(s - wide)
            decay = jnp.exp2(m_old - m)
            st_l[p, r] = st_l[p, r] * decay + jnp.broadcast_to(jnp.sum(e, axis=-1, keepdims=True), m.shape)
            st_o[p, r] = st_o[p, r] * decay + dot(e.astype(BF16), v)
            st_m[p, r] = m
            return 0

        lax.fori_loop(0, 4, step, 0)

    def finish(p):
        for r in range(4):
            rows = slice(r * 128, (r + 1) * 128)
            o = st_o[p, r] / st_l[p, r]
            att_p[rows, :] = jnp.where(first_head, o[0:128], o[128:256]).astype(BF16)
            level = st_m[p, r] * LN2 + jnp.log(st_l[p, r])
            both = jnp.where(lane == 2 * p, level[0:128], level[128:256])
            if p == 0:
                lw_s[rows, :] = both
            else:
                lw_s[rows, :] = jnp.where(lane < 2, lw_s[rows, :], both)
        att_n[p] = dot(perm[1], att_p[...]).astype(BF16)
        att_all[p, tp] = att_n[p, pl.ds(pl.multiple_of(tp * OUT_ROWS, OUT_ROWS), OUT_ROWS), :]
        for d in range(1, NTP):
            rows = pl.ds(pl.multiple_of(((tp + d) % NTP) * OUT_ROWS, OUT_ROWS), OUT_ROWS)
            start(att_n.at[p, rows], att_all.at[p, tp], R_A + p * (NTP - 1) + d - 1, t_peer[d])

    def attended_wait(p):
        for d in range(1, NTP):
            arrived(att_all.at[p, (tp + NTP - d) % NTP], R_A + p * (NTP - 1) + d - 1)

    def log_weights():
        levels = jnp.transpose(lw_s[...])[0:8, :]
        high = levels.astype(BF16)
        rest = levels - high.astype(F32)
        mid = rest.astype(BF16)
        low = (rest - mid.astype(F32)).astype(BF16)
        natural = dot(high, perm[0]) + dot(mid, perm[0]) + dot(low, perm[0])
        lw_out[...] = natural[0:4, :]

    def project():
        def step(c, squares):
            cols = pl.ds(pl.multiple_of(c * 512, 512), 512)
            total = None
            for g in range(NTP):
                a = jnp.concatenate([att_all[0, g], att_all[1, g]], axis=1)
                part = dot(a, wo_v[g, :, cols]).astype(BF16).astype(F32)
                total = part if total is None else total + part
            sum_s[:, cols] = total
            return squares + jnp.sum(total * total, axis=-1, keepdims=True)

        squares = lax.fori_loop(0, 4, step, jnp.zeros((OUT_ROWS, 1), F32))
        scale = lax.rsqrt(squares / D + EPS)
        out[...] = (sum_s[...] * scale * post[...]).astype(BF16)

    weights_y_send(0)
    wo_send()
    weights_y_send(1)
    norm()
    weights_y_wait(0)
    weights_z_send(0)
    weights_y_wait(1)
    permutation()
    permute()
    weights_z_step(0, 0)
    tables()
    biases()
    weights_z_step(0, 1)
    queries()
    weights_z_step(0, 2)
    weights_z_send(1)
    wo_step(0)
    weights_z_step(0, 3)
    keys_values(0)
    halo_send(0)
    weights_z_step(1, 0)
    near(0, 1, 4)
    weights_z_step(1, 1)
    halo_step(0, 1)
    near(0, 0, 1)
    weights_z_step(1, 2)
    far(0, (0, 1))
    weights_z_step(1, 3)
    keys_values(1)
    halo_send(1)
    halo_step(0, 2)
    wo_step(1)
    near(1, 1, 4)
    halo_step(0, 3)
    far(0, (2, 3))
    halo_step(1, 1)
    wo_step(2)
    near(1, 0, 1)
    far(1, (0, 1))
    halo_step(0, 4)
    far(0, (4,))
    finish(0)
    halo_step(1, 2)
    halo_step(1, 3)
    far(1, (2, 3))
    wo_sibling_wait()
    attended_wait(0)
    halo_step(1, 4)
    far(1, (4,))
    finish(1)
    log_weights()
    attended_wait(1)
    project()
    for copy in sends:
        copy.wait_send()


def body(hidden_in, pre_gain, query_proj, key_proj, value_proj, out_proj, post_gain):
    half = np.arange(HEAD_DIM // 2, dtype=np.float32) * np.float32(2.0) / np.float32(HEAD_DIM)
    freq = np.tile(np.power(np.float64(ROPE_BASE), -half.astype(np.float64)).astype(np.float32), 4).reshape(1, 128)
    any_spec = pl.BlockSpec(memory_space=pl.ANY)
    vmem = pl.BlockSpec(memory_space=pltpu.VMEM)
    return pl.pallas_call(
        kernel,
        out_shape=(jax.ShapeDtypeStruct((OUT_ROWS, D), BF16), jax.ShapeDtypeStruct((4, ROWS), F32)),
        in_specs=[any_spec, vmem, vmem, any_spec, any_spec, any_spec, any_spec, vmem],
        out_specs=(vmem, vmem),
        scratch_shapes=[
            pltpu.VMEM((ROWS, D), BF16),
            pltpu.VMEM((ROWS, D), BF16),
            pltpu.VMEM((D, WIDTH), BF16),
            pltpu.VMEM((2, D, WIDTH), BF16),
            pltpu.VMEM((NTP, WIDTH, D), BF16),
            pltpu.VMEM((SLOTS, 2, 2, ROWS, 128), BF16),
            pltpu.VMEM((2, 4, 256, 128), BF16),
            pltpu.VMEM((2, 4, 256, 128), F32),
            pltpu.VMEM((2, 4, 256, 128), F32),
            pltpu.VMEM((2, 4, 256, 128), F32),
            pltpu.VMEM((ROWS, 128), BF16),
            pltpu.VMEM((2, ROWS, 128), BF16),
            pltpu.VMEM((2, NTP, OUT_ROWS, 128), BF16),
            pltpu.VMEM((ROWS, 128), F32),
            pltpu.VMEM((ROWS, 128), F32),
            pltpu.VMEM((ROWS, 128), F32),
            pltpu.VMEM((128, SLOTS * 128), F32),
            pltpu.VMEM((2, 128, 256), F32),
            pltpu.VMEM((2, ROWS, ROWS), BF16),
            pltpu.VMEM((OUT_ROWS, D), F32),
            pltpu.SemaphoreType.DMA((7,)),
            pltpu.SemaphoreType.DMA((N_SEND,)),
            pltpu.SemaphoreType.DMA((R_END,)),
        ],
        compiler_params=pltpu.CompilerParams(
            collective_id=0, has_side_effects=True, vmem_limit_bytes=60 * 1024 * 1024
        ),
        name="layer",
    )(
        hidden_in, pre_gain.reshape(1, D), jnp.asarray(freq), query_proj, key_proj, value_proj, out_proj,
        post_gain.reshape(1, D),
    )


def solution(mesh):
    placed = (P("sp", None), P(), P(None, "tp"), P("sp", "tp"), P("sp", "tp"), P("tp", None), P())
    return jax.shard_map(
        body,
        mesh=mesh,
        in_specs=placed,
        out_specs=(P(("sp", "tp"), None), P("tp", "sp")),
        check_vma=False,
    )
```

```python
import functools
import math

import jax
import jax.numpy as jnp
import numpy as np
from jax import lax
from jax.experimental import pallas as pl
from jax.experimental.pallas import tpu as pltpu
from jax.sharding import PartitionSpec as P

HEAD_DIM = 64
SPAN = 128
EPS = 1e-06
ROPE_BASE = 10000.0
NY = 8
NZ = 8
NSP = NY * NZ
NTP = 8
NX = 4
ROWS = 512
D = 2048
WIDTH = 256
OUT_ROWS = 64
SLOTS = 5
NEG = -1e30
SCALE2 = math.log2(math.e) / 8.0
LN2 = math.log(2.0)
F32 = jnp.float32
BF16 = jnp.bfloat16
MESH = pl.DeviceIdType.MESH

NT = (((1,), (1,)), ((), ()))
NN = (((1,), (0,)), ((), ()))

AHEAD_ROWS = 320

R_WD = 0
R_WR = R_WD + 2 * 2 * 7
R_X = R_WR + 2 * 2 * 2 * 2 * 4
R_H = R_X + 16
R_M = R_H + 2 * SLOTS
R_A = R_M + 2 * SLOTS
R_END = R_A + 2 * (NTP - 1)
N_SEND = 140


def dot(a, b, dims=NN):
    return lax.dot_general(a, b, dims, preferred_element_type=F32)


def token_of(row):
    return (row // 128) + ((row // 8) % 4) * 4 + (row % 8) * 16 + ((row // 32) % 4) * 128


def kernel(
    hid, gain, freq, wq, wk, wv, wo, post,
    out, lw_out,
    hid_v, np_v, wq_v, w_v, wo_v, kv, passing, q_s, st_o, st_m, st_l, att_p, att_n, att_all, lw_s,
    cos_s, sin_s, bias_c, bias_n, perm, sum_s, lsem, ssem, rsem,
):
    sp = lax.axis_index("sp")
    tp = lax.axis_index("tp")
    z, y = sp // NY, sp % NY
    x, core = tp // 2, tp % 2
    sends = []

    def start(src, dst, ridx, dev):
        copy = pltpu.make_async_remote_copy(
            src_ref=src, dst_ref=dst, send_sem=ssem.at[len(sends)], recv_sem=rsem.at[ridx],
            device_id=dev, device_id_type=MESH,
        )
        copy.start()
        sends.append(copy)

    def arrived(dst, ridx):
        pltpu.make_async_remote_copy(
            src_ref=dst, dst_ref=dst, send_sem=ssem.at[0], recv_sem=rsem.at[ridx],
            device_id=((sp + 1) % NSP, tp), device_id_type=MESH,
        ).wait_recv()

    y_peer = [(z * NY + (y + d) % NY, tp) for d in range(NY)]
    z_peer = [(((z + d) % NZ) * NY + y, tp) for d in range(NZ)]
    ahead = ((sp + 1) % NSP, tp)
    behind = ((sp + NSP - 1) % NSP, tp)
    relay_of_me = y_peer[NY - 3]
    relay_to = ((z * NY + (y + 3) % NY + 4) % NSP, tp)
    source = (sp + NSP - 4) % NSP
    relay_from = ((source // NY) * NY + (source % NY + NY - 3) % NY, tp)
    t_peer = [(sp, (tp + d) % NTP) for d in range(NTP)]
    x_right = (sp, (tp + 2) % NTP)
    x_left = (sp, (tp + NTP - 2) % NTP)
    sibling = (sp, x * 2 + (1 - core))

    local = [
        pltpu.make_async_copy(w.at[:, p * 128 : (p + 1) * 128], w_v.at[i, p, z, y], lsem.at[2 * p + i])
        for p in range(2)
        for i, w in enumerate((wk, wv))
    ] + [
        pltpu.make_async_copy(wo, wo_v.at[tp], lsem.at[4]),
        pltpu.make_async_copy(hid, hid_v, lsem.at[5]),
        pltpu.make_async_copy(wq, wq_v, lsem.at[6]),
    ]
    for copy in local:
        copy.start()

    barrier = pltpu.get_barrier_semaphore()
    partners = y_peer[1:] + z_peer[1:] + t_peer[1:] + [ahead, behind, relay_to, relay_from]
    for dev in partners:
        pl.semaphore_signal(barrier, inc=1, device_id=dev, device_id_type=MESH)
    pl.semaphore_wait(barrier, len(partners))

    def weights_send(p):
        for i, peer in enumerate((y_peer, z_peer)):
            local[2 * p + i].wait()
            part = w_v.at[i, p, z, y]
            for d in range(1, 8):
                start(part, part, R_WD + (i * 2 + p) * 7 + d - 1, peer[d])

    def weights_wait(p):
        for d in range(1, 8):
            arrived(w_v.at[0, p, z, (y + NY - d) % NY], R_WD + p * 7 + d - 1)
            arrived(w_v.at[1, p, (z + NZ - d) % NZ, y], R_WD + (2 + p) * 7 + d - 1)

    def relay_part(i, p, at, half):
        piece = pl.ds(half * 4, 4)
        return w_v.at[0, p, at, piece] if i == 0 else w_v.at[1, p, piece, at]

    def relay_sem(i, p, half, direction, hop):
        return R_WR + (((i * 2 + p) * 2 + half) * 2 + direction) * 4 + hop

    def relay_dev(i, direction):
        peer = z_peer if i == 0 else y_peer
        return peer[1] if direction == 0 else peer[7]

    def relay_send(p):
        for half in range(2):
            for i, at in enumerate((z, y)):
                part = relay_part(i, p, at, half)
                for direction in range(2):
                    start(part, part, relay_sem(i, p, half, direction, 0), relay_dev(i, direction))

    def relay_step(p, hop):
        for half in range(2):
            for i, at in enumerate((z, y)):
                for direction in range(2):
                    hops = 4 if half == direction else 3
                    if hop < hops:
                        owner = (at + 7 - hop) % 8 if direction == 0 else (at + 1 + hop) % 8
                        part = relay_part(i, p, owner, half)
                        arrived(part, relay_sem(i, p, half, direction, hop))
                        if hop + 1 < hops:
                            start(part, part, relay_sem(i, p, half, direction, hop + 1), relay_dev(i, direction))

    def wo_part(delta, part):
        group = wo_v.at[(tp + delta) % NTP]
        return group if part is None else group.at[pl.ds(part * 128, 128)]

    def wo_send():
        local[4].wait()
        start(wo_part(0, 0), wo_part(0, 0), R_X + 0, x_right)
        start(wo_part(0, 1), wo_part(0, 1), R_X + 1, x_left)
        start(wo_part(0, 1), wo_part(0, 1), R_X + 2, x_right)
        start(wo_part(0, 0), wo_part(0, 0), R_X + 3, x_left)
        start(wo_part(0, None), wo_part(0, None), R_X + 6, sibling)

    def wo_step(k):
        if k == 0:
            arrived(wo_part(6, 0), R_X + 0)
            start(wo_part(6, 0), wo_part(6, 0), R_X + 4, x_right)
            start(wo_part(6, 0), wo_part(6, 0), R_X + 7, sibling)
            arrived(wo_part(2, 1), R_X + 1)
            start(wo_part(2, 1), wo_part(2, 1), R_X + 5, x_left)
            start(wo_part(2, 1), wo_part(2, 1), R_X + 8, sibling)
        elif k == 1:
            arrived(wo_part(6, 1), R_X + 2)
            start(wo_part(6, 1), wo_part(6, 1), R_X + 9, sibling)
            arrived(wo_part(2, 0), R_X + 3)
            start(wo_part(2, 0), wo_part(2, 0), R_X + 10, sibling)
        else:
            arrived(wo_part(4, 0), R_X + 4)
            start(wo_part(4, 0), wo_part(4, 0), R_X + 11, sibling)
            arrived(wo_part(4, 1), R_X + 5)
            start(wo_part(4, 1), wo_part(4, 1), R_X + 12, sibling)

    def wo_sibling_wait():
        other = x * 2 + (1 - core)

        def part_of(delta, part):
            group = wo_v.at[(other + delta) % NTP]
            return group if part is None else group.at[pl.ds(part * 128, 128)]

        arrived(part_of(0, None), R_X + 6)
        arrived(part_of(6, 0), R_X + 7)
        arrived(part_of(2, 1), R_X + 8)
        arrived(part_of(6, 1), R_X + 9)
        arrived(part_of(2, 0), R_X + 10)
        arrived(part_of(4, 0), R_X + 11)
        arrived(part_of(4, 1), R_X + 12)

    def up_part(k, p):
        return kv.at[k, p, :, 0:AHEAD_ROWS]

    def down_part(k, p):
        return kv.at[k, p, :, AHEAD_ROWS:ROWS]

    def halo_send(p):
        start(up_part(0, p), up_part(1, p), R_H + p * SLOTS + 1, ahead)
        start(down_part(0, p), passing.at[p], R_M + p * SLOTS, relay_of_me)

    def up(p, k):
        arrived(up_part(k, p), R_H + p * SLOTS + k)
        if k < SLOTS - 1:
            start(up_part(k, p), up_part(k + 1, p), R_H + p * SLOTS + k + 1, ahead)

    def down(p, k):
        if k == 0:
            arrived(passing.at[p], R_M + p * SLOTS)
            start(passing.at[p], down_part(4, p), R_M + p * SLOTS + 4, relay_to)
        else:
            arrived(down_part(k, p), R_M + p * SLOTS + k)
            if k > 1:
                start(down_part(k, p), down_part(k - 1, p), R_M + p * SLOTS + k - 1, behind)

    lane = lax.broadcasted_iota(jnp.int32, (1, 128), 1)
    first_head = lane < 64
    first_half = (lane % 64) < 32

    def norm():
        local[5].wait()

        def step(i, _):
            rows = pl.ds(pl.multiple_of(i * 32, 32), 32)
            h = hid_v[rows, :].astype(F32)
            scale = lax.rsqrt(jnp.mean(h * h, axis=-1, keepdims=True) + EPS)
            hid_v[rows, :] = (h * scale * gain[...]).astype(BF16)
            return 0

        lax.fori_loop(0, ROWS // 32, step, 0)

    def permutation():
        token = token_of(lax.broadcasted_iota(jnp.int32, (ROWS, ROWS), 0))
        col = lax.broadcasted_iota(jnp.int32, (ROWS, ROWS), 1)
        perm[0] = (token == col).astype(F32).astype(BF16)
        row = lax.broadcasted_iota(jnp.int32, (ROWS, ROWS), 0)
        token_c = token_of(lax.broadcasted_iota(jnp.int32, (ROWS, ROWS), 1))
        perm[1] = (token_c == row).astype(F32).astype(BF16)

    def permute():
        def step(i, _):
            rows = pl.ds(pl.multiple_of(i * 128, 128), 128)
            for c in range(4):
                np_v[rows, c * 512 : (c + 1) * 512] = dot(perm[0, rows, :], hid_v[:, c * 512 : (c + 1) * 512]).astype(BF16)
            return 0

        lax.fori_loop(0, 4, step, 0)

    def tables():
        token = token_of(lax.broadcasted_iota(jnp.int32, (ROWS, 128), 0))
        angle = (sp * ROWS + token).astype(F32) * freq[...]
        cos_s[...] = jnp.cos(angle)
        sine = jnp.sin(angle)
        sin_s[...] = jnp.where(first_half, -sine, sine)

    def biases():
        row = lax.broadcasted_iota(jnp.int32, (128, 128), 0)
        col = lax.broadcasted_iota(jnp.int32, (128, 128), 1)

        def class_token(r):
            return (r // 32) * 128 + (r % 8) * 16 + ((r // 8) % 4) * 4

        for k in range(SLOTS):
            delta = class_token(row) - class_token(col) + ROWS * k
            near = (delta >= 0) & (delta <= 4 * SPAN)
            far = (delta >= 0) & (delta <= 16 * SPAN) & ((row // 8) % 4 == (col // 8) % 4)
            bias = jnp.where(near & far, 1.0, jnp.where(near | far, 0.0, NEG))
            bias_c[:, k * 128 : (k + 1) * 128] = jnp.where(sp >= k, bias, NEG)

        def near_token(r):
            return (r // 32) + (r % 8) * 16 + ((r // 8) % 4) * 4

        delta = near_token(row) - near_token(col)
        own = jnp.where((delta >= 0) & (delta <= SPAN), 0.0, NEG)
        delta = delta + 128
        prev = jnp.where((delta >= 0) & (delta <= SPAN), 0.0, NEG)
        bias_n[0, :, 0:128] = jnp.where(sp >= 1, prev, NEG)
        bias_n[1, :, 0:128] = prev
        bias_n[0, :, 128:256] = own
        bias_n[1, :, 128:256] = own

    def rotate(u, rows):
        swapped = jnp.where(first_half, pltpu.roll(u, 96, 1), pltpu.roll(u, 32, 1))
        return (u * cos_s[rows, :] + swapped * sin_s[rows, :]).astype(BF16)

    def queries():
        local[6].wait()

        def step(r, _):
            rows = pl.ds(pl.multiple_of(r * 128, 128), 128)
            q = dot(np_v[rows, :], wq_v[...])
            for p in range(2):
                turned = rotate(q[:, p * 128 : (p + 1) * 128], rows)
                zero = jnp.zeros_like(turned)
                q_s[p, r, 0:128, :] = jnp.where(first_head, turned, zero)
                q_s[p, r, 128:256, :] = jnp.where(first_head, zero, turned)
            return 0

        lax.fori_loop(0, 4, step, 0)

    def keys_values(p):
        weights = jnp.concatenate([w_v[i, p].reshape(D, 128) for i in range(2)], axis=1)

        def step(r, _):
            rows = pl.ds(pl.multiple_of(r * 128, 128), 128)
            both = dot(np_v[rows, :], weights)
            kv[0, p, 0, rows, :] = rotate(both[:, 0:128], rows)
            kv[0, p, 1, rows, :] = both[:, 128:256].astype(BF16)
            return 0

        lax.fori_loop(0, 4, step, 0)

    def near(p, first, last):
        def step(b, _):
            slot = (3 - b) // 3
            before = (b + 3) % 4
            state = [(r, pl.ds(pl.multiple_of(h * 128 + b * 32, 32), 32)) for h in range(2) for r in range(4)]

            def gathered(ref):
                return jnp.concatenate([ref[p, r, at, :] for r, at in state], axis=0)

            def scattered(ref, value):
                for i, (r, at) in enumerate(state):
                    ref[p, r, at, :] = value[i * 32 : (i + 1) * 32]

            def part(r, base):
                return pl.ds(pl.multiple_of(base + r * 128, 32), 32)

            k, v = (
                jnp.concatenate(
                    [kv[slot, p, w, part(r, before * 32), :] for r in range(4)]
                    + [kv[0, p, w, part(r, b * 32), :] for r in range(4)],
                    axis=0,
                )
                for w in range(2)
            )
            o, m, total = update(
                gathered(q_s), k, v, bias_n[jnp.minimum(b, 1)], (gathered(st_o), gathered(st_m), gathered(st_l))
            )
            scattered(st_o, o)
            scattered(st_m, m)
            scattered(st_l, total)
            return 0

        lax.fori_loop(first, last, step, 0)

    def update(q, k, v, bias, state):
        s = dot(q, k, NT) * SCALE2 + jnp.concatenate([bias, bias], axis=0)
        m = jnp.broadcast_to(jnp.max(s, axis=-1, keepdims=True), q.shape)
        if state is not None:
            m = jnp.maximum(m, state[1])
        e = jnp.exp2(s - jnp.concatenate([m] * (s.shape[1] // 128), axis=1))
        total = jnp.broadcast_to(jnp.sum(e, axis=-1, keepdims=True), q.shape)
        o = dot(e.astype(BF16), v)
        if state is not None:
            decay = jnp.exp2(state[1] - m)
            total = state[2] * decay + total
            o = state[0] * decay + o
        return o, m, total

    def far(p, first, last, slots):
        def step(r, _):
            rows = pl.ds(pl.multiple_of(r * 128, 128), 128)
            k, v = (jnp.concatenate([kv[s, p, w, rows, :] for s in slots], axis=0) for w in range(2))
            bias = bias_c[:, slots[0] * 128 : (slots[-1] + 1) * 128]
            state = None if slots[0] == 0 else (st_o[p, r], st_m[p, r], st_l[p, r])
            st_o[p, r], st_m[p, r], st_l[p, r] = update(q_s[p, r], k, v, bias, state)
            return 0

        lax.fori_loop(first, last, step, 0)

    def finish(p):
        for r in range(4):
            rows = slice(r * 128, (r + 1) * 128)
            o = st_o[p, r] / st_l[p, r]
            att_p[rows, :] = jnp.where(first_head, o[0:128], o[128:256]).astype(BF16)
            level = st_m[p, r] * LN2 + jnp.log(st_l[p, r])
            both = jnp.where(lane == 2 * p, level[0:128], level[128:256])
            if p == 0:
                lw_s[rows, :] = both
            else:
                lw_s[rows, :] = jnp.where(lane < 2, lw_s[rows, :], both)
        att_n[p] = dot(perm[1], att_p[...]).astype(BF16)
        att_all[p, tp] = att_n[p, pl.ds(pl.multiple_of(tp * OUT_ROWS, OUT_ROWS), OUT_ROWS), :]
        for d in range(1, NTP):
            rows = pl.ds(pl.multiple_of(((tp + d) % NTP) * OUT_ROWS, OUT_ROWS), OUT_ROWS)
            start(att_n.at[p, rows], att_all.at[p, tp], R_A + p * (NTP - 1) + d - 1, t_peer[d])

    def attended_wait(p):
        for d in range(1, NTP):
            arrived(att_all.at[p, (tp + NTP - d) % NTP], R_A + p * (NTP - 1) + d - 1)

    def log_weights():
        levels = jnp.transpose(lw_s[...])[0:8, :]
        high = levels.astype(BF16)
        rest = levels - high.astype(F32)
        mid = rest.astype(BF16)
        low = (rest - mid.astype(F32)).astype(BF16)
        natural = dot(high, perm[0]) + dot(mid, perm[0]) + dot(low, perm[0])
        lw_out[...] = natural[0:4, :]

    def project():
        def step(c, squares):
            cols = pl.ds(pl.multiple_of(c * 512, 512), 512)
            total = None
            for g in range(NTP):
                a = jnp.concatenate([att_all[0, g], att_all[1, g]], axis=1)
                part = dot(a, wo_v[g, :, cols]).astype(BF16).astype(F32)
                total = part if total is None else total + part
            sum_s[:, cols] = total
            return squares + jnp.sum(total * total, axis=-1, keepdims=True)

        squares = lax.fori_loop(0, 4, step, jnp.zeros((OUT_ROWS, 1), F32))
        scale = lax.rsqrt(squares / D + EPS)
        out[...] = (sum_s[...] * scale * post[...]).astype(BF16)

    weights_send(0)
    weights_send(1)
    wo_send()
    norm()
    permutation()
    weights_wait(0)
    relay_send(0)
    weights_wait(1)
    relay_send(1)
    permute()
    relay_step(0, 0)
    relay_step(1, 0)
    tables()
    biases()
    relay_step(0, 1)
    relay_step(1, 1)
    queries()
    relay_step(0, 2)
    relay_step(1, 2)
    wo_step(0)
    relay_step(0, 3)
    keys_values(0)
    halo_send(0)
    relay_step(1, 3)
    keys_values(1)
    halo_send(1)
    far(0, 0, 4, (0,))
    near(0, 1, 4)
    up(0, 1)
    far(1, 0, 4, (0,))
    down(0, 0)
    up(1, 1)
    near(1, 1, 4)
    wo_step(1)
    down(1, 0)
    up(0, 2)
    far(0, 0, 2, (1, 2))
    down(0, 4)
    up(1, 2)
    far(1, 0, 2, (1, 2))
    down(1, 4)
    down(0, 3)
    up(0, 3)
    wo_step(2)
    down(1, 3)
    far(0, 3, 4, (3, 4))
    up(1, 3)
    far(1, 3, 4, (3, 4))
    down(0, 2)
    up(0, 4)
    far(0, 0, 2, (3, 4))
    down(1, 2)
    far(0, 2, 3, (3, 4))
    down(0, 1)
    far(0, 2, 4, (1, 2))
    near(0, 0, 1)
    finish(0)
    up(1, 4)
    far(1, 0, 3, (3, 4))
    down(1, 1)
    far(1, 2, 4, (1, 2))
    near(1, 0, 1)
    finish(1)
    wo_sibling_wait()
    attended_wait(0)
    log_weights()
    attended_wait(1)
    project()
    for copy in sends:
        copy.wait_send()


def body(hidden_in, pre_gain, query_proj, key_proj, value_proj, out_proj, post_gain):
    half = np.arange(HEAD_DIM // 2, dtype=np.float32) * np.float32(2.0) / np.float32(HEAD_DIM)
    freq = np.tile(np.power(np.float64(ROPE_BASE), -half.astype(np.float64)).astype(np.float32), 4).reshape(1, 128)
    any_spec = pl.BlockSpec(memory_space=pl.ANY)
    vmem = pl.BlockSpec(memory_space=pltpu.VMEM)
    return pl.pallas_call(
        kernel,
        out_shape=(jax.ShapeDtypeStruct((OUT_ROWS, D), BF16), jax.ShapeDtypeStruct((4, ROWS), F32)),
        in_specs=[any_spec, vmem, vmem, any_spec, any_spec, any_spec, any_spec, vmem],
        out_specs=(vmem, vmem),
        scratch_shapes=[
            pltpu.VMEM((ROWS, D), BF16),
            pltpu.VMEM((ROWS, D), BF16),
            pltpu.VMEM((D, WIDTH), BF16),
            pltpu.VMEM((2, 2, NZ, NY, D // NSP, 128), BF16),
            pltpu.VMEM((NTP, WIDTH, D), BF16),
            pltpu.VMEM((SLOTS, 2, 2, ROWS, 128), BF16),
            pltpu.VMEM((2, 2, ROWS - AHEAD_ROWS, 128), BF16),
            pltpu.VMEM((2, 4, 256, 128), BF16),
            pltpu.VMEM((2, 4, 256, 128), F32),
            pltpu.VMEM((2, 4, 256, 128), F32),
            pltpu.VMEM((2, 4, 256, 128), F32),
            pltpu.VMEM((ROWS, 128), BF16),
            pltpu.VMEM((2, ROWS, 128), BF16),
            pltpu.VMEM((2, NTP, OUT_ROWS, 128), BF16),
            pltpu.VMEM((ROWS, 128), F32),
            pltpu.VMEM((ROWS, 128), F32),
            pltpu.VMEM((ROWS, 128), F32),
            pltpu.VMEM((128, SLOTS * 128), F32),
            pltpu.VMEM((2, 128, 256), F32),
            pltpu.VMEM((2, ROWS, ROWS), BF16),
            pltpu.VMEM((OUT_ROWS, D), F32),
            pltpu.SemaphoreType.DMA((7,)),
            pltpu.SemaphoreType.DMA((N_SEND,)),
            pltpu.SemaphoreType.DMA((R_END,)),
        ],
        compiler_params=pltpu.CompilerParams(
            collective_id=0, has_side_effects=True, vmem_limit_bytes=60 * 1024 * 1024
        ),
        name="layer",
    )(
        hidden_in, pre_gain.reshape(1, D), jnp.asarray(freq), query_proj, key_proj, value_proj, out_proj,
        post_gain.reshape(1, D),
    )


def solution(mesh):
    placed = (P("sp", None), P(), P(None, "tp"), P("sp", "tp"), P("sp", "tp"), P("tp", None), P())
    return jax.shard_map(
        body,
        mesh=mesh,
        in_specs=placed,
        out_specs=(P(("sp", "tp"), None), P("tp", "sp")),
        check_vma=False,
    )
```

```python
import functools
import math

import jax
import jax.numpy as jnp
import numpy as np
from jax import lax
from jax.experimental import pallas as pl
from jax.experimental.pallas import tpu as pltpu
from jax.sharding import PartitionSpec as P

HEAD_DIM = 64
SPAN = 128
EPS = 1e-06
ROPE_BASE = 10000.0
NY = 8
NZ = 8
NSP = NY * NZ
NTP = 8
NX = 4
ROWS = 512
D = 2048
WIDTH = 256
OUT_ROWS = 64
SLOTS = 5
NEG = -1e30
SCALE2 = math.log2(math.e) / 8.0
LN2 = math.log(2.0)
BIG = 512
F32 = jnp.float32
BF16 = jnp.bfloat16
MESH = pl.DeviceIdType.MESH

NT = (((1,), (1,)), ((), ()))
NN = (((1,), (0,)), ((), ()))

AHEAD_ROWS = 320

R_WD = 0
R_WR = R_WD + 2 * 2 * 7
R_X = R_WR + 2 * 2 * 2 * 2 * 4
R_H = R_X + 16
R_M = R_H + 2 * SLOTS
R_A = R_M + 2 * SLOTS
R_END = R_A + 2 * (NTP - 1)
N_SEND = 140


def dot(a, b, dims=NN):
    return lax.dot_general(a, b, dims, preferred_element_type=F32)


def token_of(row):
    return (row // 128) + ((row // 8) % 4) * 4 + (row % 8) * 16 + ((row // 32) % 4) * 128


def kernel(
    hid, gain_h, freq_h, wq, wk, wv, wo, post_h,
    out_h, lw_h,
    gain, freq, post, out, lw_out, hid_v, np_v, wq_v, w_v, wo_v, kv, passing, q_s, st_o, st_m, st_l, att_p, att_n, att_all, lw_s,
    cos_s, sin_s, bias_c, bias_n, perm, sum_s, lsem, ssem, rsem,
):
    sp = lax.axis_index("sp")
    tp = lax.axis_index("tp")
    z, y = sp // NY, sp % NY
    x, core = tp // 2, tp % 2
    sends = []

    def start(src, dst, ridx, dev):
        copy = pltpu.make_async_remote_copy(
            src_ref=src, dst_ref=dst, send_sem=ssem.at[len(sends)], recv_sem=rsem.at[ridx],
            device_id=dev, device_id_type=MESH,
        )
        copy.start()
        sends.append(copy)

    def arrived(dst, ridx):
        pltpu.make_async_remote_copy(
            src_ref=dst, dst_ref=dst, send_sem=ssem.at[0], recv_sem=rsem.at[ridx],
            device_id=((sp + 1) % NSP, tp), device_id_type=MESH,
        ).wait_recv()

    y_peer = [(z * NY + (y + d) % NY, tp) for d in range(NY)]
    z_peer = [(((z + d) % NZ) * NY + y, tp) for d in range(NZ)]
    ahead = ((sp + 1) % NSP, tp)
    behind = ((sp + NSP - 1) % NSP, tp)
    relay_of_me = y_peer[NY - 3]
    relay_to = ((z * NY + (y + 3) % NY + 4) % NSP, tp)
    source = (sp + NSP - 4) % NSP
    relay_from = ((source // NY) * NY + (source % NY + NY - 3) % NY, tp)
    t_peer = [(sp, (tp + d) % NTP) for d in range(NTP)]
    x_right = (sp, (tp + 2) % NTP)
    x_left = (sp, (tp + NTP - 2) % NTP)
    sibling = (sp, x * 2 + (1 - core))

    local = [
        pltpu.make_async_copy(w.at[:, p * 128 : (p + 1) * 128], w_v.at[i, p, z, y], lsem.at[2 * p + i])
        for p in range(2)
        for i, w in enumerate((wk, wv))
    ] + [
        pltpu.make_async_copy(wo, wo_v.at[tp], lsem.at[4]),
        pltpu.make_async_copy(hid, hid_v, lsem.at[5]),
        pltpu.make_async_copy(wq, wq_v, lsem.at[6]),
        pltpu.make_async_copy(gain_h, gain, lsem.at[7]),
        pltpu.make_async_copy(freq_h, freq, lsem.at[8]),
        pltpu.make_async_copy(post_h, post, lsem.at[9]),
    ]
    for copy in local:
        copy.start()

    lw_copy = pltpu.make_async_copy(lw_out, lw_h, lsem.at[10])

    barrier = pltpu.get_barrier_semaphore()
    partners = y_peer[1:] + z_peer[1:] + t_peer[1:] + [ahead, behind, relay_to, relay_from]
    for dev in partners:
        pl.semaphore_signal(barrier, inc=1, device_id=dev, device_id_type=MESH)
    pl.semaphore_wait(barrier, len(partners))

    def weights_send(p):
        for i, peer in enumerate((y_peer, z_peer)):
            local[2 * p + i].wait()
            part = w_v.at[i, p, z, y]
            for d in range(1, 8):
                start(part, part, R_WD + (i * 2 + p) * 7 + d - 1, peer[d])

    def weights_wait(p):
        for d in range(1, 8):
            arrived(w_v.at[0, p, z, (y + NY - d) % NY], R_WD + p * 7 + d - 1)
            arrived(w_v.at[1, p, (z + NZ - d) % NZ, y], R_WD + (2 + p) * 7 + d - 1)

    def relay_part(i, p, at, half):
        piece = pl.ds(half * 4, 4)
        return w_v.at[0, p, at, piece] if i == 0 else w_v.at[1, p, piece, at]

    def relay_sem(i, p, half, direction, hop):
        return R_WR + (((i * 2 + p) * 2 + half) * 2 + direction) * 4 + hop

    def relay_dev(i, direction):
        peer = z_peer if i == 0 else y_peer
        return peer[1] if direction == 0 else peer[7]

    def relay_send(p):
        for half in range(2):
            for i, at in enumerate((z, y)):
                part = relay_part(i, p, at, half)
                for direction in range(2):
                    start(part, part, relay_sem(i, p, half, direction, 0), relay_dev(i, direction))

    def relay_step(p, hop):
        for half in range(2):
            for i, at in enumerate((z, y)):
                for direction in range(2):
                    hops = 4 if half == direction else 3
                    if hop < hops:
                        owner = (at + 7 - hop) % 8 if direction == 0 else (at + 1 + hop) % 8
                        part = relay_part(i, p, owner, half)
                        arrived(part, relay_sem(i, p, half, direction, hop))
                        if hop + 1 < hops:
                            start(part, part, relay_sem(i, p, half, direction, hop + 1), relay_dev(i, direction))

    def wo_part(delta, part):
        group = wo_v.at[(tp + delta) % NTP]
        return group if part is None else group.at[pl.ds(part * 128, 128)]

    def wo_send():
        local[4].wait()
        start(wo_part(0, 0), wo_part(0, 0), R_X + 0, x_right)
        start(wo_part(0, 1), wo_part(0, 1), R_X + 1, x_left)
        start(wo_part(0, 1), wo_part(0, 1), R_X + 2, x_right)
        start(wo_part(0, 0), wo_part(0, 0), R_X + 3, x_left)
        start(wo_part(0, None), wo_part(0, None), R_X + 6, sibling)

    def wo_step(k):
        if k == 0:
            arrived(wo_part(6, 0), R_X + 0)
            start(wo_part(6, 0), wo_part(6, 0), R_X + 4, x_right)
            start(wo_part(6, 0), wo_part(6, 0), R_X + 7, sibling)
            arrived(wo_part(2, 1), R_X + 1)
            start(wo_part(2, 1), wo_part(2, 1), R_X + 5, x_left)
            start(wo_part(2, 1), wo_part(2, 1), R_X + 8, sibling)
        elif k == 1:
            arrived(wo_part(6, 1), R_X + 2)
            start(wo_part(6, 1), wo_part(6, 1), R_X + 9, sibling)
            arrived(wo_part(2, 0), R_X + 3)
            start(wo_part(2, 0), wo_part(2, 0), R_X + 10, sibling)
        else:
            arrived(wo_part(4, 0), R_X + 4)
            start(wo_part(4, 0), wo_part(4, 0), R_X + 11, sibling)
            arrived(wo_part(4, 1), R_X + 5)
            start(wo_part(4, 1), wo_part(4, 1), R_X + 12, sibling)

    def wo_sibling_wait():
        other = x * 2 + (1 - core)

        def part_of(delta, part):
            group = wo_v.at[(other + delta) % NTP]
            return group if part is None else group.at[pl.ds(part * 128, 128)]

        arrived(part_of(0, None), R_X + 6)
        arrived(part_of(6, 0), R_X + 7)
        arrived(part_of(2, 1), R_X + 8)
        arrived(part_of(6, 1), R_X + 9)
        arrived(part_of(2, 0), R_X + 10)
        arrived(part_of(4, 0), R_X + 11)
        arrived(part_of(4, 1), R_X + 12)

    def up_part(k, p):
        return kv.at[k, p, :, 0:AHEAD_ROWS]

    def down_part(k, p):
        return kv.at[k, p, :, AHEAD_ROWS:ROWS]

    def halo_send(p):
        start(up_part(0, p), up_part(1, p), R_H + p * SLOTS + 1, ahead)
        start(down_part(0, p), passing.at[p], R_M + p * SLOTS, relay_of_me)

    def up(p, k):
        arrived(up_part(k, p), R_H + p * SLOTS + k)
        if k < SLOTS - 1:
            start(up_part(k, p), up_part(k + 1, p), R_H + p * SLOTS + k + 1, ahead)

    def down(p, k):
        if k == 0:
            arrived(passing.at[p], R_M + p * SLOTS)
            start(passing.at[p], down_part(4, p), R_M + p * SLOTS + 4, relay_to)
        else:
            arrived(down_part(k, p), R_M + p * SLOTS + k)
            if k > 1:
                start(down_part(k, p), down_part(k - 1, p), R_M + p * SLOTS + k - 1, behind)

    lane = lax.broadcasted_iota(jnp.int32, (1, 128), 1)
    first_head = lane < 64
    first_half = (lane % 64) < 32

    def norm():
        local[5].wait()
        local[7].wait()

        def step(i, _):
            rows = pl.ds(pl.multiple_of(i * 32, 32), 32)
            h = hid_v[rows, :].astype(F32)
            scale = lax.rsqrt(jnp.mean(h * h, axis=-1, keepdims=True) + EPS)
            hid_v[rows, :] = (h * scale * gain[...]).astype(BF16)
            return 0

        lax.fori_loop(0, ROWS // 32, step, 0)

    def permutation():
        token = token_of(lax.broadcasted_iota(jnp.int32, (ROWS, ROWS), 0))
        col = lax.broadcasted_iota(jnp.int32, (ROWS, ROWS), 1)
        perm[0] = (token == col).astype(F32).astype(BF16)
        row = lax.broadcasted_iota(jnp.int32, (ROWS, ROWS), 0)
        token_c = token_of(lax.broadcasted_iota(jnp.int32, (ROWS, ROWS), 1))
        perm[1] = (token_c == row).astype(F32).astype(BF16)

    def permute():
        def step(i, _):
            rows = pl.ds(pl.multiple_of(i * 128, 128), 128)
            for c in range(4):
                np_v[rows, c * 512 : (c + 1) * 512] = dot(perm[0, rows, :], hid_v[:, c * 512 : (c + 1) * 512]).astype(BF16)
            return 0

        lax.fori_loop(0, 4, step, 0, unroll=2)

    def tables():
        local[8].wait()
        token = token_of(lax.broadcasted_iota(jnp.int32, (ROWS, 128), 0))
        angle = (sp * ROWS + token).astype(F32) * freq[...]
        cos_s[...] = jnp.cos(angle)
        sine = jnp.sin(angle)
        sin_s[...] = jnp.where(first_half, -sine, sine)

    def biases():
        row = lax.broadcasted_iota(jnp.int32, (128, 128), 0)
        col = lax.broadcasted_iota(jnp.int32, (128, 128), 1)

        def class_token(r):
            return (r // 32) * 128 + (r % 8) * 16 + ((r // 8) % 4) * 4

        for k in range(SLOTS):
            delta = class_token(row) - class_token(col) + ROWS * k
            near = (delta >= 0) & (delta <= 4 * SPAN)
            far = (delta >= 0) & (delta <= 16 * SPAN) & ((row // 8) % 4 == (col // 8) % 4)
            bias = jnp.where(near & far, 1.0, jnp.where(near | far, 0.0, NEG))
            bias_c[:, k * 128 : (k + 1) * 128] = jnp.where(sp >= k, bias, NEG)

        def near_token(r):
            return (r // 32) + (r % 8) * 16 + ((r // 8) % 4) * 4

        delta = near_token(row) - near_token(col)
        own = jnp.where((delta >= 0) & (delta <= SPAN), 0.0, NEG)
        delta = delta + 128
        prev = jnp.where((delta >= 0) & (delta <= SPAN), 0.0, NEG)
        bias_n[0, :, 0:128] = jnp.where(sp >= 1, prev, NEG)
        bias_n[1, :, 0:128] = prev
        bias_n[0, :, 128:256] = own
        bias_n[1, :, 128:256] = own

    def rotate(u, rows):
        swapped = jnp.where(first_half, pltpu.roll(u, 96, 1), pltpu.roll(u, 32, 1))
        return (u * cos_s[rows, :] + swapped * sin_s[rows, :]).astype(BF16)

    def queries():
        local[6].wait()

        for r0 in range(0, ROWS, BIG):
            q = dot(np_v[r0 : r0 + BIG, :], wq_v[...])
            for r in range(BIG // 128):
                rows = slice(r0 + r * 128, r0 + r * 128 + 128)
                for p in range(2):
                    turned = rotate(q[r * 128 : r * 128 + 128, p * 128 : (p + 1) * 128], rows)
                    zero = jnp.zeros_like(turned)
                    q_s[p, r0 // 128 + r, 0:128, :] = jnp.where(first_head, turned, zero)
                    q_s[p, r0 // 128 + r, 128:256, :] = jnp.where(first_head, zero, turned)

    def keys_values(p):
        weights = jnp.concatenate([w_v[i, p].reshape(D, 128) for i in range(2)], axis=1)

        for r0 in range(0, ROWS, BIG):
            rows = slice(r0, r0 + BIG)
            both = dot(np_v[rows, :], weights)
            kv[0, p, 0, rows, :] = rotate(both[:, 0:128], rows)
            kv[0, p, 1, rows, :] = both[:, 128:256].astype(BF16)

    def near(p, first, last):
        def step(b, _):
            slot = (3 - b) // 3
            before = (b + 3) % 4
            state = [(r, pl.ds(pl.multiple_of(h * 128 + b * 32, 32), 32)) for h in range(2) for r in range(4)]

            def gathered(ref):
                return jnp.concatenate([ref[p, r, at, :] for r, at in state], axis=0)

            def scattered(ref, value):
                for i, (r, at) in enumerate(state):
                    ref[p, r, at, :] = value[i * 32 : (i + 1) * 32]

            def part(r, base):
                return pl.ds(pl.multiple_of(base + r * 128, 32), 32)

            k, v = (
                jnp.concatenate(
                    [kv[slot, p, w, part(r, before * 32), :] for r in range(4)]
                    + [kv[0, p, w, part(r, b * 32), :] for r in range(4)],
                    axis=0,
                )
                for w in range(2)
            )
            o, m, total = update(
                gathered(q_s), k, v, bias_n[jnp.minimum(b, 1)], (gathered(st_o), gathered(st_m), gathered(st_l))
            )
            scattered(st_o, o)
            scattered(st_m, m)
            scattered(st_l, total)
            return 0

        lax.fori_loop(first, last, step, 0, unroll=True)

    def update(q, k, v, bias, state):
        s = dot(q, k, NT) * SCALE2 + jnp.concatenate([bias, bias], axis=0)
        m = jnp.broadcast_to(jnp.max(s, axis=-1, keepdims=True), q.shape)
        if state is not None:
            m = jnp.maximum(m, state[1])
        e = jnp.exp2(s - jnp.concatenate([m] * (s.shape[1] // 128), axis=1))
        total = jnp.broadcast_to(jnp.sum(e, axis=-1, keepdims=True), q.shape)
        o = dot(e.astype(BF16), v)
        if state is not None:
            decay = jnp.exp2(state[1] - m)
            total = state[2] * decay + total
            o = state[0] * decay + o
        return o, m, total

    def far(p, first, last, slots):
        def step(r, _):
            rows = pl.ds(pl.multiple_of(r * 128, 128), 128)
            k, v = (jnp.concatenate([kv[s, p, w, rows, :] for s in slots], axis=0) for w in range(2))
            bias = bias_c[:, slots[0] * 128 : (slots[-1] + 1) * 128]
            state = None if slots[0] == 0 else (st_o[p, r], st_m[p, r], st_l[p, r])
            st_o[p, r], st_m[p, r], st_l[p, r] = update(q_s[p, r], k, v, bias, state)
            return 0

        lax.fori_loop(first, last, step, 0, unroll=True)

    def finish(p):
        for r in range(4):
            rows = slice(r * 128, (r + 1) * 128)
            o = st_o[p, r] / st_l[p, r]
            att_p[rows, :] = jnp.where(first_head, o[0:128], o[128:256]).astype(BF16)
            level = st_m[p, r] * LN2 + jnp.log(st_l[p, r])
            both = jnp.where(lane == 2 * p, level[0:128], level[128:256])
            if p == 0:
                lw_s[rows, :] = both
            else:
                lw_s[rows, :] = jnp.where(lane < 2, lw_s[rows, :], both)
        att_n[p] = dot(perm[1], att_p[...]).astype(BF16)
        att_all[p, tp] = att_n[p, pl.ds(pl.multiple_of(tp * OUT_ROWS, OUT_ROWS), OUT_ROWS), :]
        for d in range(1, NTP):
            rows = pl.ds(pl.multiple_of(((tp + d) % NTP) * OUT_ROWS, OUT_ROWS), OUT_ROWS)
            start(att_n.at[p, rows], att_all.at[p, tp], R_A + p * (NTP - 1) + d - 1, t_peer[d])

    def attended_wait(p):
        for d in range(1, NTP):
            arrived(att_all.at[p, (tp + NTP - d) % NTP], R_A + p * (NTP - 1) + d - 1)

    def log_weights():
        levels = jnp.transpose(lw_s[...])[0:8, :]
        high = levels.astype(BF16)
        rest = levels - high.astype(F32)
        mid = rest.astype(BF16)
        low = (rest - mid.astype(F32)).astype(BF16)
        natural = dot(high, perm[0]) + dot(mid, perm[0]) + dot(low, perm[0])
        lw_out[...] = natural[0:4, :]
        lw_copy.start()

    def project():
        def step(c, squares):
            cols = pl.ds(pl.multiple_of(c * 512, 512), 512)
            total = None
            for g in range(NTP):
                a = jnp.concatenate([att_all[0, g], att_all[1, g]], axis=1)
                part = dot(a, wo_v[g, :, cols]).astype(BF16).astype(F32)
                total = part if total is None else total + part
            sum_s[:, cols] = total
            return squares + jnp.sum(total * total, axis=-1, keepdims=True)

        squares = lax.fori_loop(0, 4, step, jnp.zeros((OUT_ROWS, 1), F32))
        scale = lax.rsqrt(squares / D + EPS)
        local[9].wait()
        out[...] = (sum_s[...] * scale * post[...]).astype(BF16)
        out_copy = pltpu.make_async_copy(out, out_h, lsem.at[11])
        out_copy.start()
        lw_copy.wait()
        out_copy.wait()

    weights_send(0)
    weights_send(1)
    wo_send()
    norm()
    permutation()
    permute()
    weights_wait(0)
    relay_send(0)
    weights_wait(1)
    relay_send(1)
    tables()
    relay_step(0, 0)
    relay_step(1, 0)
    biases()
    relay_step(0, 1)
    relay_step(1, 1)
    relay_step(0, 2)
    relay_step(1, 2)
    wo_step(0)
    relay_step(0, 3)
    keys_values(0)
    halo_send(0)
    relay_step(1, 3)
    keys_values(1)
    halo_send(1)
    queries()
    far(0, 0, 4, (0,))
    near(0, 1, 4)
    up(0, 1)
    far(1, 0, 4, (0,))
    down(0, 0)
    up(1, 1)
    near(1, 1, 4)
    wo_step(1)
    down(1, 0)
    up(0, 2)
    far(0, 0, 2, (1, 2))
    down(0, 4)
    up(1, 2)
    far(1, 0, 2, (1, 2))
    down(1, 4)
    down(0, 3)
    up(0, 3)
    wo_step(2)
    down(1, 3)
    far(0, 3, 4, (3, 4))
    up(1, 3)
    far(1, 3, 4, (3, 4))
    down(0, 2)
    up(0, 4)
    far(0, 0, 2, (3, 4))
    down(1, 2)
    far(0, 2, 3, (3, 4))
    down(0, 1)
    far(0, 2, 4, (1, 2))
    near(0, 0, 1)
    finish(0)
    up(1, 4)
    far(1, 0, 3, (3, 4))
    down(1, 1)
    far(1, 2, 4, (1, 2))
    near(1, 0, 1)
    finish(1)
    wo_sibling_wait()
    attended_wait(0)
    log_weights()
    attended_wait(1)
    project()
    for copy in sends:
        copy.wait_send()


def hand_over(out_in, lw_in, out, lw_out):
    out[...] = out_in[...]
    lw_out[...] = lw_in[...]


def body(hidden_in, pre_gain, query_proj, key_proj, value_proj, out_proj, post_gain):
    half = np.arange(HEAD_DIM // 2, dtype=np.float32) * np.float32(2.0) / np.float32(HEAD_DIM)
    freq = np.tile(np.power(np.float64(ROPE_BASE), -half.astype(np.float64)).astype(np.float32), 4).reshape(1, 128)
    any_spec = pl.BlockSpec(memory_space=pl.ANY)
    vmem = pl.BlockSpec(memory_space=pltpu.VMEM)
    results = pl.pallas_call(
        kernel,
        out_shape=(jax.ShapeDtypeStruct((OUT_ROWS, D), BF16), jax.ShapeDtypeStruct((4, ROWS), F32)),
        in_specs=[any_spec] * 8,
        out_specs=(any_spec, any_spec),
        scratch_shapes=[
            pltpu.VMEM((1, D), F32),
            pltpu.VMEM((1, 128), F32),
            pltpu.VMEM((1, D), F32),
            pltpu.VMEM((OUT_ROWS, D), BF16),
            pltpu.VMEM((4, ROWS), F32),
            pltpu.VMEM((ROWS, D), BF16),
            pltpu.VMEM((ROWS, D), BF16),
            pltpu.VMEM((D, WIDTH), BF16),
            pltpu.VMEM((2, 2, NZ, NY, D // NSP, 128), BF16),
            pltpu.VMEM((NTP, WIDTH, D), BF16),
            pltpu.VMEM((SLOTS, 2, 2, ROWS, 128), BF16),
            pltpu.VMEM((2, 2, ROWS - AHEAD_ROWS, 128), BF16),
            pltpu.VMEM((2, 4, 256, 128), BF16),
            pltpu.VMEM((2, 4, 256, 128), F32),
            pltpu.VMEM((2, 4, 256, 128), F32),
            pltpu.VMEM((2, 4, 256, 128), F32),
            pltpu.VMEM((ROWS, 128), BF16),
            pltpu.VMEM((2, ROWS, 128), BF16),
            pltpu.VMEM((2, NTP, OUT_ROWS, 128), BF16),
            pltpu.VMEM((ROWS, 128), F32),
            pltpu.VMEM((ROWS, 128), F32),
            pltpu.VMEM((ROWS, 128), F32),
            pltpu.VMEM((128, SLOTS * 128), F32),
            pltpu.VMEM((2, 128, 256), F32),
            pltpu.VMEM((2, ROWS, ROWS), BF16),
            pltpu.VMEM((OUT_ROWS, D), F32),
            pltpu.SemaphoreType.DMA((12,)),
            pltpu.SemaphoreType.DMA((N_SEND,)),
            pltpu.SemaphoreType.DMA((R_END,)),
        ],
        compiler_params=pltpu.CompilerParams(
            collective_id=0, has_side_effects=True, vmem_limit_bytes=60 * 1024 * 1024
        ),
        name="layer",
    )(
        hidden_in, pre_gain.reshape(1, D), jnp.asarray(freq), query_proj, key_proj, value_proj, out_proj,
        post_gain.reshape(1, D),
    )
    return pl.pallas_call(
        hand_over,
        out_shape=(jax.ShapeDtypeStruct((OUT_ROWS, D), BF16), jax.ShapeDtypeStruct((4, ROWS), F32)),
        in_specs=[vmem, vmem],
        out_specs=(vmem, vmem),
        name="hand_over",
    )(*results)


def solution(mesh):
    placed = (P("sp", None), P(), P(None, "tp"), P("sp", "tp"), P("sp", "tp"), P("tp", None), P())
    return jax.shard_map(
        body,
        mesh=mesh,
        in_specs=placed,
        out_specs=(P(("sp", "tp"), None), P("tp", "sp")),
        check_vma=False,
    )
```

```python
import functools
import math

import jax
import jax.numpy as jnp
import numpy as np
from jax import lax
from jax.experimental import pallas as pl
from jax.experimental.pallas import tpu as pltpu
from jax.sharding import PartitionSpec as P

HEAD_DIM = 64
SPAN = 128
EPS = 1e-06
ROPE_BASE = 10000.0
NY = 8
NZ = 8
NSP = NY * NZ
NTP = 8
NX = 4
ROWS = 512
D = 2048
WIDTH = 256
OUT_ROWS = 64
SLOTS = 5
NEG = -1e30
SCALE2 = math.log2(math.e) / 8.0
LN2 = math.log(2.0)
BIG = 512
F32 = jnp.float32
BF16 = jnp.bfloat16
MESH = pl.DeviceIdType.MESH

NT = (((1,), (1,)), ((), ()))
NN = (((1,), (0,)), ((), ()))

AHEAD_ROWS = 320

R_WD = 0
R_WR = R_WD + 2 * 2 * 7
R_X = R_WR + 2 * 2 * 2 * 2 * 4
R_H = R_X + 16
R_M = R_H + 4 * SLOTS
R_A = R_M + 4 * SLOTS
R_END = R_A + 2 * (NTP - 1)
N_SEND = 160


def dot(a, b, dims=NN):
    return lax.dot_general(a, b, dims, preferred_element_type=F32)


def token_of(row):
    return (row // 128) + ((row // 8) % 4) * 4 + (row % 8) * 16 + ((row // 32) % 4) * 128


def kernel(
    hid, gain_h, freq_h, wq, wk, wv, wo, post_h,
    out_h, lw_h,
    gain, freq, post, out, lw_out, hid_v, np_v, wq_v, w_v, wo_v, kv, passing, q_s, st_o, st_m, st_l, att_p, att_n, att_all, lw_s,
    cos_s, sin_s, bias_c, bias_n, perm, sum_s, lsem, ssem, rsem,
):
    sp = lax.axis_index("sp")
    tp = lax.axis_index("tp")
    z, y = sp // NY, sp % NY
    x, core = tp // 2, tp % 2
    sends = []

    def start(src, dst, ridx, dev):
        copy = pltpu.make_async_remote_copy(
            src_ref=src, dst_ref=dst, send_sem=ssem.at[len(sends)], recv_sem=rsem.at[ridx],
            device_id=dev, device_id_type=MESH,
        )
        copy.start()
        sends.append(copy)

    def arrived(dst, ridx):
        pltpu.make_async_remote_copy(
            src_ref=dst, dst_ref=dst, send_sem=ssem.at[0], recv_sem=rsem.at[ridx],
            device_id=((sp + 1) % NSP, tp), device_id_type=MESH,
        ).wait_recv()

    y_peer = [(z * NY + (y + d) % NY, tp) for d in range(NY)]
    z_peer = [(((z + d) % NZ) * NY + y, tp) for d in range(NZ)]
    ahead = ((sp + 1) % NSP, tp)
    behind = ((sp + NSP - 1) % NSP, tp)
    relay_of_me = (((z + y // 4) % NZ) * NY + (y + NY - 3) % NY, tp)
    source_y = (y + 3) % NY
    relay_source = (((z + NZ - source_y // 4) % NZ) * NY + source_y, tp)
    t_peer = [(sp, (tp + d) % NTP) for d in range(NTP)]
    x_right = (sp, (tp + 2) % NTP)
    x_left = (sp, (tp + NTP - 2) % NTP)
    sibling = (sp, x * 2 + (1 - core))

    local = [
        pltpu.make_async_copy(w.at[:, p * 128 : (p + 1) * 128], w_v.at[i, p, z, y], lsem.at[2 * p + i])
        for p in range(2)
        for i, w in enumerate((wk, wv))
    ] + [
        pltpu.make_async_copy(wo, wo_v.at[tp], lsem.at[4]),
        pltpu.make_async_copy(hid, hid_v, lsem.at[5]),
        pltpu.make_async_copy(wq, wq_v, lsem.at[6]),
        pltpu.make_async_copy(gain_h, gain, lsem.at[7]),
        pltpu.make_async_copy(freq_h, freq, lsem.at[8]),
        pltpu.make_async_copy(post_h, post, lsem.at[9]),
    ]
    for copy in local:
        copy.start()

    lw_copy = pltpu.make_async_copy(lw_out, lw_h, lsem.at[10])

    barrier = pltpu.get_barrier_semaphore()
    partners = y_peer[1:] + z_peer[1:] + t_peer[1:] + [ahead, behind, relay_of_me, relay_source]
    for dev in partners:
        pl.semaphore_signal(barrier, inc=1, device_id=dev, device_id_type=MESH)
    pl.semaphore_wait(barrier, len(partners))

    def weights_send(p):
        for i, peer in enumerate((y_peer, z_peer)):
            local[2 * p + i].wait()
            part = w_v.at[i, p, z, y]
            for d in range(1, 8):
                start(part, part, R_WD + (i * 2 + p) * 7 + d - 1, peer[d])

    def weights_wait(p):
        for d in range(1, 8):
            arrived(w_v.at[0, p, z, (y + NY - d) % NY], R_WD + p * 7 + d - 1)
            arrived(w_v.at[1, p, (z + NZ - d) % NZ, y], R_WD + (2 + p) * 7 + d - 1)

    def relay_part(i, p, at, half):
        piece = pl.ds(half * 4, 4)
        return w_v.at[0, p, at, piece] if i == 0 else w_v.at[1, p, piece, at]

    def relay_sem(i, p, half, direction, hop):
        return R_WR + (((i * 2 + p) * 2 + half) * 2 + direction) * 4 + hop

    def relay_dev(i, direction):
        peer = z_peer if i == 0 else y_peer
        return peer[1] if direction == 0 else peer[7]

    def relay_send(p):
        for half in range(2):
            for i, at in enumerate((z, y)):
                part = relay_part(i, p, at, half)
                for direction in range(2):
                    start(part, part, relay_sem(i, p, half, direction, 0), relay_dev(i, direction))

    def relay_step(p, hop):
        for half in range(2):
            for i, at in enumerate((z, y)):
                for direction in range(2):
                    hops = 4 if half == direction else 3
                    if hop < hops:
                        owner = (at + 7 - hop) % 8 if direction == 0 else (at + 1 + hop) % 8
                        part = relay_part(i, p, owner, half)
                        arrived(part, relay_sem(i, p, half, direction, hop))
                        if hop + 1 < hops:
                            start(part, part, relay_sem(i, p, half, direction, hop + 1), relay_dev(i, direction))

    def wo_part(delta, part):
        group = wo_v.at[(tp + delta) % NTP]
        return group if part is None else group.at[pl.ds(part * 128, 128)]

    def wo_send():
        local[4].wait()
        start(wo_part(0, 0), wo_part(0, 0), R_X + 0, x_right)
        start(wo_part(0, 1), wo_part(0, 1), R_X + 1, x_left)
        start(wo_part(0, 1), wo_part(0, 1), R_X + 2, x_right)
        start(wo_part(0, 0), wo_part(0, 0), R_X + 3, x_left)
        start(wo_part(0, None), wo_part(0, None), R_X + 6, sibling)

    def wo_step(k):
        if k == 0:
            arrived(wo_part(6, 0), R_X + 0)
            start(wo_part(6, 0), wo_part(6, 0), R_X + 4, x_right)
            start(wo_part(6, 0), wo_part(6, 0), R_X + 7, sibling)
            arrived(wo_part(2, 1), R_X + 1)
            start(wo_part(2, 1), wo_part(2, 1), R_X + 5, x_left)
            start(wo_part(2, 1), wo_part(2, 1), R_X + 8, sibling)
        elif k == 1:
            arrived(wo_part(6, 1), R_X + 2)
            start(wo_part(6, 1), wo_part(6, 1), R_X + 9, sibling)
            arrived(wo_part(2, 0), R_X + 3)
            start(wo_part(2, 0), wo_part(2, 0), R_X + 10, sibling)
        else:
            arrived(wo_part(4, 0), R_X + 4)
            start(wo_part(4, 0), wo_part(4, 0), R_X + 11, sibling)
            arrived(wo_part(4, 1), R_X + 5)
            start(wo_part(4, 1), wo_part(4, 1), R_X + 12, sibling)

    def wo_sibling_wait():
        other = x * 2 + (1 - core)

        def part_of(delta, part):
            group = wo_v.at[(other + delta) % NTP]
            return group if part is None else group.at[pl.ds(part * 128, 128)]

        arrived(part_of(0, None), R_X + 6)
        arrived(part_of(6, 0), R_X + 7)
        arrived(part_of(2, 1), R_X + 8)
        arrived(part_of(6, 1), R_X + 9)
        arrived(part_of(2, 0), R_X + 10)
        arrived(part_of(4, 0), R_X + 11)
        arrived(part_of(4, 1), R_X + 12)

    def up_part(k, p, w):
        return kv.at[k, p, w, 0:AHEAD_ROWS]

    def down_part(k, p, w):
        return kv.at[k, p, w, AHEAD_ROWS:ROWS]

    def halo_sem(base, p, k, w):
        return base + (p * SLOTS + k) * 2 + w

    def halo_send(p):
        for w in range(2):
            start(up_part(0, p, w), up_part(1, p, w), halo_sem(R_H, p, 1, w), ahead)
            start(down_part(0, p, w), passing.at[p, w], halo_sem(R_M, p, 0, w), relay_of_me)

    def up(p, k):
        for w in range(2):
            arrived(up_part(k, p, w), halo_sem(R_H, p, k, w))
            if k < SLOTS - 1:
                start(up_part(k, p, w), up_part(k + 1, p, w), halo_sem(R_H, p, k + 1, w), ahead)

    def down(p, k):
        for w in range(2):
            if k == 0:
                arrived(passing.at[p, w], halo_sem(R_M, p, 0, w))
                start(passing.at[p, w], down_part(4, p, w), halo_sem(R_M, p, 4, w), y_peer[NY - 1])
            else:
                arrived(down_part(k, p, w), halo_sem(R_M, p, k, w))
                if k > 1:
                    start(down_part(k, p, w), down_part(k - 1, p, w), halo_sem(R_M, p, k - 1, w), behind)

    lane = lax.broadcasted_iota(jnp.int32, (1, 128), 1)
    first_head = lane < 64
    first_half = (lane % 64) < 32

    def norm():
        local[5].wait()
        local[7].wait()

        def step(i, _):
            rows = pl.ds(pl.multiple_of(i * 32, 32), 32)
            h = hid_v[rows, :].astype(F32)
            scale = lax.rsqrt(jnp.mean(h * h, axis=-1, keepdims=True) + EPS)
            hid_v[rows, :] = (h * scale * gain[...]).astype(BF16)
            return 0

        lax.fori_loop(0, ROWS // 32, step, 0)

    def permutation():
        token = token_of(lax.broadcasted_iota(jnp.int32, (ROWS, ROWS), 0))
        col = lax.broadcasted_iota(jnp.int32, (ROWS, ROWS), 1)
        perm[0] = (token == col).astype(F32).astype(BF16)
        row = lax.broadcasted_iota(jnp.int32, (ROWS, ROWS), 0)
        token_c = token_of(lax.broadcasted_iota(jnp.int32, (ROWS, ROWS), 1))
        perm[1] = (token_c == row).astype(F32).astype(BF16)

    def permute():
        def step(i, _):
            rows = pl.ds(pl.multiple_of(i * 128, 128), 128)
            for c in range(4):
                np_v[rows, c * 512 : (c + 1) * 512] = dot(perm[0, rows, :], hid_v[:, c * 512 : (c + 1) * 512]).astype(BF16)
            return 0

        lax.fori_loop(0, 4, step, 0, unroll=2)

    def tables():
        local[8].wait()
        token = token_of(lax.broadcasted_iota(jnp.int32, (ROWS, 128), 0))
        angle = (sp * ROWS + token).astype(F32) * freq[...]
        cos_s[...] = jnp.cos(angle)
        sine = jnp.sin(angle)
        sin_s[...] = jnp.where(first_half, -sine, sine)

    def biases():
        row = lax.broadcasted_iota(jnp.int32, (128, 128), 0)
        col = lax.broadcasted_iota(jnp.int32, (128, 128), 1)

        def class_token(r):
            return (r // 32) * 128 + (r % 8) * 16 + ((r // 8) % 4) * 4

        for k in range(SLOTS):
            delta = class_token(row) - class_token(col) + ROWS * k
            near = (delta >= 0) & (delta <= 4 * SPAN)
            far = (delta >= 0) & (delta <= 16 * SPAN) & ((row // 8) % 4 == (col // 8) % 4)
            bias = jnp.where(near & far, 1.0, jnp.where(near | far, 0.0, NEG))
            bias_c[:, k * 128 : (k + 1) * 128] = jnp.where(sp >= k, bias, NEG)

        def near_token(r):
            return (r // 32) + (r % 8) * 16 + ((r // 8) % 4) * 4

        delta = near_token(row) - near_token(col)
        own = jnp.where((delta >= 0) & (delta <= SPAN), 0.0, NEG)
        delta = delta + 128
        prev = jnp.where((delta >= 0) & (delta <= SPAN), 0.0, NEG)
        bias_n[0, :, 0:128] = jnp.where(sp >= 1, prev, NEG)
        bias_n[1, :, 0:128] = prev
        bias_n[0, :, 128:256] = own
        bias_n[1, :, 128:256] = own

    def rotate(u, rows):
        swapped = jnp.where(first_half, pltpu.roll(u, 96, 1), pltpu.roll(u, 32, 1))
        return (u * cos_s[rows, :] + swapped * sin_s[rows, :]).astype(BF16)

    def queries():
        local[6].wait()

        for r0 in range(0, ROWS, BIG):
            q = dot(np_v[r0 : r0 + BIG, :], wq_v[...])
            for r in range(BIG // 128):
                rows = slice(r0 + r * 128, r0 + r * 128 + 128)
                for p in range(2):
                    turned = rotate(q[r * 128 : r * 128 + 128, p * 128 : (p + 1) * 128], rows)
                    zero = jnp.zeros_like(turned)
                    q_s[p, r0 // 128 + r, 0:128, :] = jnp.where(first_head, turned, zero)
                    q_s[p, r0 // 128 + r, 128:256, :] = jnp.where(first_head, zero, turned)

    def keys_values(p):
        weights = jnp.concatenate([w_v[i, p].reshape(D, 128) for i in range(2)], axis=1)

        for r0 in range(0, ROWS, BIG):
            rows = slice(r0, r0 + BIG)
            both = dot(np_v[rows, :], weights)
            kv[0, p, 0, rows, :] = rotate(both[:, 0:128], rows)
            kv[0, p, 1, rows, :] = both[:, 128:256].astype(BF16)

    def near(p, first, last):
        def step(b, _):
            slot = (3 - b) // 3
            before = (b + 3) % 4
            state = [(r, pl.ds(pl.multiple_of(h * 128 + b * 32, 32), 32)) for h in range(2) for r in range(4)]

            def gathered(ref):
                return jnp.concatenate([ref[p, r, at, :] for r, at in state], axis=0)

            def scattered(ref, value):
                for i, (r, at) in enumerate(state):
                    ref[p, r, at, :] = value[i * 32 : (i + 1) * 32]

            def part(r, base):
                return pl.ds(pl.multiple_of(base + r * 128, 32), 32)

            k, v = (
                jnp.concatenate(
                    [kv[slot, p, w, part(r, before * 32), :] for r in range(4)]
                    + [kv[0, p, w, part(r, b * 32), :] for r in range(4)],
                    axis=0,
                )
                for w in range(2)
            )
            o, m, total = update(
                gathered(q_s), k, v, bias_n[jnp.minimum(b, 1)], (gathered(st_o), gathered(st_m), gathered(st_l))
            )
            scattered(st_o, o)
            scattered(st_m, m)
            scattered(st_l, total)
            return 0

        lax.fori_loop(first, last, step, 0, unroll=True)

    def update(q, k, v, bias, state):
        s = dot(q, k, NT) * SCALE2 + jnp.concatenate([bias, bias], axis=0)
        m = jnp.broadcast_to(jnp.max(s, axis=-1, keepdims=True), q.shape)
        if state is not None:
            m = jnp.maximum(m, state[1])
        e = jnp.exp2(s - jnp.concatenate([m] * (s.shape[1] // 128), axis=1))
        total = jnp.broadcast_to(jnp.sum(e, axis=-1, keepdims=True), q.shape)
        o = dot(e.astype(BF16), v)
        if state is not None:
            decay = jnp.exp2(state[1] - m)
            total = state[2] * decay + total
            o = state[0] * decay + o
        return o, m, total

    def far(p, first, last, slots):
        def step(r, _):
            rows = pl.ds(pl.multiple_of(r * 128, 128), 128)
            k, v = (jnp.concatenate([kv[s, p, w, rows, :] for s in slots], axis=0) for w in range(2))
            bias = bias_c[:, slots[0] * 128 : (slots[-1] + 1) * 128]
            state = None if slots[0] == 0 else (st_o[p, r], st_m[p, r], st_l[p, r])
            st_o[p, r], st_m[p, r], st_l[p, r] = update(q_s[p, r], k, v, bias, state)
            return 0

        lax.fori_loop(first, last, step, 0, unroll=True)

    def finish(p):
        for r in range(4):
            rows = slice(r * 128, (r + 1) * 128)
            o = st_o[p, r] / st_l[p, r]
            att_p[rows, :] = jnp.where(first_head, o[0:128], o[128:256]).astype(BF16)
            level = st_m[p, r] * LN2 + jnp.log(st_l[p, r])
            both = jnp.where(lane == 2 * p, level[0:128], level[128:256])
            if p == 0:
                lw_s[rows, :] = both
            else:
                lw_s[rows, :] = jnp.where(lane < 2, lw_s[rows, :], both)
        att_n[p] = dot(perm[1], att_p[...]).astype(BF16)
        att_all[p, tp] = att_n[p, pl.ds(pl.multiple_of(tp * OUT_ROWS, OUT_ROWS), OUT_ROWS), :]
        for d in (4, 3, 5, 2, 6, 1, 7):
            rows = pl.ds(pl.multiple_of(((tp + d) % NTP) * OUT_ROWS, OUT_ROWS), OUT_ROWS)
            start(att_n.at[p, rows], att_all.at[p, tp], R_A + p * (NTP - 1) + d - 1, t_peer[d])

    def attended_wait(p, d):
        arrived(att_all.at[p, (tp + NTP - d) % NTP], R_A + p * (NTP - 1) + d - 1)

    def log_weights():
        levels = jnp.transpose(lw_s[...])[0:8, :]
        high = levels.astype(BF16)
        rest = levels - high.astype(F32)
        mid = rest.astype(BF16)
        low = (rest - mid.astype(F32)).astype(BF16)
        natural = dot(high, perm[0]) + dot(mid, perm[0]) + dot(low, perm[0])
        lw_out[...] = natural[0:4, :]
        lw_copy.start()

    def project(d):
        if d:
            attended_wait(0, d)
            attended_wait(1, d)
        g = (tp + NTP - d) % NTP
        a = jnp.concatenate([att_all[0, g], att_all[1, g]], axis=1)
        for c in range(2):
            cols = slice(c * 1024, c * 1024 + 1024)
            part = dot(a, wo_v[g, :, cols]).astype(BF16).astype(F32)
            sum_s[:, cols] = part if d == 0 else sum_s[:, cols] + part

    def output():
        local[9].wait()
        total = sum_s[...]
        scale = lax.rsqrt(jnp.mean(total * total, axis=-1, keepdims=True) + EPS)
        out[...] = (total * scale * post[...]).astype(BF16)
        out_copy = pltpu.make_async_copy(out, out_h, lsem.at[11])
        out_copy.start()
        lw_copy.wait()
        out_copy.wait()

    weights_send(0)
    weights_send(1)
    wo_send()
    norm()
    permutation()
    permute()
    weights_wait(0)
    relay_send(0)
    weights_wait(1)
    relay_send(1)
    tables()
    relay_step(0, 0)
    relay_step(1, 0)
    biases()
    relay_step(0, 1)
    relay_step(1, 1)
    relay_step(0, 2)
    relay_step(1, 2)
    wo_step(0)
    relay_step(0, 3)
    keys_values(0)
    halo_send(0)
    relay_step(1, 3)
    keys_values(1)
    halo_send(1)
    queries()
    far(0, 0, 4, (0,))
    near(0, 1, 4)
    up(0, 1)
    far(1, 0, 4, (0,))
    down(0, 0)
    up(1, 1)
    near(1, 1, 4)
    wo_step(1)
    down(1, 0)
    up(0, 2)
    far(0, 0, 2, (1, 2))
    down(0, 4)
    up(1, 2)
    far(1, 0, 2, (1, 2))
    down(1, 4)
    down(0, 3)
    up(0, 3)
    wo_step(2)
    down(1, 3)
    far(0, 3, 4, (3, 4))
    up(1, 3)
    far(1, 3, 4, (3, 4))
    down(0, 2)
    up(0, 4)
    far(0, 0, 2, (3, 4))
    down(1, 2)
    far(0, 2, 3, (3, 4))
    down(0, 1)
    far(0, 2, 4, (1, 2))
    near(0, 0, 1)
    finish(0)
    up(1, 4)
    far(1, 0, 3, (3, 4))
    down(1, 1)
    far(1, 2, 4, (1, 2))
    near(1, 0, 1)
    finish(1)
    wo_sibling_wait()
    project(0)
    log_weights()
    project(1)
    project(7)
    project(2)
    project(6)
    project(3)
    project(5)
    project(4)
    output()
    for copy in sends:
        copy.wait_send()


def hand_over(out_in, lw_in, out, lw_out):
    out[...] = out_in[...]
    lw_out[...] = lw_in[...]


def body(hidden_in, pre_gain, query_proj, key_proj, value_proj, out_proj, post_gain):
    half = np.arange(HEAD_DIM // 2, dtype=np.float32) * np.float32(2.0) / np.float32(HEAD_DIM)
    freq = np.tile(np.power(np.float64(ROPE_BASE), -half.astype(np.float64)).astype(np.float32), 4).reshape(1, 128)
    any_spec = pl.BlockSpec(memory_space=pl.ANY)
    vmem = pl.BlockSpec(memory_space=pltpu.VMEM)
    results = pl.pallas_call(
        kernel,
        out_shape=(jax.ShapeDtypeStruct((OUT_ROWS, D), BF16), jax.ShapeDtypeStruct((4, ROWS), F32)),
        in_specs=[any_spec] * 8,
        out_specs=(any_spec, any_spec),
        scratch_shapes=[
            pltpu.VMEM((1, D), F32),
            pltpu.VMEM((1, 128), F32),
            pltpu.VMEM((1, D), F32),
            pltpu.VMEM((OUT_ROWS, D), BF16),
            pltpu.VMEM((4, ROWS), F32),
            pltpu.VMEM((ROWS, D), BF16),
            pltpu.VMEM((ROWS, D), BF16),
            pltpu.VMEM((D, WIDTH), BF16),
            pltpu.VMEM((2, 2, NZ, NY, D // NSP, 128), BF16),
            pltpu.VMEM((NTP, WIDTH, D), BF16),
            pltpu.VMEM((SLOTS, 2, 2, ROWS, 128), BF16),
            pltpu.VMEM((2, 2, ROWS - AHEAD_ROWS, 128), BF16),
            pltpu.VMEM((2, 4, 256, 128), BF16),
            pltpu.VMEM((2, 4, 256, 128), F32),
            pltpu.VMEM((2, 4, 256, 128), F32),
            pltpu.VMEM((2, 4, 256, 128), F32),
            pltpu.VMEM((ROWS, 128), BF16),
            pltpu.VMEM((2, ROWS, 128), BF16),
            pltpu.VMEM((2, NTP, OUT_ROWS, 128), BF16),
            pltpu.VMEM((ROWS, 128), F32),
            pltpu.VMEM((ROWS, 128), F32),
            pltpu.VMEM((ROWS, 128), F32),
            pltpu.VMEM((128, SLOTS * 128), F32),
            pltpu.VMEM((2, 128, 256), F32),
            pltpu.VMEM((2, ROWS, ROWS), BF16),
            pltpu.VMEM((OUT_ROWS, D), F32),
            pltpu.SemaphoreType.DMA((12,)),
            pltpu.SemaphoreType.DMA((N_SEND,)),
            pltpu.SemaphoreType.DMA((R_END,)),
        ],
        compiler_params=pltpu.CompilerParams(
            collective_id=0, has_side_effects=True, vmem_limit_bytes=60 * 1024 * 1024
        ),
        name="layer",
    )(
        hidden_in, pre_gain.reshape(1, D), jnp.asarray(freq), query_proj, key_proj, value_proj, out_proj,
        post_gain.reshape(1, D),
    )
    return pl.pallas_call(
        hand_over,
        out_shape=(jax.ShapeDtypeStruct((OUT_ROWS, D), BF16), jax.ShapeDtypeStruct((4, ROWS), F32)),
        in_specs=[vmem, vmem],
        out_specs=(vmem, vmem),
        name="hand_over",
    )(*results)


def solution(mesh):
    placed = (P("sp", None), P(), P(None, "tp"), P("sp", "tp"), P("sp", "tp"), P("tp", None), P())
    return jax.shard_map(
        body,
        mesh=mesh,
        in_specs=placed,
        out_specs=(P(("sp", "tp"), None), P("tp", "sp")),
        check_vma=False,
    )
```

```python
import functools
import math

import jax
import jax.numpy as jnp
import numpy as np
from jax import lax
from jax.experimental import pallas as pl
from jax.experimental.pallas import tpu as pltpu
from jax.sharding import PartitionSpec as P

HEAD_DIM = 64
SPAN = 128
EPS = 1e-06
ROPE_BASE = 10000.0
NY = 8
NZ = 8
NSP = NY * NZ
NTP = 8
NX = 4
ROWS = 512
D = 2048
WIDTH = 256
OUT_ROWS = 64
SLOTS = 5
NEG = -1e30
SCALE2 = math.log2(math.e) / 8.0
LN2 = math.log(2.0)
BIG = 512
F32 = jnp.float32
BF16 = jnp.bfloat16
MESH = pl.DeviceIdType.MESH

NT = (((1,), (1,)), ((), ()))
NN = (((1,), (0,)), ((), ()))

AHEAD_ROWS = 320

R_WD = 0
R_WR = R_WD + 4
R_X = R_WR + 2 * 2 * 2 * 7
R_H = R_X + 7
R_M = R_H + 4 * (SLOTS - 1)
R_A = R_M + 4 * SLOTS
R_END = R_A + 1 + (NTP - 1)
S_WD, S_WR, S_X, S_H, S_M, S_A = range(6)


def dot(a, b, dims=NN):
    return lax.dot_general(a, b, dims, preferred_element_type=F32)


def token_of(row):
    return (row // 128) + ((row // 8) % 4) * 4 + (row % 8) * 16 + ((row // 32) % 4) * 128


def kernel(
    hid, gain_h, freq_h, wq, wk, wv, wo, post_h,
    out_h, lw_h,
    gain, freq, post, out, lw_out, hid_v, np_v, wq_v, w_v, wo_v, kv, passing, q_s, st_o, st_m, st_l, att_p, att_n, att_all, lw_s,
    cos_s, sin_s, bias_c, bias_n, perm, sum_s, lsem, ssem, rsem,
):
    sp = lax.axis_index("sp")
    tp = lax.axis_index("tp")
    z, y = sp // NY, sp % NY
    x, core = tp // 2, tp % 2

    def start(src, dst, ridx, dev, kind):
        pltpu.make_async_remote_copy(
            src_ref=src, dst_ref=dst, send_sem=ssem.at[kind], recv_sem=rsem.at[ridx],
            device_id=dev, device_id_type=MESH,
        ).start()

    def finished(size, ridx, kind):
        return pltpu.make_async_remote_copy(
            src_ref=size, dst_ref=size, send_sem=ssem.at[kind], recv_sem=rsem.at[ridx],
            device_id=((sp + 1) % NSP, tp), device_id_type=MESH,
        )

    def arrived(dst, ridx):
        finished(dst, ridx, 0).wait_recv()

    def sent(size, kind):
        finished(size, 0, kind).wait_send()

    y_peer = [(z * NY + (y + d) % NY, tp) for d in range(NY)]
    z_peer = [(((z + d) % NZ) * NY + y, tp) for d in range(NZ)]
    ahead = ((sp + 1) % NSP, tp)
    behind = ((sp + NSP - 1) % NSP, tp)
    relay_of_me = (((z + y // 4) % NZ) * NY + (y + NY - 3) % NY, tp)
    source_y = (y + 3) % NY
    relay_source = (((z + NZ - source_y // 4) % NZ) * NY + source_y, tp)
    t_peer = [(sp, (tp + d) % NTP) for d in range(NTP)]
    x_right = (sp, (tp + 2) % NTP)
    x_left = (sp, (tp + NTP - 2) % NTP)
    sibling = (sp, x * 2 + (1 - core))

    local = [
        pltpu.make_async_copy(w.at[:, p * 128 : (p + 1) * 128], w_v.at[i, p, z, y], lsem.at[2 * p + i])
        for p in range(2)
        for i, w in enumerate((wk, wv))
    ] + [
        pltpu.make_async_copy(wo, wo_v.at[tp], lsem.at[4]),
        pltpu.make_async_copy(hid, hid_v, lsem.at[5]),
        pltpu.make_async_copy(wq, wq_v, lsem.at[6]),
        pltpu.make_async_copy(gain_h, gain, lsem.at[7]),
        pltpu.make_async_copy(freq_h, freq, lsem.at[8]),
        pltpu.make_async_copy(post_h, post, lsem.at[9]),
    ]
    for copy in local:
        copy.start()

    lw_copy = pltpu.make_async_copy(lw_out, lw_h, lsem.at[10])

    barrier = pltpu.get_barrier_semaphore()
    partners = y_peer[1:] + z_peer[1:] + t_peer[1:] + [ahead, behind, relay_of_me, relay_source]
    for dev in partners:
        pl.semaphore_signal(barrier, inc=1, device_id=dev, device_id_type=MESH)
    pl.semaphore_wait(barrier, len(partners))

    def weights_send(p):
        for i, peer in enumerate((y_peer, z_peer)):
            local[2 * p + i].wait()
            part = w_v.at[i, p, z, y]
            for d in range(1, 8):
                start(part, part, R_WD + i * 2 + p, peer[d], S_WD)

    def weights_wait(p):
        for i in range(2):
            arrived(w_v.at[i, p, 0, 0:7], R_WD + i * 2 + p)

    def relay_part(i, p, at, half):
        piece = pl.ds(half * 4, 4)
        return w_v.at[0, p, at, piece] if i == 0 else w_v.at[1, p, piece, at]

    def relay_sem(i, p, half, direction, hop):
        return R_WR + ((i * 2 + p) * 2 + half) * 7 + (hop if direction == 0 else 6 - hop)

    def relay_dev(i, direction):
        peer = z_peer if i == 0 else y_peer
        return peer[1] if direction == 0 else peer[7]

    def relay_send(p):
        for half in range(2):
            for i, at in enumerate((z, y)):
                part = relay_part(i, p, at, half)
                for direction in range(2):
                    start(part, part, relay_sem(i, p, half, direction, 0), relay_dev(i, direction), S_WR)

    def relay_step(p, hop):
        for half in range(2):
            for i, at in enumerate((z, y)):
                for direction in range(2):
                    hops = 4 if half == direction else 3
                    if hop < hops:
                        owner = (at + 7 - hop) % 8 if direction == 0 else (at + 1 + hop) % 8
                        part = relay_part(i, p, owner, half)
                        arrived(part, relay_sem(i, p, half, direction, hop))
                        if hop + 1 < hops:
                            start(part, part, relay_sem(i, p, half, direction, hop + 1), relay_dev(i, direction), S_WR)

    def wo_part(delta, part):
        group = wo_v.at[(tp + delta) % NTP]
        return group if part is None else group.at[pl.ds(part * 128, 128)]

    def wo_send():
        local[4].wait()
        start(wo_part(0, 0), wo_part(0, 0), R_X + 0, x_right, S_X)
        start(wo_part(0, 1), wo_part(0, 1), R_X + 1, x_left, S_X)
        start(wo_part(0, 1), wo_part(0, 1), R_X + 2, x_right, S_X)
        start(wo_part(0, 0), wo_part(0, 0), R_X + 3, x_left, S_X)
        start(wo_part(0, None), wo_part(0, None), R_X + 6, sibling, S_X)

    def wo_step(k):
        if k == 0:
            arrived(wo_part(6, 0), R_X + 0)
            start(wo_part(6, 0), wo_part(6, 0), R_X + 4, x_right, S_X)
            start(wo_part(6, 0), wo_part(6, 0), R_X + 6, sibling, S_X)
            arrived(wo_part(2, 1), R_X + 1)
            start(wo_part(2, 1), wo_part(2, 1), R_X + 5, x_left, S_X)
            start(wo_part(2, 1), wo_part(2, 1), R_X + 6, sibling, S_X)
        elif k == 1:
            arrived(wo_part(6, 1), R_X + 2)
            start(wo_part(6, 1), wo_part(6, 1), R_X + 6, sibling, S_X)
            arrived(wo_part(2, 0), R_X + 3)
            start(wo_part(2, 0), wo_part(2, 0), R_X + 6, sibling, S_X)
        else:
            arrived(wo_part(4, 0), R_X + 4)
            start(wo_part(4, 0), wo_part(4, 0), R_X + 6, sibling, S_X)
            arrived(wo_part(4, 1), R_X + 5)
            start(wo_part(4, 1), wo_part(4, 1), R_X + 6, sibling, S_X)

    def wo_sibling_wait():
        arrived(wo_v.at[0:4], R_X + 6)

    def up_part(k, p, w):
        return kv.at[k, p, w, 0:AHEAD_ROWS]

    def down_part(k, p, w):
        return kv.at[k, p, w, AHEAD_ROWS:ROWS]

    def up_sem(p, k, w):
        return R_H + (p * (SLOTS - 1) + k - 1) * 2 + w

    def down_sem(p, k, w):
        return R_M + (p * SLOTS + k) * 2 + w

    def halo_send(p):
        for w in range(2):
            start(up_part(0, p, w), up_part(1, p, w), up_sem(p, 1, w), ahead, S_H)
            start(down_part(0, p, w), passing.at[p, w], down_sem(p, 0, w), relay_of_me, S_M)

    def up(p, k):
        for w in range(2):
            arrived(up_part(k, p, w), up_sem(p, k, w))
            if k < SLOTS - 1:
                start(up_part(k, p, w), up_part(k + 1, p, w), up_sem(p, k + 1, w), ahead, S_H)

    def down(p, k):
        for w in range(2):
            if k == 0:
                arrived(passing.at[p, w], down_sem(p, 0, w))
                start(passing.at[p, w], down_part(4, p, w), down_sem(p, 4, w), y_peer[NY - 1], S_M)
            else:
                arrived(down_part(k, p, w), down_sem(p, k, w))
                if k > 1:
                    start(down_part(k, p, w), down_part(k - 1, p, w), down_sem(p, k - 1, w), behind, S_M)

    lane = lax.broadcasted_iota(jnp.int32, (1, 128), 1)
    first_head = lane < 64
    first_half = (lane % 64) < 32

    def norm():
        local[5].wait()
        local[7].wait()

        def step(i, _):
            rows = pl.ds(pl.multiple_of(i * 32, 32), 32)
            h = hid_v[rows, :].astype(F32)
            scale = lax.rsqrt(jnp.mean(h * h, axis=-1, keepdims=True) + EPS)
            hid_v[rows, :] = (h * scale * gain[...]).astype(BF16)
            return 0

        lax.fori_loop(0, ROWS // 32, step, 0)

    def permutation():
        token = token_of(lax.broadcasted_iota(jnp.int32, (ROWS, ROWS), 0))
        col = lax.broadcasted_iota(jnp.int32, (ROWS, ROWS), 1)
        perm[0] = (token == col).astype(F32).astype(BF16)
        row = lax.broadcasted_iota(jnp.int32, (ROWS, ROWS), 0)
        token_c = token_of(lax.broadcasted_iota(jnp.int32, (ROWS, ROWS), 1))
        perm[1] = (token_c == row).astype(F32).astype(BF16)

    def permute():
        def step(i, _):
            rows = pl.ds(pl.multiple_of(i * 128, 128), 128)
            for c in range(4):
                np_v[rows, c * 512 : (c + 1) * 512] = dot(perm[0, rows, :], hid_v[:, c * 512 : (c + 1) * 512]).astype(BF16)
            return 0

        lax.fori_loop(0, 4, step, 0, unroll=2)

    def tables():
        local[8].wait()
        token = token_of(lax.broadcasted_iota(jnp.int32, (ROWS, 128), 0))
        angle = (sp * ROWS + token).astype(F32) * freq[...]
        cos_s[...] = jnp.cos(angle)
        sine = jnp.sin(angle)
        sin_s[...] = jnp.where(first_half, -sine, sine)

    def biases():
        row = lax.broadcasted_iota(jnp.int32, (128, 128), 0)
        col = lax.broadcasted_iota(jnp.int32, (128, 128), 1)

        def class_token(r):
            return (r // 32) * 128 + (r % 8) * 16 + ((r // 8) % 4) * 4

        for k in range(SLOTS):
            delta = class_token(row) - class_token(col) + ROWS * k
            near = (delta >= 0) & (delta <= 4 * SPAN)
            far = (delta >= 0) & (delta <= 16 * SPAN) & ((row // 8) % 4 == (col // 8) % 4)
            bias = jnp.where(near & far, 1.0, jnp.where(near | far, 0.0, NEG))
            bias_c[:, k * 128 : (k + 1) * 128] = jnp.where(sp >= k, bias, NEG)

        def near_token(r):
            return (r // 32) + (r % 8) * 16 + ((r // 8) % 4) * 4

        delta = near_token(row) - near_token(col)
        own = jnp.where((delta >= 0) & (delta <= SPAN), 0.0, NEG)
        delta = delta + 128
        prev = jnp.where((delta >= 0) & (delta <= SPAN), 0.0, NEG)
        bias_n[0, :, 0:128] = jnp.where(sp >= 1, prev, NEG)
        bias_n[1, :, 0:128] = prev
        bias_n[0, :, 128:256] = own
        bias_n[1, :, 128:256] = own

    def rotate(u, rows):
        swapped = jnp.where(first_half, pltpu.roll(u, 96, 1), pltpu.roll(u, 32, 1))
        return (u * cos_s[rows, :] + swapped * sin_s[rows, :]).astype(BF16)

    def queries():
        local[6].wait()

        for r0 in range(0, ROWS, BIG):
            q = dot(np_v[r0 : r0 + BIG, :], wq_v[...])
            for r in range(BIG // 128):
                rows = slice(r0 + r * 128, r0 + r * 128 + 128)
                for p in range(2):
                    turned = rotate(q[r * 128 : r * 128 + 128, p * 128 : (p + 1) * 128], rows)
                    zero = jnp.zeros_like(turned)
                    q_s[p, r0 // 128 + r, 0:128, :] = jnp.where(first_head, turned, zero)
                    q_s[p, r0 // 128 + r, 128:256, :] = jnp.where(first_head, zero, turned)

    def keys_values(p):
        weights = jnp.concatenate([w_v[i, p].reshape(D, 128) for i in range(2)], axis=1)

        for r0 in range(0, ROWS, BIG):
            rows = slice(r0, r0 + BIG)
            both = dot(np_v[rows, :], weights)
            kv[0, p, 0, rows, :] = rotate(both[:, 0:128], rows)
            kv[0, p, 1, rows, :] = both[:, 128:256].astype(BF16)

    def near(p, first, last):
        def step(b, _):
            slot = (3 - b) // 3
            before = (b + 3) % 4
            state = [(r, pl.ds(pl.multiple_of(h * 128 + b * 32, 32), 32)) for h in range(2) for r in range(4)]

            def gathered(ref):
                return jnp.concatenate([ref[p, r, at, :] for r, at in state], axis=0)

            def scattered(ref, value):
                for i, (r, at) in enumerate(state):
                    ref[p, r, at, :] = value[i * 32 : (i + 1) * 32]

            def part(r, base):
                return pl.ds(pl.multiple_of(base + r * 128, 32), 32)

            k, v = (
                jnp.concatenate(
                    [kv[slot, p, w, part(r, before * 32), :] for r in range(4)]
                    + [kv[0, p, w, part(r, b * 32), :] for r in range(4)],
                    axis=0,
                )
                for w in range(2)
            )
            o, m, total = update(
                gathered(q_s), k, v, bias_n[jnp.minimum(b, 1)], (gathered(st_o), gathered(st_m), gathered(st_l))
            )
            scattered(st_o, o)
            scattered(st_m, m)
            scattered(st_l, total)
            return 0

        lax.fori_loop(first, last, step, 0, unroll=True)

    def update(q, k, v, bias, state):
        s = dot(q, k, NT) * SCALE2 + jnp.concatenate([bias, bias], axis=0)
        m = jnp.broadcast_to(jnp.max(s, axis=-1, keepdims=True), q.shape)
        if state is not None:
            m = jnp.maximum(m, state[1])
        e = jnp.exp2(s - jnp.concatenate([m] * (s.shape[1] // 128), axis=1))
        total = jnp.broadcast_to(jnp.sum(e, axis=-1, keepdims=True), q.shape)
        o = dot(e.astype(BF16), v)
        if state is not None:
            decay = jnp.exp2(state[1] - m)
            total = state[2] * decay + total
            o = state[0] * decay + o
        return o, m, total

    def far(p, first, last, slots):
        def step(r, _):
            rows = pl.ds(pl.multiple_of(r * 128, 128), 128)
            k, v = (jnp.concatenate([kv[s, p, w, rows, :] for s in slots], axis=0) for w in range(2))
            bias = bias_c[:, slots[0] * 128 : (slots[-1] + 1) * 128]
            state = None if slots[0] == 0 else (st_o[p, r], st_m[p, r], st_l[p, r])
            st_o[p, r], st_m[p, r], st_l[p, r] = update(q_s[p, r], k, v, bias, state)
            return 0

        lax.fori_loop(first, last, step, 0, unroll=True)

    def finish(p):
        for r in range(4):
            rows = slice(r * 128, (r + 1) * 128)
            o = st_o[p, r] / st_l[p, r]
            att_p[rows, :] = jnp.where(first_head, o[0:128], o[128:256]).astype(BF16)
            level = st_m[p, r] * LN2 + jnp.log(st_l[p, r])
            both = jnp.where(lane == 2 * p, level[0:128], level[128:256])
            if p == 0:
                lw_s[rows, :] = both
            else:
                lw_s[rows, :] = jnp.where(lane < 2, lw_s[rows, :], both)
        att_n[p] = dot(perm[1], att_p[...]).astype(BF16)
        att_all[p, tp] = att_n[p, pl.ds(pl.multiple_of(tp * OUT_ROWS, OUT_ROWS), OUT_ROWS), :]
        for d in (4, 3, 5, 2, 6, 1, 7):
            rows = pl.ds(pl.multiple_of(((tp + d) % NTP) * OUT_ROWS, OUT_ROWS), OUT_ROWS)
            start(att_n.at[p, rows], att_all.at[p, tp], R_A + p * d, t_peer[d], S_A)

    def log_weights():
        levels = jnp.transpose(lw_s[...])[0:8, :]
        high = levels.astype(BF16)
        rest = levels - high.astype(F32)
        mid = rest.astype(BF16)
        low = (rest - mid.astype(F32)).astype(BF16)
        natural = dot(high, perm[0]) + dot(mid, perm[0]) + dot(low, perm[0])
        lw_out[...] = natural[0:4, :]
        lw_copy.start()

    def project(d):
        g = (tp + NTP - d) % NTP
        if d == 1:
            arrived(att_all.at[0, 0:7], R_A)
        if d:
            arrived(att_all.at[1, g], R_A + d)
        a = jnp.concatenate([att_all[0, g], att_all[1, g]], axis=1)
        for c in range(2):
            cols = slice(c * 1024, c * 1024 + 1024)
            part = dot(a, wo_v[g, :, cols]).astype(BF16).astype(F32)
            sum_s[:, cols] = part if d == 0 else sum_s[:, cols] + part

    def output():
        local[9].wait()
        total = sum_s[...]
        scale = lax.rsqrt(jnp.mean(total * total, axis=-1, keepdims=True) + EPS)
        out[...] = (total * scale * post[...]).astype(BF16)
        out_copy = pltpu.make_async_copy(out, out_h, lsem.at[11])
        out_copy.start()
        lw_copy.wait()
        out_copy.wait()

    weights_send(0)
    weights_send(1)
    wo_send()
    norm()
    permutation()
    permute()
    weights_wait(0)
    relay_send(0)
    weights_wait(1)
    relay_send(1)
    tables()
    relay_step(0, 0)
    relay_step(1, 0)
    biases()
    relay_step(0, 1)
    relay_step(1, 1)
    relay_step(0, 2)
    relay_step(1, 2)
    wo_step(0)
    relay_step(0, 3)
    keys_values(0)
    halo_send(0)
    relay_step(1, 3)
    keys_values(1)
    halo_send(1)
    queries()
    far(0, 0, 4, (0,))
    near(0, 1, 4)
    up(0, 1)
    far(1, 0, 4, (0,))
    down(0, 0)
    up(1, 1)
    near(1, 1, 4)
    wo_step(1)
    down(1, 0)
    up(0, 2)
    far(0, 0, 2, (1, 2))
    down(0, 4)
    up(1, 2)
    far(1, 0, 2, (1, 2))
    down(1, 4)
    down(0, 3)
    up(0, 3)
    wo_step(2)
    down(1, 3)
    far(0, 3, 4, (3, 4))
    up(1, 3)
    far(1, 3, 4, (3, 4))
    down(0, 2)
    up(0, 4)
    far(0, 0, 2, (3, 4))
    down(1, 2)
    far(0, 2, 3, (3, 4))
    down(0, 1)
    far(0, 2, 4, (1, 2))
    near(0, 0, 1)
    finish(0)
    up(1, 4)
    far(1, 0, 3, (3, 4))
    down(1, 1)
    far(1, 2, 4, (1, 2))
    near(1, 0, 1)
    finish(1)
    wo_sibling_wait()
    project(0)
    log_weights()
    project(1)
    project(7)
    project(2)
    project(6)
    project(3)
    project(5)
    project(4)
    output()
    sent(w_v.at[0, 0, 0:4, 0:7], S_WD)
    sent(w_v.at[:, :, 0:7], S_WR)
    sent(wo_v.at[0:7], S_X)
    sent(kv.at[0:4, :, :, 0:AHEAD_ROWS], S_H)
    sent(kv.at[:, :, :, AHEAD_ROWS:ROWS], S_M)
    sent(att_all.at[:, 0:7], S_A)


def hand_over(out_in, lw_in, out, lw_out):
    out[...] = out_in[...]
    lw_out[...] = lw_in[...]


def body(hidden_in, pre_gain, query_proj, key_proj, value_proj, out_proj, post_gain):
    half = np.arange(HEAD_DIM // 2, dtype=np.float32) * np.float32(2.0) / np.float32(HEAD_DIM)
    freq = np.tile(np.power(np.float64(ROPE_BASE), -half.astype(np.float64)).astype(np.float32), 4).reshape(1, 128)
    any_spec = pl.BlockSpec(memory_space=pl.ANY)
    vmem = pl.BlockSpec(memory_space=pltpu.VMEM)
    results = pl.pallas_call(
        kernel,
        out_shape=(jax.ShapeDtypeStruct((OUT_ROWS, D), BF16), jax.ShapeDtypeStruct((4, ROWS), F32)),
        in_specs=[any_spec] * 8,
        out_specs=(any_spec, any_spec),
        scratch_shapes=[
            pltpu.VMEM((1, D), F32),
            pltpu.VMEM((1, 128), F32),
            pltpu.VMEM((1, D), F32),
            pltpu.VMEM((OUT_ROWS, D), BF16),
            pltpu.VMEM((4, ROWS), F32),
            pltpu.VMEM((ROWS, D), BF16),
            pltpu.VMEM((ROWS, D), BF16),
            pltpu.VMEM((D, WIDTH), BF16),
            pltpu.VMEM((2, 2, NZ, NY, D // NSP, 128), BF16),
            pltpu.VMEM((NTP, WIDTH, D), BF16),
            pltpu.VMEM((SLOTS, 2, 2, ROWS, 128), BF16),
            pltpu.VMEM((2, 2, ROWS - AHEAD_ROWS, 128), BF16),
            pltpu.VMEM((2, 4, 256, 128), BF16),
            pltpu.VMEM((2, 4, 256, 128), F32),
            pltpu.VMEM((2, 4, 256, 128), F32),
            pltpu.VMEM((2, 4, 256, 128), F32),
            pltpu.VMEM((ROWS, 128), BF16),
            pltpu.VMEM((2, ROWS, 128), BF16),
            pltpu.VMEM((2, NTP, OUT_ROWS, 128), BF16),
            pltpu.VMEM((ROWS, 128), F32),
            pltpu.VMEM((ROWS, 128), F32),
            pltpu.VMEM((ROWS, 128), F32),
            pltpu.VMEM((128, SLOTS * 128), F32),
            pltpu.VMEM((2, 128, 256), F32),
            pltpu.VMEM((2, ROWS, ROWS), BF16),
            pltpu.VMEM((OUT_ROWS, D), F32),
            pltpu.SemaphoreType.DMA((12,)),
            pltpu.SemaphoreType.DMA((6,)),
            pltpu.SemaphoreType.DMA((R_END,)),
        ],
        compiler_params=pltpu.CompilerParams(
            collective_id=0, has_side_effects=True, vmem_limit_bytes=60 * 1024 * 1024
        ),
        name="layer",
    )(
        hidden_in, pre_gain.reshape(1, D), jnp.asarray(freq), query_proj, key_proj, value_proj, out_proj,
        post_gain.reshape(1, D),
    )
    return pl.pallas_call(
        hand_over,
        out_shape=(jax.ShapeDtypeStruct((OUT_ROWS, D), BF16), jax.ShapeDtypeStruct((4, ROWS), F32)),
        in_specs=[vmem, vmem],
        out_specs=(vmem, vmem),
        name="hand_over",
    )(*results)


def solution(mesh):
    placed = (P("sp", None), P(), P(None, "tp"), P("sp", "tp"), P("sp", "tp"), P("tp", None), P())
    return jax.shard_map(
        body,
        mesh=mesh,
        in_specs=placed,
        out_specs=(P(("sp", "tp"), None), P("tp", "sp")),
        check_vma=False,
    )
```

```python
import functools
import math

import jax
import jax.numpy as jnp
import numpy as np
from jax import lax
from jax.experimental import pallas as pl
from jax.experimental.pallas import tpu as pltpu
from jax.sharding import PartitionSpec as P

HEAD_DIM = 64
SPAN = 128
EPS = 1e-06
ROPE_BASE = 10000.0
NY = 8
NZ = 8
NSP = NY * NZ
NTP = 8
NX = 4
ROWS = 512
D = 2048
WIDTH = 256
OUT_ROWS = 64
SLOTS = 5
NEG = -1e30
SCALE2 = math.log2(math.e) / 8.0
LN2 = math.log(2.0)
BIG = 512
F32 = jnp.float32
BF16 = jnp.bfloat16
MESH = pl.DeviceIdType.MESH

NT = (((1,), (1,)), ((), ()))
NN = (((1,), (0,)), ((), ()))

AHEAD_ROWS = 320

R_WD = 0
R_WR = R_WD + 4
R_X = R_WR + 2 * 2 * 2 * 7
R_H = R_X + 7
R_M = R_H + 4 * (SLOTS - 1)
R_A = R_M + 4 * SLOTS
R_END = R_A + 1 + (NTP - 1)
S_WD, S_WR, S_X, S_H, S_M, S_A = range(6)


def dot(a, b, dims=NN):
    return lax.dot_general(a, b, dims, preferred_element_type=F32)


def token_of(row):
    return (row // 128) + ((row // 8) % 4) * 4 + (row % 8) * 16 + ((row // 32) % 4) * 128


def kernel(
    hid, gain_h, freq_h, wq, wk, wv, wo, post_h,
    out_h, lw_h,
    gain, freq, post, out, lw_out, hid_v, np_v, wq_v, w_v, wo_v, kv, passing, q_s, st_o, st_m, st_l, att_p, att_n, att_all, lw_s,
    cos_s, sin_s, bias_c, bias_n, perm, sum_s, lsem, ssem, rsem,
):
    sp = lax.axis_index("sp")
    tp = lax.axis_index("tp")
    z, y = sp // NY, sp % NY
    x, core = tp // 2, tp % 2

    def start(src, dst, ridx, dev, kind):
        pltpu.make_async_remote_copy(
            src_ref=src, dst_ref=dst, send_sem=ssem.at[kind], recv_sem=rsem.at[ridx],
            device_id=dev, device_id_type=MESH,
        ).start()

    def finished(size, ridx, kind):
        return pltpu.make_async_remote_copy(
            src_ref=size, dst_ref=size, send_sem=ssem.at[kind], recv_sem=rsem.at[ridx],
            device_id=((sp + 1) % NSP, tp), device_id_type=MESH,
        )

    def arrived(dst, ridx):
        finished(dst, ridx, 0).wait_recv()

    def sent(size, kind):
        finished(size, 0, kind).wait_send()

    y_peer = [(z * NY + (y + d) % NY, tp) for d in range(NY)]
    z_peer = [(((z + d) % NZ) * NY + y, tp) for d in range(NZ)]
    ahead = ((sp + 1) % NSP, tp)
    behind = ((sp + NSP - 1) % NSP, tp)
    relay_of_me = (((z + y // 4) % NZ) * NY + (y + NY - 3) % NY, tp)
    source_y = (y + 3) % NY
    relay_source = (((z + NZ - source_y // 4) % NZ) * NY + source_y, tp)
    t_peer = [(sp, (tp + d) % NTP) for d in range(NTP)]
    x_right = (sp, (tp + 2) % NTP)
    x_left = (sp, (tp + NTP - 2) % NTP)
    sibling = (sp, x * 2 + (1 - core))

    local = [
        pltpu.make_async_copy(w.at[:, p * 128 : (p + 1) * 128], w_v.at[i, p, z, y], lsem.at[2 * p + i])
        for p in range(2)
        for i, w in enumerate((wk, wv))
    ] + [
        pltpu.make_async_copy(wo, wo_v.at[tp], lsem.at[4]),
        pltpu.make_async_copy(hid, hid_v, lsem.at[5]),
        pltpu.make_async_copy(wq, wq_v, lsem.at[6]),
        pltpu.make_async_copy(gain_h, gain, lsem.at[7]),
        pltpu.make_async_copy(freq_h, freq, lsem.at[8]),
        pltpu.make_async_copy(post_h, post, lsem.at[9]),
    ]
    for copy in local:
        copy.start()

    lw_copy = pltpu.make_async_copy(lw_out, lw_h, lsem.at[10])

    barrier = pltpu.get_barrier_semaphore()
    partners = y_peer[1:] + z_peer[1:] + t_peer[1:] + [ahead, behind, relay_of_me, relay_source]
    for dev in partners:
        pl.semaphore_signal(barrier, inc=1, device_id=dev, device_id_type=MESH)
    pl.semaphore_wait(barrier, len(partners))

    def weights_send(p):
        for i, peer in enumerate((y_peer, z_peer)):
            local[2 * p + i].wait()
            part = w_v.at[i, p, z, y]
            for d in (4, 3, 5, 2, 6, 1, 7):
                start(part, part, R_WD + i * 2 + p, peer[d], S_WD)

    def weights_wait(p):
        for i in range(2):
            arrived(w_v.at[i, p, 0, 0:7], R_WD + i * 2 + p)

    def relay_part(i, p, at, half):
        piece = pl.ds(half * 4, 4)
        return w_v.at[0, p, at, piece] if i == 0 else w_v.at[1, p, piece, at]

    def relay_sem(i, p, half, direction, hop):
        return R_WR + ((i * 2 + p) * 2 + half) * 7 + (hop if direction == 0 else 6 - hop)

    def relay_dev(i, direction):
        peer = z_peer if i == 0 else y_peer
        return peer[1] if direction == 0 else peer[7]

    def relay_order():
        for late in range(2):
            for i, at in enumerate((z, y)):
                for direction in range(2):
                    yield direction ^ late, i, at, direction, 4 - late

    def relay_send(p):
        for half, i, at, direction, _ in relay_order():
            part = relay_part(i, p, at, half)
            start(part, part, relay_sem(i, p, half, direction, 0), relay_dev(i, direction), S_WR)

    def relay_step(p, hop):
        for half, i, at, direction, hops in relay_order():
            if hop < hops:
                owner = (at + 7 - hop) % 8 if direction == 0 else (at + 1 + hop) % 8
                part = relay_part(i, p, owner, half)
                arrived(part, relay_sem(i, p, half, direction, hop))
                if hop + 1 < hops:
                    start(part, part, relay_sem(i, p, half, direction, hop + 1), relay_dev(i, direction), S_WR)

    def wo_part(delta, part):
        group = wo_v.at[(tp + delta) % NTP]
        return group if part is None else group.at[pl.ds(part * 128, 128)]

    def wo_send():
        local[4].wait()
        start(wo_part(0, 0), wo_part(0, 0), R_X + 0, x_right, S_X)
        start(wo_part(0, 1), wo_part(0, 1), R_X + 1, x_left, S_X)
        start(wo_part(0, 1), wo_part(0, 1), R_X + 2, x_right, S_X)
        start(wo_part(0, 0), wo_part(0, 0), R_X + 3, x_left, S_X)
        start(wo_part(0, None), wo_part(0, None), R_X + 6, sibling, S_X)

    def wo_step(k):
        if k == 0:
            arrived(wo_part(6, 0), R_X + 0)
            start(wo_part(6, 0), wo_part(6, 0), R_X + 4, x_right, S_X)
            start(wo_part(6, 0), wo_part(6, 0), R_X + 6, sibling, S_X)
            arrived(wo_part(2, 1), R_X + 1)
            start(wo_part(2, 1), wo_part(2, 1), R_X + 5, x_left, S_X)
            start(wo_part(2, 1), wo_part(2, 1), R_X + 6, sibling, S_X)
        elif k == 1:
            arrived(wo_part(6, 1), R_X + 2)
            start(wo_part(6, 1), wo_part(6, 1), R_X + 6, sibling, S_X)
            arrived(wo_part(2, 0), R_X + 3)
            start(wo_part(2, 0), wo_part(2, 0), R_X + 6, sibling, S_X)
        else:
            arrived(wo_part(4, 0), R_X + 4)
            start(wo_part(4, 0), wo_part(4, 0), R_X + 6, sibling, S_X)
            arrived(wo_part(4, 1), R_X + 5)
            start(wo_part(4, 1), wo_part(4, 1), R_X + 6, sibling, S_X)

    def wo_sibling_wait():
        arrived(wo_v.at[0:4], R_X + 6)

    def up_part(k, p, w):
        return kv.at[k, p, w, 0:AHEAD_ROWS]

    def down_part(k, p, w):
        return kv.at[k, p, w, AHEAD_ROWS:ROWS]

    def up_sem(p, k, w):
        return R_H + (p * (SLOTS - 1) + k - 1) * 2 + w

    def down_sem(p, k, w):
        return R_M + (p * SLOTS + k) * 2 + w

    def clear():
        for k in range(1, SLOTS):

            @pl.when(sp < k)
            def _():
                kv[k, :, :, 0:AHEAD_ROWS] = jnp.zeros((2, 2, AHEAD_ROWS, 128), BF16)

    def halo_send(p):
        @pl.when(sp < NSP - 1)
        def _():
            for w in range(2):
                start(up_part(0, p, w), up_part(1, p, w), up_sem(p, 1, w), ahead, S_H)

        for w in range(2):
            start(down_part(0, p, w), passing.at[p, w], down_sem(p, 0, w), relay_of_me, S_M)

    def up(p, k):
        for w in range(2):

            @pl.when(sp >= k)
            def _():
                arrived(up_part(k, p, w), up_sem(p, k, w))

            if k < SLOTS - 1:

                @pl.when((sp >= k) & (sp < NSP - 1))
                def _():
                    start(up_part(k, p, w), up_part(k + 1, p, w), up_sem(p, k + 1, w), ahead, S_H)

    def down(p, k):
        for w in range(2):
            if k == 0:
                arrived(passing.at[p, w], down_sem(p, 0, w))
                start(passing.at[p, w], down_part(4, p, w), down_sem(p, 4, w), y_peer[NY - 1], S_M)
            else:
                arrived(down_part(k, p, w), down_sem(p, k, w))
                if k > 1:
                    start(down_part(k, p, w), down_part(k - 1, p, w), down_sem(p, k - 1, w), behind, S_M)

    lane = lax.broadcasted_iota(jnp.int32, (1, 128), 1)
    first_head = lane < 64
    first_half = (lane % 64) < 32

    def norm():
        local[5].wait()
        local[7].wait()

        def step(i, _):
            rows = pl.ds(pl.multiple_of(i * 32, 32), 32)
            h = hid_v[rows, :].astype(F32)
            scale = lax.rsqrt(jnp.mean(h * h, axis=-1, keepdims=True) + EPS)
            hid_v[rows, :] = (h * scale * gain[...]).astype(BF16)
            return 0

        lax.fori_loop(0, ROWS // 32, step, 0)

    def permutation():
        token = token_of(lax.broadcasted_iota(jnp.int32, (ROWS, ROWS), 0))
        col = lax.broadcasted_iota(jnp.int32, (ROWS, ROWS), 1)
        perm[0] = (token == col).astype(F32).astype(BF16)
        row = lax.broadcasted_iota(jnp.int32, (ROWS, ROWS), 0)
        token_c = token_of(lax.broadcasted_iota(jnp.int32, (ROWS, ROWS), 1))
        perm[1] = (token_c == row).astype(F32).astype(BF16)

    def permute():
        def step(i, _):
            rows = pl.ds(pl.multiple_of(i * 128, 128), 128)
            for c in range(4):
                np_v[rows, c * 512 : (c + 1) * 512] = dot(perm[0, rows, :], hid_v[:, c * 512 : (c + 1) * 512]).astype(BF16)
            return 0

        lax.fori_loop(0, 4, step, 0, unroll=2)

    def tables():
        local[8].wait()
        token = token_of(lax.broadcasted_iota(jnp.int32, (ROWS, 128), 0))
        angle = (sp * ROWS + token).astype(F32) * freq[...]
        cos_s[...] = jnp.cos(angle)
        sine = jnp.sin(angle)
        sin_s[...] = jnp.where(first_half, -sine, sine)

    def biases():
        row = lax.broadcasted_iota(jnp.int32, (128, 128), 0)
        col = lax.broadcasted_iota(jnp.int32, (128, 128), 1)

        def class_token(r):
            return (r // 32) * 128 + (r % 8) * 16 + ((r // 8) % 4) * 4

        for k in range(SLOTS):
            delta = class_token(row) - class_token(col) + ROWS * k
            near = (delta >= 0) & (delta <= 4 * SPAN)
            far = (delta >= 0) & (delta <= 16 * SPAN) & ((row // 8) % 4 == (col // 8) % 4)
            bias = jnp.where(near & far, 1.0, jnp.where(near | far, 0.0, NEG))
            bias_c[:, k * 128 : (k + 1) * 128] = jnp.where(sp >= k, bias, NEG)

        def near_token(r):
            return (r // 32) + (r % 8) * 16 + ((r // 8) % 4) * 4

        delta = near_token(row) - near_token(col)
        own = jnp.where((delta >= 0) & (delta <= SPAN), 0.0, NEG)
        delta = delta + 128
        prev = jnp.where((delta >= 0) & (delta <= SPAN), 0.0, NEG)
        bias_n[0, :, 0:128] = jnp.where(sp >= 1, prev, NEG)
        bias_n[1, :, 0:128] = prev
        bias_n[0, :, 128:256] = own
        bias_n[1, :, 128:256] = own

    def rotate(u, rows):
        swapped = jnp.where(first_half, pltpu.roll(u, 96, 1), pltpu.roll(u, 32, 1))
        return (u * cos_s[rows, :] + swapped * sin_s[rows, :]).astype(BF16)

    def queries():
        local[6].wait()

        for r0 in range(0, ROWS, BIG):
            q = dot(np_v[r0 : r0 + BIG, :], wq_v[...])
            for r in range(BIG // 128):
                rows = slice(r0 + r * 128, r0 + r * 128 + 128)
                for p in range(2):
                    turned = rotate(q[r * 128 : r * 128 + 128, p * 128 : (p + 1) * 128], rows)
                    zero = jnp.zeros_like(turned)
                    q_s[p, r0 // 128 + r, 0:128, :] = jnp.where(first_head, turned, zero)
                    q_s[p, r0 // 128 + r, 128:256, :] = jnp.where(first_head, zero, turned)

    def keys_values(p):
        weights = jnp.concatenate([w_v[i, p].reshape(D, 128) for i in range(2)], axis=1)

        for r0 in range(0, ROWS, BIG):
            rows = slice(r0, r0 + BIG)
            both = dot(np_v[rows, :], weights)
            kv[0, p, 0, rows, :] = rotate(both[:, 0:128], rows)
            kv[0, p, 1, rows, :] = both[:, 128:256].astype(BF16)

    def near(p, first, last):
        def step(b, _):
            slot = (3 - b) // 3
            before = (b + 3) % 4
            state = [(r, pl.ds(pl.multiple_of(h * 128 + b * 32, 32), 32)) for h in range(2) for r in range(4)]

            def gathered(ref):
                return jnp.concatenate([ref[p, r, at, :] for r, at in state], axis=0)

            def scattered(ref, value):
                for i, (r, at) in enumerate(state):
                    ref[p, r, at, :] = value[i * 32 : (i + 1) * 32]

            def part(r, base):
                return pl.ds(pl.multiple_of(base + r * 128, 32), 32)

            k, v = (
                jnp.concatenate(
                    [kv[slot, p, w, part(r, before * 32), :] for r in range(4)]
                    + [kv[0, p, w, part(r, b * 32), :] for r in range(4)],
                    axis=0,
                )
                for w in range(2)
            )
            o, m, total = update(
                gathered(q_s), k, v, bias_n[jnp.minimum(b, 1)], (gathered(st_o), gathered(st_m), gathered(st_l))
            )
            scattered(st_o, o)
            scattered(st_m, m)
            scattered(st_l, total)
            return 0

        lax.fori_loop(first, last, step, 0, unroll=True)

    def update(q, k, v, bias, state):
        s = dot(q, k, NT) * SCALE2 + jnp.concatenate([bias, bias], axis=0)
        m = jnp.broadcast_to(jnp.max(s, axis=-1, keepdims=True), q.shape)
        if state is not None:
            m = jnp.maximum(m, state[1])
        e = jnp.exp2(s - jnp.concatenate([m] * (s.shape[1] // 128), axis=1))
        total = jnp.broadcast_to(jnp.sum(e, axis=-1, keepdims=True), q.shape)
        o = dot(e.astype(BF16), v)
        if state is not None:
            decay = jnp.exp2(state[1] - m)
            total = state[2] * decay + total
            o = state[0] * decay + o
        return o, m, total

    def far(p, first, last, slots):
        def step(r, _):
            rows = pl.ds(pl.multiple_of(r * 128, 128), 128)
            k, v = (jnp.concatenate([kv[s, p, w, rows, :] for s in slots], axis=0) for w in range(2))
            bias = bias_c[:, slots[0] * 128 : (slots[-1] + 1) * 128]
            state = None if slots[0] == 0 else (st_o[p, r], st_m[p, r], st_l[p, r])
            st_o[p, r], st_m[p, r], st_l[p, r] = update(q_s[p, r], k, v, bias, state)
            return 0

        lax.fori_loop(first, last, step, 0, unroll=True)

    def levels(p):
        for r in range(4):
            rows = slice(r * 128, (r + 1) * 128)
            level = st_m[p, r] * LN2 + jnp.log(st_l[p, r])
            both = jnp.where(lane == 2 * p, level[0:128], level[128:256])
            lw_s[rows, :] = both if p == 0 else jnp.where(lane < 2, lw_s[rows, :], both)

    def finish(p):
        for r in range(4):
            rows = slice(r * 128, (r + 1) * 128)
            o = st_o[p, r] / st_l[p, r]
            att_p[rows, :] = jnp.where(first_head, o[0:128], o[128:256]).astype(BF16)
        att_n[p] = dot(perm[1], att_p[...]).astype(BF16)
        att_all[p, tp] = att_n[p, pl.ds(pl.multiple_of(tp * OUT_ROWS, OUT_ROWS), OUT_ROWS), :]
        for d in (4, 3, 5, 2, 6, 1, 7):
            rows = pl.ds(pl.multiple_of(((tp + d) % NTP) * OUT_ROWS, OUT_ROWS), OUT_ROWS)
            start(att_n.at[p, rows], att_all.at[p, tp], R_A + p * d, t_peer[d], S_A)

    def log_weights():
        levels = jnp.transpose(lw_s[...])[0:8, :]
        high = levels.astype(BF16)
        rest = levels - high.astype(F32)
        mid = rest.astype(BF16)
        low = (rest - mid.astype(F32)).astype(BF16)
        natural = dot(high, perm[0]) + dot(mid, perm[0]) + dot(low, perm[0])
        lw_out[...] = natural[0:4, :]
        lw_copy.start()

    def project(d):
        g = (tp + NTP - d) % NTP
        if d == 1:
            arrived(att_all.at[0, 0:7], R_A)
        if d:
            arrived(att_all.at[1, g], R_A + d)
        a = jnp.concatenate([att_all[0, g], att_all[1, g]], axis=1)
        for c in range(2):
            cols = slice(c * 1024, c * 1024 + 1024)
            part = dot(a, wo_v[g, :, cols]).astype(BF16).astype(F32)
            sum_s[:, cols] = part if d == 0 else sum_s[:, cols] + part

    def output():
        local[9].wait()
        total = sum_s[...]
        scale = lax.rsqrt(jnp.mean(total * total, axis=-1, keepdims=True) + EPS)
        out[...] = (total * scale * post[...]).astype(BF16)
        out_copy = pltpu.make_async_copy(out, out_h, lsem.at[11])
        out_copy.start()
        lw_copy.wait()
        out_copy.wait()

    weights_send(0)
    weights_send(1)
    wo_send()
    norm()
    permutation()
    clear()
    permute()
    weights_wait(0)
    relay_send(0)
    weights_wait(1)
    relay_send(1)
    tables()
    relay_step(0, 0)
    relay_step(1, 0)
    biases()
    relay_step(0, 1)
    relay_step(1, 1)
    relay_step(0, 2)
    relay_step(1, 2)
    wo_step(0)
    relay_step(0, 3)
    keys_values(0)
    halo_send(0)
    relay_step(1, 3)
    keys_values(1)
    halo_send(1)
    queries()
    far(0, 0, 4, (0,))
    near(0, 1, 4)
    up(0, 1)
    far(1, 0, 4, (0,))
    down(0, 0)
    up(1, 1)
    near(1, 1, 4)
    wo_step(1)
    down(1, 0)
    up(0, 2)
    far(0, 0, 2, (1, 2))
    down(0, 4)
    up(1, 2)
    far(1, 0, 2, (1, 2))
    down(1, 4)
    down(0, 3)
    up(0, 3)
    wo_step(2)
    down(1, 3)
    far(0, 3, 4, (3, 4))
    up(1, 3)
    far(1, 3, 4, (3, 4))
    down(0, 2)
    down(1, 2)
    up(0, 4)
    far(0, 0, 3, (3, 4))
    down(0, 1)
    far(0, 2, 4, (1, 2))
    near(0, 0, 1)
    finish(0)
    levels(0)
    up(1, 4)
    far(1, 0, 3, (3, 4))
    down(1, 1)
    far(1, 2, 4, (1, 2))
    near(1, 0, 1)
    finish(1)
    wo_sibling_wait()
    project(0)
    levels(1)
    log_weights()
    project(1)
    project(7)
    project(2)
    project(6)
    project(3)
    project(5)
    project(4)
    output()
    sent(w_v.at[0, 0, 0:4, 0:7], S_WD)
    sent(w_v.at[:, :, 0:7], S_WR)
    sent(wo_v.at[0:7], S_X)
    for k in range(SLOTS - 1):

        @pl.when((sp >= k) & (sp < NSP - 1))
        def _():
            sent(kv.at[k, :, :, 0:AHEAD_ROWS], S_H)

    sent(kv.at[:, :, :, AHEAD_ROWS:ROWS], S_M)
    sent(att_all.at[:, 0:7], S_A)


def hand_over(out_in, lw_in, out, lw_out):
    out[...] = out_in[...]
    lw_out[...] = lw_in[...]


def body(hidden_in, pre_gain, query_proj, key_proj, value_proj, out_proj, post_gain):
    half = np.arange(HEAD_DIM // 2, dtype=np.float32) * np.float32(2.0) / np.float32(HEAD_DIM)
    freq = np.tile(np.power(np.float64(ROPE_BASE), -half.astype(np.float64)).astype(np.float32), 4).reshape(1, 128)
    any_spec = pl.BlockSpec(memory_space=pl.ANY)
    vmem = pl.BlockSpec(memory_space=pltpu.VMEM)
    results = pl.pallas_call(
        kernel,
        out_shape=(jax.ShapeDtypeStruct((OUT_ROWS, D), BF16), jax.ShapeDtypeStruct((4, ROWS), F32)),
        in_specs=[any_spec] * 8,
        out_specs=(any_spec, any_spec),
        scratch_shapes=[
            pltpu.VMEM((1, D), F32),
            pltpu.VMEM((1, 128), F32),
            pltpu.VMEM((1, D), F32),
            pltpu.VMEM((OUT_ROWS, D), BF16),
            pltpu.VMEM((4, ROWS), F32),
            pltpu.VMEM((ROWS, D), BF16),
            pltpu.VMEM((ROWS, D), BF16),
            pltpu.VMEM((D, WIDTH), BF16),
            pltpu.VMEM((2, 2, NZ, NY, D // NSP, 128), BF16),
            pltpu.VMEM((NTP, WIDTH, D), BF16),
            pltpu.VMEM((SLOTS, 2, 2, ROWS, 128), BF16),
            pltpu.VMEM((2, 2, ROWS - AHEAD_ROWS, 128), BF16),
            pltpu.VMEM((2, 4, 256, 128), BF16),
            pltpu.VMEM((2, 4, 256, 128), F32),
            pltpu.VMEM((2, 4, 256, 128), F32),
            pltpu.VMEM((2, 4, 256, 128), F32),
            pltpu.VMEM((ROWS, 128), BF16),
            pltpu.VMEM((2, ROWS, 128), BF16),
            pltpu.VMEM((2, NTP, OUT_ROWS, 128), BF16),
            pltpu.VMEM((ROWS, 128), F32),
            pltpu.VMEM((ROWS, 128), F32),
            pltpu.VMEM((ROWS, 128), F32),
            pltpu.VMEM((128, SLOTS * 128), F32),
            pltpu.VMEM((2, 128, 256), F32),
            pltpu.VMEM((2, ROWS, ROWS), BF16),
            pltpu.VMEM((OUT_ROWS, D), F32),
            pltpu.SemaphoreType.DMA((12,)),
            pltpu.SemaphoreType.DMA((6,)),
            pltpu.SemaphoreType.DMA((R_END,)),
        ],
        compiler_params=pltpu.CompilerParams(
            collective_id=0, has_side_effects=True, vmem_limit_bytes=60 * 1024 * 1024
        ),
        name="layer",
    )(
        hidden_in, pre_gain.reshape(1, D), jnp.asarray(freq), query_proj, key_proj, value_proj, out_proj,
        post_gain.reshape(1, D),
    )
    return pl.pallas_call(
        hand_over,
        out_shape=(jax.ShapeDtypeStruct((OUT_ROWS, D), BF16), jax.ShapeDtypeStruct((4, ROWS), F32)),
        in_specs=[vmem, vmem],
        out_specs=(vmem, vmem),
        name="hand_over",
    )(*results)


def solution(mesh):
    placed = (P("sp", None), P(), P(None, "tp"), P("sp", "tp"), P("sp", "tp"), P("tp", None), P())
    return jax.shard_map(
        body,
        mesh=mesh,
        in_specs=placed,
        out_specs=(P(("sp", "tp"), None), P("tp", "sp")),
        check_vma=False,
    )
```

```python
import functools
import math

import jax
import jax.numpy as jnp
import numpy as np
from jax import lax
from jax.experimental import pallas as pl
from jax.experimental.pallas import tpu as pltpu
from jax.sharding import PartitionSpec as P

HEAD_DIM = 64
SPAN = 128
EPS = 1e-06
ROPE_BASE = 10000.0
NY = 8
NZ = 8
NSP = NY * NZ
NTP = 8
NX = 4
ROWS = 512
D = 2048
WIDTH = 256
OUT_ROWS = 64
SLOTS = 5
NEG = -1e30
SCALE2 = math.log2(math.e) / 8.0
LN2 = math.log(2.0)
BIG = 512
F32 = jnp.float32
BF16 = jnp.bfloat16
MESH = pl.DeviceIdType.MESH

NT = (((1,), (1,)), ((), ()))
NN = (((1,), (0,)), ((), ()))

AHEAD_ROWS = 320

R_WD = 0
R_WR = R_WD + 4
R_X = R_WR + 2 * 2 * 2 * 7
R_H = R_X + 7
R_M = R_H + 4 * (SLOTS - 1)
R_A = R_M + 4 * SLOTS
R_END = R_A + 1 + (NTP - 1)
S_WD, S_WR, S_X, S_H, S_M, S_A = range(6)


def dot(a, b, dims=NN):
    return lax.dot_general(a, b, dims, preferred_element_type=F32)


def token_of(row):
    return (row // 128) + ((row // 8) % 4) * 4 + (row % 8) * 16 + ((row // 32) % 4) * 128


def kernel(
    hid, gain_h, freq_h, wq, wk, wv, wo, post_h,
    out, lw_out,
    gain, freq, post, hid_v, np_v, wq_v, w_v, wo_v, kv, passing, q_s, st_o, st_m, st_l, att_p, att_n, att_all, lw_s,
    cos_s, sin_s, bias_c, bias_n, perm, sum_s, lsem, ssem, rsem,
):
    sp = lax.axis_index("sp")
    tp = lax.axis_index("tp")
    z, y = sp // NY, sp % NY
    x, core = tp // 2, tp % 2

    def start(src, dst, ridx, dev, kind):
        pltpu.make_async_remote_copy(
            src_ref=src, dst_ref=dst, send_sem=ssem.at[kind], recv_sem=rsem.at[ridx],
            device_id=dev, device_id_type=MESH,
        ).start()

    def finished(size, ridx, kind):
        return pltpu.make_async_remote_copy(
            src_ref=size, dst_ref=size, send_sem=ssem.at[kind], recv_sem=rsem.at[ridx],
            device_id=((sp + 1) % NSP, tp), device_id_type=MESH,
        )

    def arrived(dst, ridx):
        finished(dst, ridx, 0).wait_recv()

    def sent(size, kind):
        finished(size, 0, kind).wait_send()

    y_peer = [(z * NY + (y + d) % NY, tp) for d in range(NY)]
    z_peer = [(((z + d) % NZ) * NY + y, tp) for d in range(NZ)]
    ahead = ((sp + 1) % NSP, tp)
    behind = ((sp + NSP - 1) % NSP, tp)
    relay_of_me = (((z + y // 4) % NZ) * NY + (y + NY - 3) % NY, tp)
    source_y = (y + 3) % NY
    relay_source = (((z + NZ - source_y // 4) % NZ) * NY + source_y, tp)
    t_peer = [(sp, (tp + d) % NTP) for d in range(NTP)]
    x_right = (sp, (tp + 2) % NTP)
    x_left = (sp, (tp + NTP - 2) % NTP)
    sibling = (sp, x * 2 + (1 - core))

    local = [
        pltpu.make_async_copy(w.at[:, p * 128 : (p + 1) * 128], w_v.at[i, p, z, y], lsem.at[2 * p + i])
        for p in range(2)
        for i, w in enumerate((wk, wv))
    ] + [
        pltpu.make_async_copy(wo, wo_v.at[tp], lsem.at[4]),
        pltpu.make_async_copy(hid, hid_v, lsem.at[5]),
        pltpu.make_async_copy(wq, wq_v, lsem.at[6]),
        pltpu.make_async_copy(gain_h, gain, lsem.at[7]),
        pltpu.make_async_copy(freq_h, freq, lsem.at[8]),
        pltpu.make_async_copy(post_h, post, lsem.at[9]),
    ]
    for copy in local:
        copy.start()

    barrier = pltpu.get_barrier_semaphore()
    partners = y_peer[1:] + z_peer[1:] + t_peer[1:] + [ahead, behind, relay_of_me, relay_source]
    for dev in partners:
        pl.semaphore_signal(barrier, inc=1, device_id=dev, device_id_type=MESH)
    pl.semaphore_wait(barrier, len(partners))

    def weights_send(p):
        for i, peer in enumerate((y_peer, z_peer)):
            local[2 * p + i].wait()
            part = w_v.at[i, p, z, y]
            for d in (4, 3, 5, 2, 6, 1, 7):
                start(part, part, R_WD + i * 2 + p, peer[d], S_WD)

    def weights_wait(p):
        for i in range(2):
            arrived(w_v.at[i, p, 0, 0:7], R_WD + i * 2 + p)

    def relay_part(i, p, at, half):
        piece = pl.ds(half * 4, 4)
        return w_v.at[0, p, at, piece] if i == 0 else w_v.at[1, p, piece, at]

    def relay_sem(i, p, half, direction, hop):
        return R_WR + ((i * 2 + p) * 2 + half) * 7 + (hop if direction == 0 else 6 - hop)

    def relay_dev(i, direction):
        peer = z_peer if i == 0 else y_peer
        return peer[1] if direction == 0 else peer[7]

    def relay_order():
        for late in range(2):
            for i, at in enumerate((z, y)):
                for direction in range(2):
                    yield direction ^ late, i, at, direction, 4 - late

    def relay_send(p):
        for half, i, at, direction, _ in relay_order():
            part = relay_part(i, p, at, half)
            start(part, part, relay_sem(i, p, half, direction, 0), relay_dev(i, direction), S_WR)

    def relay_step(p, hop):
        for half, i, at, direction, hops in relay_order():
            if hop < hops:
                owner = (at + 7 - hop) % 8 if direction == 0 else (at + 1 + hop) % 8
                part = relay_part(i, p, owner, half)
                arrived(part, relay_sem(i, p, half, direction, hop))
                if hop + 1 < hops:
                    start(part, part, relay_sem(i, p, half, direction, hop + 1), relay_dev(i, direction), S_WR)

    def wo_part(delta, part):
        group = wo_v.at[(tp + delta) % NTP]
        return group if part is None else group.at[pl.ds(part * 128, 128)]

    def wo_send():
        local[4].wait()
        start(wo_part(0, 0), wo_part(0, 0), R_X + 0, x_right, S_X)
        start(wo_part(0, 1), wo_part(0, 1), R_X + 1, x_left, S_X)
        start(wo_part(0, 1), wo_part(0, 1), R_X + 2, x_right, S_X)
        start(wo_part(0, 0), wo_part(0, 0), R_X + 3, x_left, S_X)
        start(wo_part(0, None), wo_part(0, None), R_X + 6, sibling, S_X)

    def wo_step(k):
        if k == 0:
            arrived(wo_part(6, 0), R_X + 0)
            start(wo_part(6, 0), wo_part(6, 0), R_X + 4, x_right, S_X)
            start(wo_part(6, 0), wo_part(6, 0), R_X + 6, sibling, S_X)
            arrived(wo_part(2, 1), R_X + 1)
            start(wo_part(2, 1), wo_part(2, 1), R_X + 5, x_left, S_X)
            start(wo_part(2, 1), wo_part(2, 1), R_X + 6, sibling, S_X)
        elif k == 1:
            arrived(wo_part(6, 1), R_X + 2)
            start(wo_part(6, 1), wo_part(6, 1), R_X + 6, sibling, S_X)
            arrived(wo_part(2, 0), R_X + 3)
            start(wo_part(2, 0), wo_part(2, 0), R_X + 6, sibling, S_X)
        else:
            arrived(wo_part(4, 0), R_X + 4)
            start(wo_part(4, 0), wo_part(4, 0), R_X + 6, sibling, S_X)
            arrived(wo_part(4, 1), R_X + 5)
            start(wo_part(4, 1), wo_part(4, 1), R_X + 6, sibling, S_X)

    def wo_sibling_wait():
        arrived(wo_v.at[0:4], R_X + 6)

    def up_part(k, p, w):
        return kv.at[k, p, w, 0:AHEAD_ROWS]

    def down_part(k, p, w):
        return kv.at[k, p, w, AHEAD_ROWS:ROWS]

    def up_sem(p, k, w):
        return R_H + (p * (SLOTS - 1) + k - 1) * 2 + w

    def down_sem(p, k, w):
        return R_M + (p * SLOTS + k) * 2 + w

    def clear():
        for k in range(1, SLOTS):

            @pl.when(sp < k)
            def _():
                kv[k, :, :, 0:AHEAD_ROWS] = jnp.zeros((2, 2, AHEAD_ROWS, 128), BF16)

    def halo_send(p):
        @pl.when(sp < NSP - 1)
        def _():
            for w in range(2):
                start(up_part(0, p, w), up_part(1, p, w), up_sem(p, 1, w), ahead, S_H)

        for w in range(2):
            start(down_part(0, p, w), passing.at[p, w], down_sem(p, 0, w), relay_of_me, S_M)

    def up(p, k):
        for w in range(2):

            @pl.when(sp >= k)
            def _():
                arrived(up_part(k, p, w), up_sem(p, k, w))

            if k < SLOTS - 1:

                @pl.when((sp >= k) & (sp < NSP - 1))
                def _():
                    start(up_part(k, p, w), up_part(k + 1, p, w), up_sem(p, k + 1, w), ahead, S_H)

    def down(p, k):
        for w in range(2):
            if k == 0:
                arrived(passing.at[p, w], down_sem(p, 0, w))
                start(passing.at[p, w], down_part(4, p, w), down_sem(p, 4, w), y_peer[NY - 1], S_M)
            else:
                arrived(down_part(k, p, w), down_sem(p, k, w))
                if k > 1:
                    start(down_part(k, p, w), down_part(k - 1, p, w), down_sem(p, k - 1, w), behind, S_M)

    lane = lax.broadcasted_iota(jnp.int32, (1, 128), 1)
    first_head = lane < 64
    first_half = (lane % 64) < 32

    def norm():
        local[5].wait()
        local[7].wait()

        def step(i, _):
            rows = pl.ds(pl.multiple_of(i * 32, 32), 32)
            h = hid_v[rows, :].astype(F32)
            scale = lax.rsqrt(jnp.mean(h * h, axis=-1, keepdims=True) + EPS)
            hid_v[rows, :] = (h * scale * gain[...]).astype(BF16)
            return 0

        lax.fori_loop(0, ROWS // 32, step, 0)

    def permutation():
        token = token_of(lax.broadcasted_iota(jnp.int32, (ROWS, ROWS), 0))
        col = lax.broadcasted_iota(jnp.int32, (ROWS, ROWS), 1)
        perm[0] = (token == col).astype(F32).astype(BF16)
        row = lax.broadcasted_iota(jnp.int32, (ROWS, ROWS), 0)
        token_c = token_of(lax.broadcasted_iota(jnp.int32, (ROWS, ROWS), 1))
        perm[1] = (token_c == row).astype(F32).astype(BF16)

    def permute():
        def step(i, _):
            rows = pl.ds(pl.multiple_of(i * 128, 128), 128)
            for c in range(4):
                np_v[rows, c * 512 : (c + 1) * 512] = dot(perm[0, rows, :], hid_v[:, c * 512 : (c + 1) * 512]).astype(BF16)
            return 0

        lax.fori_loop(0, 4, step, 0, unroll=2)

    def tables():
        local[8].wait()
        token = token_of(lax.broadcasted_iota(jnp.int32, (ROWS, 128), 0))
        angle = (sp * ROWS + token).astype(F32) * freq[...]
        cos_s[...] = jnp.cos(angle)
        sine = jnp.sin(angle)
        sin_s[...] = jnp.where(first_half, -sine, sine)

    def biases():
        row = lax.broadcasted_iota(jnp.int32, (128, 128), 0)
        col = lax.broadcasted_iota(jnp.int32, (128, 128), 1)

        def class_token(r):
            return (r // 32) * 128 + (r % 8) * 16 + ((r // 8) % 4) * 4

        for k in range(SLOTS):
            delta = class_token(row) - class_token(col) + ROWS * k
            near = (delta >= 0) & (delta <= 4 * SPAN)
            far = (delta >= 0) & (delta <= 16 * SPAN) & ((row // 8) % 4 == (col // 8) % 4)
            bias = jnp.where(near & far, 1.0, jnp.where(near | far, 0.0, NEG))
            bias_c[:, k * 128 : (k + 1) * 128] = jnp.where(sp >= k, bias, NEG)

        def near_token(r):
            return (r // 32) + (r % 8) * 16 + ((r // 8) % 4) * 4

        delta = near_token(row) - near_token(col)
        own = jnp.where((delta >= 0) & (delta <= SPAN), 0.0, NEG)
        delta = delta + 128
        prev = jnp.where((delta >= 0) & (delta <= SPAN), 0.0, NEG)
        bias_n[0, :, 0:128] = jnp.where(sp >= 1, prev, NEG)
        bias_n[1, :, 0:128] = prev
        bias_n[0, :, 128:256] = own
        bias_n[1, :, 128:256] = own

    def rotate(u, rows):
        swapped = jnp.where(first_half, pltpu.roll(u, 96, 1), pltpu.roll(u, 32, 1))
        return (u * cos_s[rows, :] + swapped * sin_s[rows, :]).astype(BF16)

    def queries():
        local[6].wait()

        for r0 in range(0, ROWS, BIG):
            q = dot(np_v[r0 : r0 + BIG, :], wq_v[...])
            for r in range(BIG // 128):
                rows = slice(r0 + r * 128, r0 + r * 128 + 128)
                for p in range(2):
                    turned = rotate(q[r * 128 : r * 128 + 128, p * 128 : (p + 1) * 128], rows)
                    zero = jnp.zeros_like(turned)
                    q_s[p, r0 // 128 + r, 0:128, :] = jnp.where(first_head, turned, zero)
                    q_s[p, r0 // 128 + r, 128:256, :] = jnp.where(first_head, zero, turned)

    def keys_values(p):
        weights = jnp.concatenate([w_v[i, p].reshape(D, 128) for i in range(2)], axis=1)

        for r0 in range(0, ROWS, BIG):
            rows = slice(r0, r0 + BIG)
            both = dot(np_v[rows, :], weights)
            kv[0, p, 0, rows, :] = rotate(both[:, 0:128], rows)
            kv[0, p, 1, rows, :] = both[:, 128:256].astype(BF16)

    def near(p, first, last):
        def step(b, _):
            slot = (3 - b) // 3
            before = (b + 3) % 4
            state = [(r, pl.ds(pl.multiple_of(h * 128 + b * 32, 32), 32)) for h in range(2) for r in range(4)]

            def gathered(ref):
                return jnp.concatenate([ref[p, r, at, :] for r, at in state], axis=0)

            def scattered(ref, value):
                for i, (r, at) in enumerate(state):
                    ref[p, r, at, :] = value[i * 32 : (i + 1) * 32]

            def part(r, base):
                return pl.ds(pl.multiple_of(base + r * 128, 32), 32)

            k, v = (
                jnp.concatenate(
                    [kv[slot, p, w, part(r, before * 32), :] for r in range(4)]
                    + [kv[0, p, w, part(r, b * 32), :] for r in range(4)],
                    axis=0,
                )
                for w in range(2)
            )
            o, m, total = update(
                gathered(q_s), k, v, bias_n[jnp.minimum(b, 1)], (gathered(st_o), gathered(st_m), gathered(st_l))
            )
            scattered(st_o, o)
            scattered(st_m, m)
            scattered(st_l, total)
            return 0

        lax.fori_loop(first, last, step, 0, unroll=True)

    def update(q, k, v, bias, state):
        s = dot(q, k, NT) * SCALE2 + jnp.concatenate([bias, bias], axis=0)
        m = jnp.broadcast_to(jnp.max(s, axis=-1, keepdims=True), q.shape)
        if state is not None:
            m = jnp.maximum(m, state[1])
        e = jnp.exp2(s - jnp.concatenate([m] * (s.shape[1] // 128), axis=1))
        total = jnp.broadcast_to(jnp.sum(e, axis=-1, keepdims=True), q.shape)
        o = dot(e.astype(BF16), v)
        if state is not None:
            decay = jnp.exp2(state[1] - m)
            total = state[2] * decay + total
            o = state[0] * decay + o
        return o, m, total

    def far(p, first, last, slots):
        def step(r, _):
            rows = pl.ds(pl.multiple_of(r * 128, 128), 128)
            k, v = (jnp.concatenate([kv[s, p, w, rows, :] for s in slots], axis=0) for w in range(2))
            bias = bias_c[:, slots[0] * 128 : (slots[-1] + 1) * 128]
            state = None if slots[0] == 0 else (st_o[p, r], st_m[p, r], st_l[p, r])
            st_o[p, r], st_m[p, r], st_l[p, r] = update(q_s[p, r], k, v, bias, state)
            return 0

        lax.fori_loop(first, last, step, 0, unroll=True)

    def levels(p):
        for r in range(4):
            rows = slice(r * 128, (r + 1) * 128)
            level = st_m[p, r] * LN2 + jnp.log(st_l[p, r])
            both = jnp.where(lane == 2 * p, level[0:128], level[128:256])
            lw_s[rows, :] = both if p == 0 else jnp.where(lane < 2, lw_s[rows, :], both)

    def finish(p):
        for r in range(4):
            rows = slice(r * 128, (r + 1) * 128)
            o = st_o[p, r] / st_l[p, r]
            att_p[rows, :] = jnp.where(first_head, o[0:128], o[128:256]).astype(BF16)
        att_n[p] = dot(perm[1], att_p[...]).astype(BF16)
        att_all[p, tp] = att_n[p, pl.ds(pl.multiple_of(tp * OUT_ROWS, OUT_ROWS), OUT_ROWS), :]
        for d in (4, 3, 5, 2, 6, 1, 7):
            rows = pl.ds(pl.multiple_of(((tp + d) % NTP) * OUT_ROWS, OUT_ROWS), OUT_ROWS)
            start(att_n.at[p, rows], att_all.at[p, tp], R_A + p * d, t_peer[d], S_A)

    def log_weights():
        levels = jnp.transpose(lw_s[...])[0:8, :]
        high = levels.astype(BF16)
        rest = levels - high.astype(F32)
        mid = rest.astype(BF16)
        low = (rest - mid.astype(F32)).astype(BF16)
        natural = dot(high, perm[0]) + dot(mid, perm[0]) + dot(low, perm[0])
        lw_out[...] = natural[0:4, :]

    def project(d):
        g = (tp + NTP - d) % NTP
        if d == 1:
            arrived(att_all.at[0, 0:7], R_A)
        if d:
            arrived(att_all.at[1, g], R_A + d)
        a = jnp.concatenate([att_all[0, g], att_all[1, g]], axis=1)
        for c in range(2):
            cols = slice(c * 1024, c * 1024 + 1024)
            part = dot(a, wo_v[g, :, cols]).astype(BF16).astype(F32)
            sum_s[:, cols] = part if d == 0 else sum_s[:, cols] + part

    def output():
        local[9].wait()
        total = sum_s[...]
        scale = lax.rsqrt(jnp.mean(total * total, axis=-1, keepdims=True) + EPS)
        out[...] = (total * scale * post[...]).astype(BF16)

    weights_send(0)
    weights_send(1)
    wo_send()
    norm()
    permutation()
    clear()
    permute()
    weights_wait(0)
    relay_send(0)
    weights_wait(1)
    relay_send(1)
    tables()
    relay_step(0, 0)
    relay_step(1, 0)
    biases()
    relay_step(0, 1)
    relay_step(1, 1)
    relay_step(0, 2)
    relay_step(1, 2)
    wo_step(0)
    relay_step(0, 3)
    keys_values(0)
    halo_send(0)
    relay_step(1, 3)
    keys_values(1)
    halo_send(1)
    queries()
    far(0, 0, 4, (0,))
    near(0, 1, 4)
    up(0, 1)
    far(1, 0, 4, (0,))
    down(0, 0)
    up(1, 1)
    near(1, 1, 4)
    wo_step(1)
    down(1, 0)
    up(0, 2)
    far(0, 0, 2, (1, 2))
    down(0, 4)
    up(1, 2)
    far(1, 0, 2, (1, 2))
    down(1, 4)
    down(0, 3)
    up(0, 3)
    wo_step(2)
    down(1, 3)
    far(0, 3, 4, (3, 4))
    up(1, 3)
    far(1, 3, 4, (3, 4))
    down(0, 2)
    down(1, 2)
    up(0, 4)
    far(0, 0, 3, (3, 4))
    down(0, 1)
    far(0, 2, 4, (1, 2))
    near(0, 0, 1)
    finish(0)
    levels(0)
    up(1, 4)
    far(1, 0, 3, (3, 4))
    down(1, 1)
    far(1, 2, 4, (1, 2))
    near(1, 0, 1)
    finish(1)
    wo_sibling_wait()
    project(0)
    levels(1)
    log_weights()
    project(1)
    project(7)
    project(2)
    project(6)
    project(3)
    project(5)
    project(4)
    output()
    sent(w_v.at[0, 0, 0:4, 0:7], S_WD)
    sent(w_v.at[:, :, 0:7], S_WR)
    sent(wo_v.at[0:7], S_X)
    for k in range(SLOTS - 1):

        @pl.when((sp >= k) & (sp < NSP - 1))
        def _():
            sent(kv.at[k, :, :, 0:AHEAD_ROWS], S_H)

    sent(kv.at[:, :, :, AHEAD_ROWS:ROWS], S_M)
    sent(att_all.at[:, 0:7], S_A)


def hand_over(out_in, lw_in, out, lw_out):
    out[...] = out_in[...]
    lw_out[...] = lw_in[...]


def body(hidden_in, pre_gain, query_proj, key_proj, value_proj, out_proj, post_gain):
    half = np.arange(HEAD_DIM // 2, dtype=np.float32) * np.float32(2.0) / np.float32(HEAD_DIM)
    freq = np.tile(np.power(np.float64(ROPE_BASE), -half.astype(np.float64)).astype(np.float32), 4).reshape(1, 128)
    hbm = pl.BlockSpec(memory_space=pltpu.HBM)
    vmem = pl.BlockSpec(memory_space=pltpu.VMEM)
    results = pl.pallas_call(
        kernel,
        out_shape=(jax.ShapeDtypeStruct((OUT_ROWS, D), BF16), jax.ShapeDtypeStruct((4, ROWS), F32)),
        in_specs=[hbm] * 8,
        out_specs=(vmem, vmem),
        scratch_shapes=[
            pltpu.VMEM((1, D), F32),
            pltpu.VMEM((1, 128), F32),
            pltpu.VMEM((1, D), F32),
            pltpu.VMEM((ROWS, D), BF16),
            pltpu.VMEM((ROWS, D), BF16),
            pltpu.VMEM((D, WIDTH), BF16),
            pltpu.VMEM((2, 2, NZ, NY, D // NSP, 128), BF16),
            pltpu.VMEM((NTP, WIDTH, D), BF16),
            pltpu.VMEM((SLOTS, 2, 2, ROWS, 128), BF16),
            pltpu.VMEM((2, 2, ROWS - AHEAD_ROWS, 128), BF16),
            pltpu.VMEM((2, 4, 256, 128), BF16),
            pltpu.VMEM((2, 4, 256, 128), F32),
            pltpu.VMEM((2, 4, 256, 128), F32),
            pltpu.VMEM((2, 4, 256, 128), F32),
            pltpu.VMEM((ROWS, 128), BF16),
            pltpu.VMEM((2, ROWS, 128), BF16),
            pltpu.VMEM((2, NTP, OUT_ROWS, 128), BF16),
            pltpu.VMEM((ROWS, 128), F32),
            pltpu.VMEM((ROWS, 128), F32),
            pltpu.VMEM((ROWS, 128), F32),
            pltpu.VMEM((128, SLOTS * 128), F32),
            pltpu.VMEM((2, 128, 256), F32),
            pltpu.VMEM((2, ROWS, ROWS), BF16),
            pltpu.VMEM((OUT_ROWS, D), F32),
            pltpu.SemaphoreType.DMA((10,)),
            pltpu.SemaphoreType.DMA((6,)),
            pltpu.SemaphoreType.DMA((R_END,)),
        ],
        compiler_params=pltpu.CompilerParams(
            collective_id=0, has_side_effects=True, vmem_limit_bytes=53 * 1024 * 1024
        ),
        name="layer",
    )(*(
        pltpu.with_memory_space_constraint(a, pltpu.HBM)
        for a in (
            hidden_in, pre_gain.reshape(1, D), jnp.asarray(freq), query_proj, key_proj, value_proj, out_proj,
            post_gain.reshape(1, D),
        )
    ))
    return pl.pallas_call(
        hand_over,
        out_shape=(jax.ShapeDtypeStruct((OUT_ROWS, D), BF16), jax.ShapeDtypeStruct((4, ROWS), F32)),
        in_specs=[vmem, vmem],
        out_specs=(vmem, vmem),
        compiler_params=pltpu.CompilerParams(vmem_limit_bytes=4 * 1024 * 1024),
        name="hand_over",
    )(*results)


def solution(mesh):
    placed = (P("sp", None), P(), P(None, "tp"), P("sp", "tp"), P("sp", "tp"), P("tp", None), P())
    return jax.shard_map(
        body,
        mesh=mesh,
        in_specs=placed,
        out_specs=(P(("sp", "tp"), None), P("tp", "sp")),
        check_vma=False,
    )
```

```python
import functools
import math

import jax
import jax.numpy as jnp
import numpy as np
from jax import lax
from jax.experimental import pallas as pl
from jax.experimental.pallas import tpu as pltpu
from jax.sharding import PartitionSpec as P

HEAD_DIM = 64
SPAN = 128
EPS = 1e-06
ROPE_BASE = 10000.0
NY = 8
NZ = 8
NSP = NY * NZ
NTP = 8
NX = 4
ROWS = 512
D = 2048
WIDTH = 256
OUT_ROWS = 64
SLOTS = 5
NEG = -1e30
SCALE2 = math.log2(math.e) / 8.0
LN2 = math.log(2.0)
BIG = 512
F32 = jnp.float32
BF16 = jnp.bfloat16
MESH = pl.DeviceIdType.MESH

NT = (((1,), (1,)), ((), ()))
NN = (((1,), (0,)), ((), ()))

AHEAD_ROWS = 320

R_WD = 0
R_WR = R_WD + 4
R_X = R_WR + 2 * 2 * 2 * 7
R_H = R_X + 7
R_M = R_H + 4 * (SLOTS - 1)
R_A = R_M + 4 * SLOTS
R_END = R_A + 1 + (NTP - 1)
S_WD, S_WR, S_X, S_H, S_M, S_A = range(6)


def dot(a, b, dims=NN):
    return lax.dot_general(a, b, dims, preferred_element_type=F32)


def token_of(row):
    return (row // 128) + ((row // 8) % 4) * 4 + (row % 8) * 16 + ((row // 32) % 4) * 128


def kernel(
    hid, gain_h, freq_h, wq, wk, wv, wo, post_h,
    out, lw_out,
    gain, freq, post, hid_v, np_v, wq_v, w_v, wo_v, kv, passing, q_s, st_o, st_m, st_l, att_p, att_n, att_all, lw_s,
    cos_s, sin_s, bias_c, bias_n, perm, sum_s, lsem, ssem, rsem,
):
    sp = lax.axis_index("sp")
    tp = lax.axis_index("tp")
    z, y = sp // NY, sp % NY
    x, core = tp // 2, tp % 2

    def start(src, dst, ridx, dev, kind):
        pltpu.make_async_remote_copy(
            src_ref=src, dst_ref=dst, send_sem=ssem.at[kind], recv_sem=rsem.at[ridx],
            device_id=dev, device_id_type=MESH,
        ).start()

    def finished(size, ridx, kind):
        return pltpu.make_async_remote_copy(
            src_ref=size, dst_ref=size, send_sem=ssem.at[kind], recv_sem=rsem.at[ridx],
            device_id=((sp + 1) % NSP, tp), device_id_type=MESH,
        )

    def arrived(dst, ridx):
        finished(dst, ridx, 0).wait_recv()

    def sent(size, kind):
        finished(size, 0, kind).wait_send()

    y_peer = [(z * NY + (y + d) % NY, tp) for d in range(NY)]
    z_peer = [(((z + d) % NZ) * NY + y, tp) for d in range(NZ)]
    ahead = ((sp + 1) % NSP, tp)
    behind = ((sp + NSP - 1) % NSP, tp)
    relay_of_me = (((z + y // 4) % NZ) * NY + (y + NY - 3) % NY, tp)
    source_y = (y + 3) % NY
    relay_source = (((z + NZ - source_y // 4) % NZ) * NY + source_y, tp)
    t_peer = [(sp, (tp + d) % NTP) for d in range(NTP)]
    x_right = (sp, (tp + 2) % NTP)
    x_left = (sp, (tp + NTP - 2) % NTP)
    sibling = (sp, x * 2 + (1 - core))

    local = [
        pltpu.make_async_copy(w.at[:, p * 128 : (p + 1) * 128], w_v.at[i, p, z, y], lsem.at[2 * p + i])
        for p in range(2)
        for i, w in enumerate((wk, wv))
    ] + [
        pltpu.make_async_copy(wo, wo_v.at[tp], lsem.at[4]),
        pltpu.make_async_copy(hid, hid_v, lsem.at[5]),
        pltpu.make_async_copy(wq, wq_v, lsem.at[6]),
        pltpu.make_async_copy(gain_h, gain, lsem.at[7]),
        pltpu.make_async_copy(freq_h, freq, lsem.at[8]),
        pltpu.make_async_copy(post_h, post, lsem.at[9]),
    ]
    for copy in local:
        copy.start()

    barrier = pltpu.get_barrier_semaphore()
    partners = y_peer[1:] + z_peer[1:] + t_peer[1:] + [ahead, behind, relay_of_me, relay_source]
    for dev in partners:
        pl.semaphore_signal(barrier, inc=1, device_id=dev, device_id_type=MESH)
    pl.semaphore_wait(barrier, len(partners))

    def weights_send(p):
        for i, peer in enumerate((y_peer, z_peer)):
            local[2 * p + i].wait()
            part = w_v.at[i, p, z, y]
            for d in (4, 3, 5, 2, 6, 1, 7):
                start(part, part, R_WD + i * 2 + p, peer[d], S_WD)

    def weights_wait(p):
        for i in range(2):
            arrived(w_v.at[i, p, 0, 0:7], R_WD + i * 2 + p)

    def relay_part(i, p, at, half):
        piece = pl.ds(half * 4, 4)
        return w_v.at[0, p, at, piece] if i == 0 else w_v.at[1, p, piece, at]

    def relay_sem(i, p, half, direction, hop):
        return R_WR + ((i * 2 + p) * 2 + half) * 7 + (hop if direction == 0 else 6 - hop)

    def relay_dev(i, direction):
        peer = z_peer if i == 0 else y_peer
        return peer[1] if direction == 0 else peer[7]

    def relay_order():
        for late in range(2):
            for i, at in enumerate((z, y)):
                for direction in range(2):
                    yield direction ^ late, i, at, direction, 4 - late

    def relay_send(p):
        for half, i, at, direction, _ in relay_order():
            part = relay_part(i, p, at, half)
            start(part, part, relay_sem(i, p, half, direction, 0), relay_dev(i, direction), S_WR)

    def relay_step(p, hop):
        for half, i, at, direction, hops in relay_order():
            if hop < hops:
                owner = (at + 7 - hop) % 8 if direction == 0 else (at + 1 + hop) % 8
                part = relay_part(i, p, owner, half)
                arrived(part, relay_sem(i, p, half, direction, hop))
                if hop + 1 < hops:
                    start(part, part, relay_sem(i, p, half, direction, hop + 1), relay_dev(i, direction), S_WR)

    def wo_part(delta, part):
        group = wo_v.at[(tp + delta) % NTP]
        return group if part is None else group.at[pl.ds(part * 128, 128)]

    def wo_send():
        local[4].wait()
        start(wo_part(0, 0), wo_part(0, 0), R_X + 0, x_right, S_X)
        start(wo_part(0, 1), wo_part(0, 1), R_X + 1, x_left, S_X)
        start(wo_part(0, 1), wo_part(0, 1), R_X + 2, x_right, S_X)
        start(wo_part(0, 0), wo_part(0, 0), R_X + 3, x_left, S_X)
        start(wo_part(0, None), wo_part(0, None), R_X + 6, sibling, S_X)

    def wo_step(k):
        if k == 0:
            arrived(wo_part(6, 0), R_X + 0)
            start(wo_part(6, 0), wo_part(6, 0), R_X + 4, x_right, S_X)
            start(wo_part(6, 0), wo_part(6, 0), R_X + 6, sibling, S_X)
            arrived(wo_part(2, 1), R_X + 1)
            start(wo_part(2, 1), wo_part(2, 1), R_X + 5, x_left, S_X)
            start(wo_part(2, 1), wo_part(2, 1), R_X + 6, sibling, S_X)
        elif k == 1:
            arrived(wo_part(6, 1), R_X + 2)
            start(wo_part(6, 1), wo_part(6, 1), R_X + 6, sibling, S_X)
            arrived(wo_part(2, 0), R_X + 3)
            start(wo_part(2, 0), wo_part(2, 0), R_X + 6, sibling, S_X)
        else:
            arrived(wo_part(4, 0), R_X + 4)
            start(wo_part(4, 0), wo_part(4, 0), R_X + 6, sibling, S_X)
            arrived(wo_part(4, 1), R_X + 5)
            start(wo_part(4, 1), wo_part(4, 1), R_X + 6, sibling, S_X)

    def wo_sibling_wait():
        arrived(wo_v.at[0:4], R_X + 6)

    def up_part(k, p, w):
        return kv.at[k, p, w, 0:AHEAD_ROWS]

    def down_part(k, p, w):
        return kv.at[k, p, w, AHEAD_ROWS:ROWS]

    def up_sem(p, k, w):
        return R_H + (p * (SLOTS - 1) + k - 1) * 2 + w

    def down_sem(p, k, w):
        return R_M + (p * SLOTS + k) * 2 + w

    def clear():
        for k in range(1, SLOTS):

            @pl.when(sp < k)
            def _():
                kv[k, :, :, 0:AHEAD_ROWS] = jnp.zeros((2, 2, AHEAD_ROWS, 128), BF16)

            @pl.when(sp == k - 1)
            def _():
                kv[k, :, :, AHEAD_ROWS:ROWS] = jnp.zeros((2, 2, ROWS - AHEAD_ROWS, 128), BF16)

    def halo_send(p):
        @pl.when(sp < NSP - 1)
        def _():
            for w in range(2):
                start(up_part(0, p, w), up_part(1, p, w), up_sem(p, 1, w), ahead, S_H)

        @pl.when(sp != NSP - 1)
        def _():
            for w in range(2):
                start(down_part(0, p, w), passing.at[p, w], down_sem(p, 0, w), relay_of_me, S_M)

    def up(p, k):
        for w in range(2):

            @pl.when(sp >= k)
            def _():
                arrived(up_part(k, p, w), up_sem(p, k, w))

            if k < SLOTS - 1:

                @pl.when((sp >= k) & (sp < NSP - 1))
                def _():
                    start(up_part(k, p, w), up_part(k + 1, p, w), up_sem(p, k + 1, w), ahead, S_H)

    def down(p, k):
        @pl.when(sp != (4 if k == 0 else k - 1))
        def _():
            for w in range(2):
                if k == 0:
                    arrived(passing.at[p, w], down_sem(p, 0, w))
                    start(passing.at[p, w], down_part(4, p, w), down_sem(p, 4, w), y_peer[NY - 1], S_M)
                else:
                    arrived(down_part(k, p, w), down_sem(p, k, w))
                    if k > 1:
                        start(down_part(k, p, w), down_part(k - 1, p, w), down_sem(p, k - 1, w), behind, S_M)

    lane = lax.broadcasted_iota(jnp.int32, (1, 128), 1)
    first_head = lane < 64
    first_half = (lane % 64) < 32

    def norm():
        local[5].wait()
        local[7].wait()

        def step(i, _):
            rows = pl.ds(pl.multiple_of(i * 32, 32), 32)
            h = hid_v[rows, :].astype(F32)
            scale = lax.rsqrt(jnp.mean(h * h, axis=-1, keepdims=True) + EPS)
            hid_v[rows, :] = (h * scale * gain[...]).astype(BF16)
            return 0

        lax.fori_loop(0, ROWS // 32, step, 0)

    def permutation():
        token = token_of(lax.broadcasted_iota(jnp.int32, (ROWS, ROWS), 0))
        col = lax.broadcasted_iota(jnp.int32, (ROWS, ROWS), 1)
        perm[0] = (token == col).astype(F32).astype(BF16)
        row = lax.broadcasted_iota(jnp.int32, (ROWS, ROWS), 0)
        token_c = token_of(lax.broadcasted_iota(jnp.int32, (ROWS, ROWS), 1))
        perm[1] = (token_c == row).astype(F32).astype(BF16)

    def permute():
        def step(i, _):
            rows = pl.ds(pl.multiple_of(i * 128, 128), 128)
            for c in range(4):
                np_v[rows, c * 512 : (c + 1) * 512] = dot(perm[0, rows, :], hid_v[:, c * 512 : (c + 1) * 512]).astype(BF16)
            return 0

        lax.fori_loop(0, 4, step, 0, unroll=2)

    def tables():
        local[8].wait()
        token = token_of(lax.broadcasted_iota(jnp.int32, (ROWS, 128), 0))
        angle = (sp * ROWS + token).astype(F32) * freq[...]
        cos_s[...] = jnp.cos(angle)
        sine = jnp.sin(angle)
        sin_s[...] = jnp.where(first_half, -sine, sine)

    def biases():
        row = lax.broadcasted_iota(jnp.int32, (128, 128), 0)
        col = lax.broadcasted_iota(jnp.int32, (128, 128), 1)

        def class_token(r):
            return (r // 32) * 128 + (r % 8) * 16 + ((r // 8) % 4) * 4

        for k in range(SLOTS):
            delta = class_token(row) - class_token(col) + ROWS * k
            near = (delta >= 0) & (delta <= 4 * SPAN)
            far = (delta >= 0) & (delta <= 16 * SPAN) & ((row // 8) % 4 == (col // 8) % 4)
            bias = jnp.where(near & far, 1.0, jnp.where(near | far, 0.0, NEG))
            bias_c[:, k * 128 : (k + 1) * 128] = jnp.where(sp >= k, bias, NEG)

        def near_token(r):
            return (r // 32) + (r % 8) * 16 + ((r // 8) % 4) * 4

        delta = near_token(row) - near_token(col)
        own = jnp.where((delta >= 0) & (delta <= SPAN), 0.0, NEG)
        delta = delta + 128
        prev = jnp.where((delta >= 0) & (delta <= SPAN), 0.0, NEG)
        bias_n[0, :, 0:128] = jnp.where(sp >= 1, prev, NEG)
        bias_n[1, :, 0:128] = prev
        bias_n[0, :, 128:256] = own
        bias_n[1, :, 128:256] = own

    def rotate(u, rows):
        swapped = jnp.where(first_half, pltpu.roll(u, 96, 1), pltpu.roll(u, 32, 1))
        return (u * cos_s[rows, :] + swapped * sin_s[rows, :]).astype(BF16)

    def queries():
        local[6].wait()

        for r0 in range(0, ROWS, BIG):
            q = dot(np_v[r0 : r0 + BIG, :], wq_v[...])
            for r in range(BIG // 128):
                rows = slice(r0 + r * 128, r0 + r * 128 + 128)
                for p in range(2):
                    turned = rotate(q[r * 128 : r * 128 + 128, p * 128 : (p + 1) * 128], rows)
                    zero = jnp.zeros_like(turned)
                    q_s[p, r0 // 128 + r, 0:128, :] = jnp.where(first_head, turned, zero)
                    q_s[p, r0 // 128 + r, 128:256, :] = jnp.where(first_head, zero, turned)

    def keys_values(p):
        weights = jnp.concatenate([w_v[i, p].reshape(D, 128) for i in range(2)], axis=1)

        for r0 in range(0, ROWS, BIG):
            rows = slice(r0, r0 + BIG)
            both = dot(np_v[rows, :], weights)
            kv[0, p, 0, rows, :] = rotate(both[:, 0:128], rows)
            kv[0, p, 1, rows, :] = both[:, 128:256].astype(BF16)

    def near(p, first, last):
        def step(b, _):
            slot = (3 - b) // 3
            before = (b + 3) % 4
            state = [(r, pl.ds(pl.multiple_of(h * 128 + b * 32, 32), 32)) for h in range(2) for r in range(4)]

            def gathered(ref):
                return jnp.concatenate([ref[p, r, at, :] for r, at in state], axis=0)

            def scattered(ref, value):
                for i, (r, at) in enumerate(state):
                    ref[p, r, at, :] = value[i * 32 : (i + 1) * 32]

            def part(r, base):
                return pl.ds(pl.multiple_of(base + r * 128, 32), 32)

            k, v = (
                jnp.concatenate(
                    [kv[slot, p, w, part(r, before * 32), :] for r in range(4)]
                    + [kv[0, p, w, part(r, b * 32), :] for r in range(4)],
                    axis=0,
                )
                for w in range(2)
            )
            o, m, total = update(
                gathered(q_s), k, v, bias_n[jnp.minimum(b, 1)], (gathered(st_o), gathered(st_m), gathered(st_l))
            )
            scattered(st_o, o)
            scattered(st_m, m)
            scattered(st_l, total)
            return 0

        lax.fori_loop(first, last, step, 0, unroll=True)

    def update(q, k, v, bias, state):
        s = dot(q, k, NT) * SCALE2 + jnp.concatenate([bias, bias], axis=0)
        m = jnp.broadcast_to(jnp.max(s, axis=-1, keepdims=True), q.shape)
        if state is not None:
            m = jnp.maximum(m, state[1])
        e = jnp.exp2(s - jnp.concatenate([m] * (s.shape[1] // 128), axis=1))
        total = jnp.broadcast_to(jnp.sum(e, axis=-1, keepdims=True), q.shape)
        o = dot(e.astype(BF16), v)
        if state is not None:
            decay = jnp.exp2(state[1] - m)
            total = state[2] * decay + total
            o = state[0] * decay + o
        return o, m, total

    def far(p, first, last, slots):
        def step(r, _):
            rows = pl.ds(pl.multiple_of(r * 128, 128), 128)
            k, v = (jnp.concatenate([kv[s, p, w, rows, :] for s in slots], axis=0) for w in range(2))
            bias = bias_c[:, slots[0] * 128 : (slots[-1] + 1) * 128]
            state = None if slots[0] == 0 else (st_o[p, r], st_m[p, r], st_l[p, r])
            st_o[p, r], st_m[p, r], st_l[p, r] = update(q_s[p, r], k, v, bias, state)
            return 0

        lax.fori_loop(first, last, step, 0, unroll=True)

    def levels(p):
        for r in range(4):
            rows = slice(r * 128, (r + 1) * 128)
            level = st_m[p, r] * LN2 + jnp.log(st_l[p, r])
            both = jnp.where(lane == 2 * p, level[0:128], level[128:256])
            lw_s[rows, :] = both if p == 0 else jnp.where(lane < 2, lw_s[rows, :], both)

    def finish(p):
        for r in range(4):
            rows = slice(r * 128, (r + 1) * 128)
            o = st_o[p, r] / st_l[p, r]
            att_p[rows, :] = jnp.where(first_head, o[0:128], o[128:256]).astype(BF16)
        att_n[p] = dot(perm[1], att_p[...]).astype(BF16)
        att_all[p, tp] = att_n[p, pl.ds(pl.multiple_of(tp * OUT_ROWS, OUT_ROWS), OUT_ROWS), :]
        for d in (4, 3, 5, 2, 6, 1, 7):
            rows = pl.ds(pl.multiple_of(((tp + d) % NTP) * OUT_ROWS, OUT_ROWS), OUT_ROWS)
            start(att_n.at[p, rows], att_all.at[p, tp], R_A + p * d, t_peer[d], S_A)

    def log_weights():
        levels = jnp.transpose(lw_s[...])[0:8, :]
        high = levels.astype(BF16)
        rest = levels - high.astype(F32)
        mid = rest.astype(BF16)
        low = (rest - mid.astype(F32)).astype(BF16)
        natural = dot(high, perm[0]) + dot(mid, perm[0]) + dot(low, perm[0])
        lw_out[...] = natural[0:4, :]

    def project(d):
        g = (tp + NTP - d) % NTP
        if d == 1:
            arrived(att_all.at[0, 0:7], R_A)
        if d:
            arrived(att_all.at[1, g], R_A + d)
        a = jnp.concatenate([att_all[0, g], att_all[1, g]], axis=1)
        for c in range(2):
            cols = slice(c * 1024, c * 1024 + 1024)
            part = dot(a, wo_v[g, :, cols]).astype(BF16).astype(F32)
            sum_s[:, cols] = part if d == 0 else sum_s[:, cols] + part

    def output():
        local[9].wait()
        total = sum_s[...]
        scale = lax.rsqrt(jnp.mean(total * total, axis=-1, keepdims=True) + EPS)
        out[...] = (total * scale * post[...]).astype(BF16)

    weights_send(0)
    weights_send(1)
    wo_send()
    norm()
    permutation()
    clear()
    permute()
    weights_wait(0)
    relay_send(0)
    weights_wait(1)
    relay_send(1)
    tables()
    relay_step(0, 0)
    relay_step(1, 0)
    biases()
    relay_step(0, 1)
    relay_step(1, 1)
    relay_step(0, 2)
    relay_step(1, 2)
    wo_step(0)
    relay_step(0, 3)
    keys_values(0)
    halo_send(0)
    relay_step(1, 3)
    keys_values(1)
    halo_send(1)
    queries()
    far(0, 0, 4, (0,))
    near(0, 1, 4)
    up(0, 1)
    far(1, 0, 4, (0,))
    down(0, 0)
    up(1, 1)
    near(1, 1, 4)
    wo_step(1)
    down(1, 0)
    up(0, 2)
    far(0, 0, 2, (1, 2))
    down(0, 4)
    up(1, 2)
    far(1, 0, 2, (1, 2))
    down(1, 4)
    down(0, 3)
    up(0, 3)
    wo_step(2)
    down(1, 3)
    far(0, 3, 4, (3, 4))
    up(1, 3)
    far(1, 3, 4, (3, 4))
    down(0, 2)
    down(1, 2)
    up(0, 4)
    far(0, 0, 3, (3, 4))
    down(0, 1)
    far(0, 2, 4, (1, 2))
    near(0, 0, 1)
    finish(0)
    levels(0)
    up(1, 4)
    far(1, 0, 3, (3, 4))
    down(1, 1)
    far(1, 2, 4, (1, 2))
    near(1, 0, 1)
    finish(1)
    wo_sibling_wait()
    project(0)
    levels(1)
    log_weights()
    project(1)
    project(7)
    project(2)
    project(6)
    project(3)
    project(5)
    project(4)
    output()
    sent(w_v.at[0, 0, 0:4, 0:7], S_WD)
    sent(w_v.at[:, :, 0:7], S_WR)
    sent(wo_v.at[0:7], S_X)
    for k in range(SLOTS - 1):

        @pl.when((sp >= k) & (sp < NSP - 1))
        def _():
            sent(kv.at[k, :, :, 0:AHEAD_ROWS], S_H)

    one_short = (sp == NSP - 1) | ((sp >= 1) & (sp <= 4))

    @pl.when(one_short)
    def _():
        sent(kv.at[0:4, :, :, AHEAD_ROWS:ROWS], S_M)

    @pl.when(jnp.logical_not(one_short))
    def _():
        sent(kv.at[:, :, :, AHEAD_ROWS:ROWS], S_M)

    sent(att_all.at[:, 0:7], S_A)


def hand_over(out_in, lw_in, out, lw_out):
    out[...] = out_in[...]
    lw_out[...] = lw_in[...]


def body(hidden_in, pre_gain, query_proj, key_proj, value_proj, out_proj, post_gain):
    half = np.arange(HEAD_DIM // 2, dtype=np.float32) * np.float32(2.0) / np.float32(HEAD_DIM)
    freq = np.tile(np.power(np.float64(ROPE_BASE), -half.astype(np.float64)).astype(np.float32), 4).reshape(1, 128)
    hbm = pl.BlockSpec(memory_space=pltpu.HBM)
    vmem = pl.BlockSpec(memory_space=pltpu.VMEM)
    results = pl.pallas_call(
        kernel,
        out_shape=(jax.ShapeDtypeStruct((OUT_ROWS, D), BF16), jax.ShapeDtypeStruct((4, ROWS), F32)),
        in_specs=[hbm] * 8,
        out_specs=(vmem, vmem),
        scratch_shapes=[
            pltpu.VMEM((1, D), F32),
            pltpu.VMEM((1, 128), F32),
            pltpu.VMEM((1, D), F32),
            pltpu.VMEM((ROWS, D), BF16),
            pltpu.VMEM((ROWS, D), BF16),
            pltpu.VMEM((D, WIDTH), BF16),
            pltpu.VMEM((2, 2, NZ, NY, D // NSP, 128), BF16),
            pltpu.VMEM((NTP, WIDTH, D), BF16),
            pltpu.VMEM((SLOTS, 2, 2, ROWS, 128), BF16),
            pltpu.VMEM((2, 2, ROWS - AHEAD_ROWS, 128), BF16),
            pltpu.VMEM((2, 4, 256, 128), BF16),
            pltpu.VMEM((2, 4, 256, 128), F32),
            pltpu.VMEM((2, 4, 256, 128), F32),
            pltpu.VMEM((2, 4, 256, 128), F32),
            pltpu.VMEM((ROWS, 128), BF16),
            pltpu.VMEM((2, ROWS, 128), BF16),
            pltpu.VMEM((2, NTP, OUT_ROWS, 128), BF16),
            pltpu.VMEM((ROWS, 128), F32),
            pltpu.VMEM((ROWS, 128), F32),
            pltpu.VMEM((ROWS, 128), F32),
            pltpu.VMEM((128, SLOTS * 128), F32),
            pltpu.VMEM((2, 128, 256), F32),
            pltpu.VMEM((2, ROWS, ROWS), BF16),
            pltpu.VMEM((OUT_ROWS, D), F32),
            pltpu.SemaphoreType.DMA((10,)),
            pltpu.SemaphoreType.DMA((6,)),
            pltpu.SemaphoreType.DMA((R_END,)),
        ],
        compiler_params=pltpu.CompilerParams(
            collective_id=0, has_side_effects=True, vmem_limit_bytes=53 * 1024 * 1024
        ),
        name="layer",
    )(*(
        pltpu.with_memory_space_constraint(a, pltpu.HBM)
        for a in (
            hidden_in, pre_gain.reshape(1, D), jnp.asarray(freq), query_proj, key_proj, value_proj, out_proj,
            post_gain.reshape(1, D),
        )
    ))
    return pl.pallas_call(
        hand_over,
        out_shape=(jax.ShapeDtypeStruct((OUT_ROWS, D), BF16), jax.ShapeDtypeStruct((4, ROWS), F32)),
        in_specs=[vmem, vmem],
        out_specs=(vmem, vmem),
        compiler_params=pltpu.CompilerParams(vmem_limit_bytes=4 * 1024 * 1024),
        name="hand_over",
    )(*results)


def solution(mesh):
    placed = (P("sp", None), P(), P(None, "tp"), P("sp", "tp"), P("sp", "tp"), P("tp", None), P())
    return jax.shard_map(
        body,
        mesh=mesh,
        in_specs=placed,
        out_specs=(P(("sp", "tp"), None), P("tp", "sp")),
        check_vma=False,
    )
```

```python
import functools
import math

import jax
import jax.numpy as jnp
import numpy as np
from jax import lax
from jax.experimental import pallas as pl
from jax.experimental.pallas import tpu as pltpu
from jax.sharding import PartitionSpec as P

HEAD_DIM = 64
SPAN = 128
EPS = 1e-06
ROPE_BASE = 10000.0
NY = 8
NZ = 8
NSP = NY * NZ
NTP = 8
NX = 4
ROWS = 512
D = 2048
WIDTH = 256
OUT_ROWS = 64
SLOTS = 5
NEG = -1e30
SCALE2 = math.log2(math.e) / 8.0
LN2 = math.log(2.0)
BIG = 512
F32 = jnp.float32
BF16 = jnp.bfloat16
MESH = pl.DeviceIdType.MESH

NT = (((1,), (1,)), ((), ()))
NN = (((1,), (0,)), ((), ()))

AHEAD_ROWS = 320

R_WD = 0
R_WR = R_WD + 4
R_X = R_WR + 2 * 2 * 2 * 7
R_H = R_X + 7
R_M = R_H + 4 * (SLOTS - 1)
R_A = R_M + 4 * SLOTS
R_END = R_A + 1 + (NTP - 1)
S_WD, S_WR, S_X, S_H, S_M, S_A = range(6)


def dot(a, b, dims=NN):
    return lax.dot_general(a, b, dims, preferred_element_type=F32)


def token_of(row):
    return (row // 128) + ((row // 8) % 4) * 4 + (row % 8) * 16 + ((row // 32) % 4) * 128


def kernel(
    hid, gain_h, freq_h, wq, wk, wv, wo, post_h,
    out, lw_out,
    gain, freq, post, hid_v, np_v, wq_v, w_v, wo_v, kv, passing, q_s, st_o, st_m, st_l, att_p, att_n, att_all, lw_s,
    cos_s, sin_s, bias_c, bias_n, perm, sum_s, lsem, ssem, rsem,
):
    sp = lax.axis_index("sp")
    tp = lax.axis_index("tp")
    z, y = sp // NY, sp % NY
    x, core = tp // 2, tp % 2

    def start(src, dst, ridx, dev, kind):
        pltpu.make_async_remote_copy(
            src_ref=src, dst_ref=dst, send_sem=ssem.at[kind], recv_sem=rsem.at[ridx],
            device_id=dev, device_id_type=MESH,
        ).start()

    def finished(size, ridx, kind):
        return pltpu.make_async_remote_copy(
            src_ref=size, dst_ref=size, send_sem=ssem.at[kind], recv_sem=rsem.at[ridx],
            device_id=((sp + 1) % NSP, tp), device_id_type=MESH,
        )

    def arrived(dst, ridx):
        finished(dst, ridx, 0).wait_recv()

    def sent(size, kind):
        finished(size, 0, kind).wait_send()

    y_peer = [(z * NY + (y + d) % NY, tp) for d in range(NY)]
    z_peer = [(((z + d) % NZ) * NY + y, tp) for d in range(NZ)]
    ahead = ((sp + 1) % NSP, tp)
    behind = ((sp + NSP - 1) % NSP, tp)
    relay_of_me = (((z + y // 4) % NZ) * NY + (y + NY - 3) % NY, tp)
    source_y = (y + 3) % NY
    relay_source = (((z + NZ - source_y // 4) % NZ) * NY + source_y, tp)
    t_peer = [(sp, (tp + d) % NTP) for d in range(NTP)]
    x_right = (sp, (tp + 2) % NTP)
    x_left = (sp, (tp + NTP - 2) % NTP)
    sibling = (sp, x * 2 + (1 - core))

    local = [
        pltpu.make_async_copy(w.at[:, p * 128 : (p + 1) * 128], w_v.at[i, p, z, y], lsem.at[2 * p + i])
        for p in range(2)
        for i, w in enumerate((wk, wv))
    ] + [
        pltpu.make_async_copy(wo, wo_v.at[tp], lsem.at[4]),
        pltpu.make_async_copy(hid, hid_v, lsem.at[5]),
        pltpu.make_async_copy(wq, wq_v, lsem.at[6]),
        pltpu.make_async_copy(gain_h, gain, lsem.at[7]),
        pltpu.make_async_copy(freq_h, freq, lsem.at[8]),
        pltpu.make_async_copy(post_h, post, lsem.at[9]),
    ]
    barrier = pltpu.get_barrier_semaphore()
    partners = y_peer[1:] + z_peer[1:] + t_peer[1:] + [ahead, behind, relay_of_me, relay_source]
    for dev in partners:
        pl.semaphore_signal(barrier, inc=1, device_id=dev, device_id_type=MESH)
    for copy in local:
        copy.start()
    pl.semaphore_wait(barrier, len(partners))

    def weights_send(p):
        for i, peer in enumerate((y_peer, z_peer)):
            local[2 * p + i].wait()
            part = w_v.at[i, p, z, y]
            for d in (4, 3, 5, 2, 6, 1, 7):
                start(part, part, R_WD + i * 2 + p, peer[d], S_WD)

    def weights_wait(p):
        for i in range(2):
            arrived(w_v.at[i, p, 0, 0:7], R_WD + i * 2 + p)

    def relay_part(i, p, at, half):
        piece = pl.ds(half * 4, 4)
        return w_v.at[0, p, at, piece] if i == 0 else w_v.at[1, p, piece, at]

    def relay_sem(i, p, half, direction, hop):
        return R_WR + ((i * 2 + p) * 2 + half) * 7 + (hop if direction == 0 else 6 - hop)

    def relay_dev(i, direction):
        peer = z_peer if i == 0 else y_peer
        return peer[1] if direction == 0 else peer[7]

    def relay_order():
        for late in range(2):
            for i, at in enumerate((z, y)):
                for direction in range(2):
                    yield direction ^ late, i, at, direction, 4 - late

    def relay_send(p):
        for half, i, at, direction, _ in relay_order():
            part = relay_part(i, p, at, half)
            start(part, part, relay_sem(i, p, half, direction, 0), relay_dev(i, direction), S_WR)

    def relay_step(p, hop):
        for half, i, at, direction, hops in relay_order():
            if hop < hops:
                owner = (at + 7 - hop) % 8 if direction == 0 else (at + 1 + hop) % 8
                part = relay_part(i, p, owner, half)
                arrived(part, relay_sem(i, p, half, direction, hop))
                if hop + 1 < hops:
                    start(part, part, relay_sem(i, p, half, direction, hop + 1), relay_dev(i, direction), S_WR)

    def wo_part(delta, part):
        group = wo_v.at[(tp + delta) % NTP]
        return group if part is None else group.at[pl.ds(part * 128, 128)]

    def wo_send():
        local[4].wait()
        start(wo_part(0, 0), wo_part(0, 0), R_X + 0, x_right, S_X)
        start(wo_part(0, 1), wo_part(0, 1), R_X + 1, x_left, S_X)
        start(wo_part(0, 1), wo_part(0, 1), R_X + 2, x_right, S_X)
        start(wo_part(0, 0), wo_part(0, 0), R_X + 3, x_left, S_X)
        start(wo_part(0, None), wo_part(0, None), R_X + 6, sibling, S_X)

    def wo_step(k):
        if k == 0:
            arrived(wo_part(6, 0), R_X + 0)
            start(wo_part(6, 0), wo_part(6, 0), R_X + 4, x_right, S_X)
            start(wo_part(6, 0), wo_part(6, 0), R_X + 6, sibling, S_X)
            arrived(wo_part(2, 1), R_X + 1)
            start(wo_part(2, 1), wo_part(2, 1), R_X + 5, x_left, S_X)
            start(wo_part(2, 1), wo_part(2, 1), R_X + 6, sibling, S_X)
        elif k == 1:
            arrived(wo_part(6, 1), R_X + 2)
            start(wo_part(6, 1), wo_part(6, 1), R_X + 6, sibling, S_X)
            arrived(wo_part(2, 0), R_X + 3)
            start(wo_part(2, 0), wo_part(2, 0), R_X + 6, sibling, S_X)
        else:
            arrived(wo_part(4, 0), R_X + 4)
            start(wo_part(4, 0), wo_part(4, 0), R_X + 6, sibling, S_X)
            arrived(wo_part(4, 1), R_X + 5)
            start(wo_part(4, 1), wo_part(4, 1), R_X + 6, sibling, S_X)

    def wo_sibling_wait():
        arrived(wo_v.at[0:4], R_X + 6)

    def up_part(k, p, w):
        return kv.at[k, p, w, 0:AHEAD_ROWS]

    def down_part(k, p, w):
        return kv.at[k, p, w, AHEAD_ROWS:ROWS]

    def up_sem(p, k, w):
        return R_H + (p * (SLOTS - 1) + k - 1) * 2 + w

    def down_sem(p, k, w):
        return R_M + (p * SLOTS + k) * 2 + w

    def clear():
        for k in range(1, SLOTS):

            @pl.when(sp < k)
            def _():
                kv[k, :, :, 0:AHEAD_ROWS] = jnp.zeros((2, 2, AHEAD_ROWS, 128), BF16)

            @pl.when(sp == k - 1)
            def _():
                kv[k, :, :, AHEAD_ROWS:ROWS] = jnp.zeros((2, 2, ROWS - AHEAD_ROWS, 128), BF16)

    def up_send(p):
        @pl.when(sp < NSP - 1)
        def _():
            for w in range(2):
                start(up_part(0, p, w), up_part(1, p, w), up_sem(p, 1, w), ahead, S_H)

    def down_send(p):
        @pl.when(sp != NSP - 1)
        def _():
            for w in range(2):
                start(down_part(0, p, w), passing.at[p, w], down_sem(p, 0, w), relay_of_me, S_M)

    def up(p, k):
        for w in range(2):

            @pl.when(sp >= k)
            def _():
                arrived(up_part(k, p, w), up_sem(p, k, w))

            if k < SLOTS - 1:

                @pl.when((sp >= k) & (sp < NSP - 1))
                def _():
                    start(up_part(k, p, w), up_part(k + 1, p, w), up_sem(p, k + 1, w), ahead, S_H)

    def down(p, k):
        @pl.when(sp != (4 if k == 0 else k - 1))
        def _():
            for w in range(2):
                if k == 0:
                    arrived(passing.at[p, w], down_sem(p, 0, w))
                    start(passing.at[p, w], down_part(4, p, w), down_sem(p, 4, w), y_peer[NY - 1], S_M)
                else:
                    arrived(down_part(k, p, w), down_sem(p, k, w))
                    if k > 1:
                        start(down_part(k, p, w), down_part(k - 1, p, w), down_sem(p, k - 1, w), behind, S_M)

    lane = lax.broadcasted_iota(jnp.int32, (1, 128), 1)
    first_head = lane < 64
    first_half = (lane % 64) < 32

    def norm():
        local[5].wait()
        local[7].wait()

        def step(i, _):
            rows = pl.ds(pl.multiple_of(i * 32, 32), 32)
            h = hid_v[rows, :].astype(F32)
            scale = lax.rsqrt(jnp.mean(h * h, axis=-1, keepdims=True) + EPS)
            hid_v[rows, :] = (h * scale * gain[...]).astype(BF16)
            return 0

        lax.fori_loop(0, ROWS // 32, step, 0)

    def permutation():
        token = token_of(lax.broadcasted_iota(jnp.int32, (ROWS, ROWS), 0))
        col = lax.broadcasted_iota(jnp.int32, (ROWS, ROWS), 1)
        perm[0] = (token == col).astype(F32).astype(BF16)
        row = lax.broadcasted_iota(jnp.int32, (ROWS, ROWS), 0)
        token_c = token_of(lax.broadcasted_iota(jnp.int32, (ROWS, ROWS), 1))
        perm[1] = (token_c == row).astype(F32).astype(BF16)

    def permute():
        def step(i, _):
            rows = pl.ds(pl.multiple_of(i * 128, 128), 128)
            for c in range(4):
                np_v[rows, c * 512 : (c + 1) * 512] = dot(perm[0, rows, :], hid_v[:, c * 512 : (c + 1) * 512]).astype(BF16)
            return 0

        lax.fori_loop(0, 4, step, 0, unroll=2)

    def tables():
        local[8].wait()
        token = token_of(lax.broadcasted_iota(jnp.int32, (ROWS, 128), 0))
        angle = (sp * ROWS + token).astype(F32) * freq[...]
        cos_s[...] = jnp.cos(angle)
        sine = jnp.sin(angle)
        sin_s[...] = jnp.where(first_half, -sine, sine)

    def biases():
        row = lax.broadcasted_iota(jnp.int32, (128, 128), 0)
        col = lax.broadcasted_iota(jnp.int32, (128, 128), 1)

        def class_token(r):
            return (r // 32) * 128 + (r % 8) * 16 + ((r // 8) % 4) * 4

        for k in range(SLOTS):
            delta = class_token(row) - class_token(col) + ROWS * k
            near = (delta >= 0) & (delta <= 4 * SPAN)
            far = (delta >= 0) & (delta <= 16 * SPAN) & ((row // 8) % 4 == (col // 8) % 4)
            bias = jnp.where(near & far, 1.0, jnp.where(near | far, 0.0, NEG))
            bias_c[:, k * 128 : (k + 1) * 128] = jnp.where(sp >= k, bias, NEG)

        def near_token(r):
            return (r // 32) + (r % 8) * 16 + ((r // 8) % 4) * 4

        delta = near_token(row) - near_token(col)
        own = jnp.where((delta >= 0) & (delta <= SPAN), 0.0, NEG)
        delta = delta + 128
        prev = jnp.where((delta >= 0) & (delta <= SPAN), 0.0, NEG)
        bias_n[0, :, 0:128] = jnp.where(sp >= 1, prev, NEG)
        bias_n[1, :, 0:128] = prev
        bias_n[0, :, 128:256] = own
        bias_n[1, :, 128:256] = own

    def rotate(u, rows):
        swapped = jnp.where(first_half, pltpu.roll(u, 96, 1), pltpu.roll(u, 32, 1))
        return (u * cos_s[rows, :] + swapped * sin_s[rows, :]).astype(BF16)

    def queries():
        local[6].wait()

        for r0 in range(0, ROWS, BIG):
            q = dot(np_v[r0 : r0 + BIG, :], wq_v[...])
            for r in range(BIG // 128):
                rows = slice(r0 + r * 128, r0 + r * 128 + 128)
                for p in range(2):
                    turned = rotate(q[r * 128 : r * 128 + 128, p * 128 : (p + 1) * 128], rows)
                    zero = jnp.zeros_like(turned)
                    q_s[p, r0 // 128 + r, 0:128, :] = jnp.where(first_head, turned, zero)
                    q_s[p, r0 // 128 + r, 128:256, :] = jnp.where(first_head, zero, turned)

    def keys_values(p, first, last):
        weights = jnp.concatenate([w_v[i, p].reshape(D, 128) for i in range(2)], axis=1)

        for rows in (slice(first, last),):
            both = dot(np_v[rows, :], weights)
            kv[0, p, 0, rows, :] = rotate(both[:, 0:128], rows)
            kv[0, p, 1, rows, :] = both[:, 128:256].astype(BF16)

    def near(p, first, last):
        def step(b, _):
            slot = (3 - b) // 3
            before = (b + 3) % 4
            state = [(r, pl.ds(pl.multiple_of(h * 128 + b * 32, 32), 32)) for h in range(2) for r in range(4)]

            def gathered(ref):
                return jnp.concatenate([ref[p, r, at, :] for r, at in state], axis=0)

            def scattered(ref, value):
                for i, (r, at) in enumerate(state):
                    ref[p, r, at, :] = value[i * 32 : (i + 1) * 32]

            def part(r, base):
                return pl.ds(pl.multiple_of(base + r * 128, 32), 32)

            k, v = (
                jnp.concatenate(
                    [kv[slot, p, w, part(r, before * 32), :] for r in range(4)]
                    + [kv[0, p, w, part(r, b * 32), :] for r in range(4)],
                    axis=0,
                )
                for w in range(2)
            )
            o, m, total = update(
                gathered(q_s), k, v, bias_n[jnp.minimum(b, 1)], (gathered(st_o), gathered(st_m), gathered(st_l))
            )
            scattered(st_o, o)
            scattered(st_m, m)
            scattered(st_l, total)
            return 0

        lax.fori_loop(first, last, step, 0, unroll=True)

    def update(q, k, v, bias, state):
        s = dot(q, k, NT) * SCALE2 + jnp.concatenate([bias, bias], axis=0)
        m = jnp.broadcast_to(jnp.max(s, axis=-1, keepdims=True), q.shape)
        if state is not None:
            m = jnp.maximum(m, state[1])
        e = jnp.exp2(s - jnp.concatenate([m] * (s.shape[1] // 128), axis=1))
        total = jnp.broadcast_to(jnp.sum(e, axis=-1, keepdims=True), q.shape)
        o = dot(e.astype(BF16), v)
        if state is not None:
            decay = jnp.exp2(state[1] - m)
            total = state[2] * decay + total
            o = state[0] * decay + o
        return o, m, total

    def far(p, first, last, slots):
        def step(r, _):
            rows = pl.ds(pl.multiple_of(r * 128, 128), 128)
            k, v = (jnp.concatenate([kv[s, p, w, rows, :] for s in slots], axis=0) for w in range(2))
            bias = bias_c[:, slots[0] * 128 : (slots[-1] + 1) * 128]
            state = None if slots[0] == 0 else (st_o[p, r], st_m[p, r], st_l[p, r])
            st_o[p, r], st_m[p, r], st_l[p, r] = update(q_s[p, r], k, v, bias, state)
            return 0

        lax.fori_loop(first, last, step, 0, unroll=True)

    def levels(p):
        for r in range(4):
            rows = slice(r * 128, (r + 1) * 128)
            level = st_m[p, r] * LN2 + jnp.log(st_l[p, r])
            both = jnp.where(lane == 2 * p, level[0:128], level[128:256])
            lw_s[rows, :] = both if p == 0 else jnp.where(lane < 2, lw_s[rows, :], both)

    def finish(p):
        for r in range(4):
            rows = slice(r * 128, (r + 1) * 128)
            o = st_o[p, r] / st_l[p, r]
            att_p[rows, :] = jnp.where(first_head, o[0:128], o[128:256]).astype(BF16)
        att_n[p] = dot(perm[1], att_p[...]).astype(BF16)
        att_all[p, tp] = att_n[p, pl.ds(pl.multiple_of(tp * OUT_ROWS, OUT_ROWS), OUT_ROWS), :]
        for d in (4, 3, 5, 2, 6, 1, 7):
            rows = pl.ds(pl.multiple_of(((tp + d) % NTP) * OUT_ROWS, OUT_ROWS), OUT_ROWS)
            start(att_n.at[p, rows], att_all.at[p, tp], R_A + p * d, t_peer[d], S_A)

    def log_weights():
        levels = jnp.transpose(lw_s[...])[0:8, :]
        high = levels.astype(BF16)
        rest = levels - high.astype(F32)
        mid = rest.astype(BF16)
        low = (rest - mid.astype(F32)).astype(BF16)
        natural = dot(high, perm[0]) + dot(mid, perm[0]) + dot(low, perm[0])
        lw_out[...] = natural[0:4, :]

    def project(d):
        g = (tp + NTP - d) % NTP
        if d == 1:
            arrived(att_all.at[0, 0:7], R_A)
        if d:
            arrived(att_all.at[1, g], R_A + d)
        a = jnp.concatenate([att_all[0, g], att_all[1, g]], axis=1)
        for c in range(2):
            cols = slice(c * 1024, c * 1024 + 1024)
            part = dot(a, wo_v[g, :, cols]).astype(BF16).astype(F32)
            sum_s[:, cols] = part if d == 0 else sum_s[:, cols] + part

    def output():
        local[9].wait()
        total = sum_s[...]
        scale = lax.rsqrt(jnp.mean(total * total, axis=-1, keepdims=True) + EPS)
        out[...] = (total * scale * post[...]).astype(BF16)

    weights_send(0)
    weights_send(1)
    wo_send()
    norm()
    permutation()
    clear()
    permute()
    weights_wait(0)
    relay_send(0)
    weights_wait(1)
    relay_send(1)
    tables()
    relay_step(0, 0)
    relay_step(1, 0)
    biases()
    relay_step(0, 1)
    relay_step(1, 1)
    relay_step(0, 2)
    relay_step(1, 2)
    wo_step(0)
    relay_step(0, 3)
    keys_values(0, 0, AHEAD_ROWS)
    up_send(0)
    keys_values(0, AHEAD_ROWS, ROWS)
    down_send(0)
    relay_step(1, 3)
    keys_values(1, 0, ROWS)
    up_send(1)
    down_send(1)
    queries()
    far(0, 0, 4, (0,))
    near(0, 1, 4)
    up(0, 1)
    far(1, 0, 4, (0,))
    down(0, 0)
    up(1, 1)
    near(1, 1, 4)
    wo_step(1)
    down(1, 0)
    up(0, 2)
    far(0, 0, 2, (1, 2))
    down(0, 4)
    up(1, 2)
    far(1, 0, 2, (1, 2))
    down(1, 4)
    down(0, 3)
    up(0, 3)
    wo_step(2)
    down(1, 3)
    far(0, 3, 4, (3, 4))
    up(1, 3)
    far(1, 3, 4, (3, 4))
    down(0, 2)
    down(1, 2)
    up(0, 4)
    far(0, 0, 3, (3, 4))
    down(0, 1)
    far(0, 2, 4, (1, 2))
    near(0, 0, 1)
    finish(0)
    levels(0)
    up(1, 4)
    far(1, 0, 3, (3, 4))
    down(1, 1)
    far(1, 2, 4, (1, 2))
    near(1, 0, 1)
    finish(1)
    wo_sibling_wait()
    project(0)
    levels(1)
    log_weights()
    project(1)
    project(7)
    project(2)
    project(6)
    project(3)
    project(5)
    project(4)
    output()
    sent(w_v.at[0, 0, 0:4, 0:7], S_WD)
    sent(w_v.at[:, :, 0:7], S_WR)
    sent(wo_v.at[0:7], S_X)
    for k in range(SLOTS - 1):

        @pl.when((sp >= k) & (sp < NSP - 1))
        def _():
            sent(kv.at[k, :, :, 0:AHEAD_ROWS], S_H)

    one_short = (sp == NSP - 1) | ((sp >= 1) & (sp <= 4))

    @pl.when(one_short)
    def _():
        sent(kv.at[0:4, :, :, AHEAD_ROWS:ROWS], S_M)

    @pl.when(jnp.logical_not(one_short))
    def _():
        sent(kv.at[:, :, :, AHEAD_ROWS:ROWS], S_M)

    sent(att_all.at[:, 0:7], S_A)


def hand_over(out_in, lw_in, out, lw_out):
    out[...] = out_in[...]
    lw_out[...] = lw_in[...]


def body(hidden_in, pre_gain, query_proj, key_proj, value_proj, out_proj, post_gain):
    half = np.arange(HEAD_DIM // 2, dtype=np.float32) * np.float32(2.0) / np.float32(HEAD_DIM)
    freq = np.tile(np.power(np.float64(ROPE_BASE), -half.astype(np.float64)).astype(np.float32), 4).reshape(1, 128)
    hbm = pl.BlockSpec(memory_space=pltpu.HBM)
    vmem = pl.BlockSpec(memory_space=pltpu.VMEM)
    results = pl.pallas_call(
        kernel,
        out_shape=(jax.ShapeDtypeStruct((OUT_ROWS, D), BF16), jax.ShapeDtypeStruct((4, ROWS), F32)),
        in_specs=[hbm] * 8,
        out_specs=(vmem, vmem),
        scratch_shapes=[
            pltpu.VMEM((1, D), F32),
            pltpu.VMEM((1, 128), F32),
            pltpu.VMEM((1, D), F32),
            pltpu.VMEM((ROWS, D), BF16),
            pltpu.VMEM((ROWS, D), BF16),
            pltpu.VMEM((D, WIDTH), BF16),
            pltpu.VMEM((2, 2, NZ, NY, D // NSP, 128), BF16),
            pltpu.VMEM((NTP, WIDTH, D), BF16),
            pltpu.VMEM((SLOTS, 2, 2, ROWS, 128), BF16),
            pltpu.VMEM((2, 2, ROWS - AHEAD_ROWS, 128), BF16),
            pltpu.VMEM((2, 4, 256, 128), BF16),
            pltpu.VMEM((2, 4, 256, 128), F32),
            pltpu.VMEM((2, 4, 256, 128), F32),
            pltpu.VMEM((2, 4, 256, 128), F32),
            pltpu.VMEM((ROWS, 128), BF16),
            pltpu.VMEM((2, ROWS, 128), BF16),
            pltpu.VMEM((2, NTP, OUT_ROWS, 128), BF16),
            pltpu.VMEM((ROWS, 128), F32),
            pltpu.VMEM((ROWS, 128), F32),
            pltpu.VMEM((ROWS, 128), F32),
            pltpu.VMEM((128, SLOTS * 128), F32),
            pltpu.VMEM((2, 128, 256), F32),
            pltpu.VMEM((2, ROWS, ROWS), BF16),
            pltpu.VMEM((OUT_ROWS, D), F32),
            pltpu.SemaphoreType.DMA((10,)),
            pltpu.SemaphoreType.DMA((6,)),
            pltpu.SemaphoreType.DMA((R_END,)),
        ],
        compiler_params=pltpu.CompilerParams(
            collective_id=0, has_side_effects=True, vmem_limit_bytes=53 * 1024 * 1024
        ),
        name="layer",
    )(*(
        pltpu.with_memory_space_constraint(a, pltpu.HBM)
        for a in (
            hidden_in, pre_gain.reshape(1, D), jnp.asarray(freq), query_proj, key_proj, value_proj, out_proj,
            post_gain.reshape(1, D),
        )
    ))
    return pl.pallas_call(
        hand_over,
        out_shape=(jax.ShapeDtypeStruct((OUT_ROWS, D), BF16), jax.ShapeDtypeStruct((4, ROWS), F32)),
        in_specs=[vmem, vmem],
        out_specs=(vmem, vmem),
        compiler_params=pltpu.CompilerParams(vmem_limit_bytes=4 * 1024 * 1024),
        name="hand_over",
    )(*results)


def solution(mesh):
    placed = (P("sp", None), P(), P(None, "tp"), P("sp", "tp"), P("sp", "tp"), P("tp", None), P())
    return jax.shard_map(
        body,
        mesh=mesh,
        in_specs=placed,
        out_specs=(P(("sp", "tp"), None), P("tp", "sp")),
        check_vma=False,
    )
```

```python
import functools
import math

import jax
import jax.numpy as jnp
import numpy as np
from jax import lax
from jax.experimental import pallas as pl
from jax.experimental.pallas import tpu as pltpu
from jax.sharding import PartitionSpec as P

HEAD_DIM = 64
SPAN = 128
EPS = 1e-06
ROPE_BASE = 10000.0
NY = 8
NZ = 8
NSP = NY * NZ
NTP = 8
NX = 4
ROWS = 512
D = 2048
WIDTH = 256
OUT_ROWS = 64
SLOTS = 5
NEG = -1e30
SCALE2 = math.log2(math.e) / 8.0
LN2 = math.log(2.0)
BIG = 512
F32 = jnp.float32
BF16 = jnp.bfloat16
MESH = pl.DeviceIdType.MESH

NT = (((1,), (1,)), ((), ()))
NN = (((1,), (0,)), ((), ()))

AHEAD_ROWS = 320

R_WD = 0
R_WR = R_WD + 4
R_X = R_WR + 2 * 2 * 2 * 7
R_H = R_X + 7
R_M = R_H + 4 * (SLOTS - 1)
R_A = R_M + 4 * SLOTS
R_END = R_A + 1 + (NTP - 1)
S_WD, S_WR, S_X, S_H, S_M, S_A = range(6)


def dot(a, b, dims=NN):
    return lax.dot_general(a, b, dims, preferred_element_type=F32)


def token_of(row):
    return (row // 128) + ((row // 8) % 4) * 4 + (row % 8) * 16 + ((row // 32) % 4) * 128


def kernel(
    hid, gain_h, freq_h, wq, wk, wv, wo, post_h,
    out, lw_out,
    gain, freq, post, hid_v, np_v, wq_v, w_v, wo_v, kv, passing, q_s, st_o, st_m, st_l, att_p, att_n, att_all, lw_s,
    cos_s, sin_s, bias_c, bias_n, perm, sum_s, lsem, ssem, rsem,
):
    sp = lax.axis_index("sp")
    tp = lax.axis_index("tp")
    z, y = sp // NY, sp % NY
    x, core = tp // 2, tp % 2

    def start(src, dst, ridx, dev, kind):
        pltpu.make_async_remote_copy(
            src_ref=src, dst_ref=dst, send_sem=ssem.at[kind], recv_sem=rsem.at[ridx],
            device_id=dev, device_id_type=MESH,
        ).start()

    def finished(size, ridx, kind):
        return pltpu.make_async_remote_copy(
            src_ref=size, dst_ref=size, send_sem=ssem.at[kind], recv_sem=rsem.at[ridx],
            device_id=((sp + 1) % NSP, tp), device_id_type=MESH,
        )

    def arrived(dst, ridx):
        finished(dst, ridx, 0).wait_recv()

    def sent(size, kind):
        finished(size, 0, kind).wait_send()

    y_peer = [(z * NY + (y + d) % NY, tp) for d in range(NY)]
    z_peer = [(((z + d) % NZ) * NY + y, tp) for d in range(NZ)]
    ahead = ((sp + 1) % NSP, tp)
    behind = ((sp + NSP - 1) % NSP, tp)
    relay_of_me = (((z + y // 4) % NZ) * NY + (y + NY - 3) % NY, tp)
    source_y = (y + 3) % NY
    relay_source = (((z + NZ - source_y // 4) % NZ) * NY + source_y, tp)
    t_peer = [(sp, (tp + d) % NTP) for d in range(NTP)]
    x_right = (sp, (tp + 2) % NTP)
    x_left = (sp, (tp + NTP - 2) % NTP)
    sibling = (sp, x * 2 + (1 - core))

    local = [
        pltpu.make_async_copy(w.at[:, p * 128 : (p + 1) * 128], w_v.at[i, p, z, y], lsem.at[2 * p + i])
        for p in range(2)
        for i, w in enumerate((wk, wv))
    ] + [
        pltpu.make_async_copy(wo, wo_v.at[tp], lsem.at[4]),
        pltpu.make_async_copy(hid, hid_v, lsem.at[5]),
        pltpu.make_async_copy(wq, wq_v, lsem.at[6]),
        pltpu.make_async_copy(gain_h, gain, lsem.at[7]),
        pltpu.make_async_copy(freq_h, freq, lsem.at[8]),
        pltpu.make_async_copy(post_h, post, lsem.at[9]),
    ]
    barrier = pltpu.get_barrier_semaphore()
    partners = y_peer[1:] + z_peer[1:] + t_peer[1:] + [ahead, behind, relay_of_me, relay_source]
    for dev in partners:
        pl.semaphore_signal(barrier, inc=1, device_id=dev, device_id_type=MESH)
    for copy in local:
        copy.start()
    pl.semaphore_wait(barrier, len(partners))

    def weights_send(p):
        for i, peer in enumerate((y_peer, z_peer)):
            local[2 * p + i].wait()
            part = w_v.at[i, p, z, y]
            for d in (4, 3, 5, 2, 6, 1, 7):
                start(part, part, R_WD + i * 2 + p, peer[d], S_WD)

    def weights_wait(p):
        for i in range(2):
            arrived(w_v.at[i, p, 0, 0:7], R_WD + i * 2 + p)

    def relay_part(i, p, at, half):
        piece = pl.ds(half * 4, 4)
        return w_v.at[0, p, at, piece] if i == 0 else w_v.at[1, p, piece, at]

    def relay_sem(i, p, half, direction, hop):
        return R_WR + ((i * 2 + p) * 2 + half) * 7 + (hop if direction == 0 else 6 - hop)

    def relay_dev(i, direction):
        peer = z_peer if i == 0 else y_peer
        return peer[1] if direction == 0 else peer[7]

    def relay_order():
        for late in range(2):
            for i, at in enumerate((z, y)):
                for direction in range(2):
                    yield direction ^ late, i, at, direction, 4 - late

    def relay_send(p):
        for half, i, at, direction, _ in relay_order():
            part = relay_part(i, p, at, half)
            start(part, part, relay_sem(i, p, half, direction, 0), relay_dev(i, direction), S_WR)

    def relay_step(p, hop):
        for half, i, at, direction, hops in relay_order():
            if hop < hops:
                owner = (at + 7 - hop) % 8 if direction == 0 else (at + 1 + hop) % 8
                part = relay_part(i, p, owner, half)
                arrived(part, relay_sem(i, p, half, direction, hop))
                if hop + 1 < hops:
                    start(part, part, relay_sem(i, p, half, direction, hop + 1), relay_dev(i, direction), S_WR)

    def wo_part(delta, part):
        group = wo_v.at[(tp + delta) % NTP]
        return group if part is None else group.at[pl.ds(part * 128, 128)]

    def wo_send():
        local[4].wait()
        start(wo_part(0, 0), wo_part(0, 0), R_X + 0, x_right, S_X)
        start(wo_part(0, 1), wo_part(0, 1), R_X + 1, x_left, S_X)
        start(wo_part(0, 1), wo_part(0, 1), R_X + 2, x_right, S_X)
        start(wo_part(0, 0), wo_part(0, 0), R_X + 3, x_left, S_X)
        start(wo_part(0, None), wo_part(0, None), R_X + 6, sibling, S_X)

    def wo_step(k):
        if k == 0:
            arrived(wo_part(6, 0), R_X + 0)
            start(wo_part(6, 0), wo_part(6, 0), R_X + 4, x_right, S_X)
            start(wo_part(6, 0), wo_part(6, 0), R_X + 6, sibling, S_X)
            arrived(wo_part(2, 1), R_X + 1)
            start(wo_part(2, 1), wo_part(2, 1), R_X + 5, x_left, S_X)
            start(wo_part(2, 1), wo_part(2, 1), R_X + 6, sibling, S_X)
        elif k == 1:
            arrived(wo_part(6, 1), R_X + 2)
            start(wo_part(6, 1), wo_part(6, 1), R_X + 6, sibling, S_X)
            arrived(wo_part(2, 0), R_X + 3)
            start(wo_part(2, 0), wo_part(2, 0), R_X + 6, sibling, S_X)
        else:
            arrived(wo_part(4, 0), R_X + 4)
            start(wo_part(4, 0), wo_part(4, 0), R_X + 6, sibling, S_X)
            arrived(wo_part(4, 1), R_X + 5)
            start(wo_part(4, 1), wo_part(4, 1), R_X + 6, sibling, S_X)

    def wo_sibling_wait():
        arrived(wo_v.at[0:4], R_X + 6)

    def up_part(k, p, w):
        return kv.at[k, p, w, 0:AHEAD_ROWS]

    def down_part(k, p, w):
        return kv.at[k, p, w, AHEAD_ROWS:ROWS]

    def up_sem(p, k, w):
        return R_H + (p * (SLOTS - 1) + k - 1) * 2 + w

    def down_sem(p, k, w):
        return R_M + (p * SLOTS + k) * 2 + w

    def clear():
        for k in range(1, SLOTS):

            @pl.when(sp < k)
            def _():
                kv[k, :, :, 0:AHEAD_ROWS] = jnp.zeros((2, 2, AHEAD_ROWS, 128), BF16)

            @pl.when(sp == k - 1)
            def _():
                kv[k, :, :, AHEAD_ROWS:ROWS] = jnp.zeros((2, 2, ROWS - AHEAD_ROWS, 128), BF16)

    def up_send(p):
        @pl.when(sp < NSP - 1)
        def _():
            for w in range(2):
                start(up_part(0, p, w), up_part(1, p, w), up_sem(p, 1, w), ahead, S_H)

    def down_send(p):
        @pl.when(sp != NSP - 1)
        def _():
            for w in range(2):
                start(down_part(0, p, w), passing.at[p, w], down_sem(p, 0, w), relay_of_me, S_M)

    def up(p, k):
        for w in range(2):

            @pl.when(sp >= k)
            def _():
                arrived(up_part(k, p, w), up_sem(p, k, w))

            if k < SLOTS - 1:

                @pl.when((sp >= k) & (sp < NSP - 1))
                def _():
                    start(up_part(k, p, w), up_part(k + 1, p, w), up_sem(p, k + 1, w), ahead, S_H)

    def down(p, k):
        @pl.when(sp != (4 if k == 0 else k - 1))
        def _():
            for w in range(2):
                if k == 0:
                    arrived(passing.at[p, w], down_sem(p, 0, w))
                    start(passing.at[p, w], down_part(4, p, w), down_sem(p, 4, w), y_peer[NY - 1], S_M)
                else:
                    arrived(down_part(k, p, w), down_sem(p, k, w))
                    if k > 1:
                        start(down_part(k, p, w), down_part(k - 1, p, w), down_sem(p, k - 1, w), behind, S_M)

    lane = lax.broadcasted_iota(jnp.int32, (1, 128), 1)
    first_head = lane < 64
    first_half = (lane % 64) < 32

    def norm():
        local[5].wait()
        local[7].wait()

        def step(i, _):
            rows = pl.ds(pl.multiple_of(i * 32, 32), 32)
            h = hid_v[rows, :].astype(F32)
            scale = lax.rsqrt(jnp.mean(h * h, axis=-1, keepdims=True) + EPS)
            hid_v[rows, :] = (h * scale * gain[...]).astype(BF16)
            return 0

        lax.fori_loop(0, ROWS // 32, step, 0)

    def permutation():
        token = token_of(lax.broadcasted_iota(jnp.int32, (ROWS, ROWS), 0))
        col = lax.broadcasted_iota(jnp.int32, (ROWS, ROWS), 1)
        perm[0] = (token == col).astype(F32).astype(BF16)
        row = lax.broadcasted_iota(jnp.int32, (ROWS, ROWS), 0)
        token_c = token_of(lax.broadcasted_iota(jnp.int32, (ROWS, ROWS), 1))
        perm[1] = (token_c == row).astype(F32).astype(BF16)

    def permute():
        def step(i, _):
            rows = pl.ds(pl.multiple_of(i * 128, 128), 128)
            for c in range(4):
                np_v[rows, c * 512 : (c + 1) * 512] = dot(perm[0, rows, :], hid_v[:, c * 512 : (c + 1) * 512]).astype(BF16)
            return 0

        lax.fori_loop(0, 4, step, 0, unroll=2)

    def tables():
        local[8].wait()
        token = token_of(lax.broadcasted_iota(jnp.int32, (ROWS, 128), 0))
        angle = (sp * ROWS + token).astype(F32) * freq[...]
        cos_s[...] = jnp.cos(angle)
        sine = jnp.sin(angle)
        sin_s[...] = jnp.where(first_half, -sine, sine)

    def biases():
        row = lax.broadcasted_iota(jnp.int32, (128, 128), 0)
        col = lax.broadcasted_iota(jnp.int32, (128, 128), 1)

        def class_token(r):
            return (r // 32) * 128 + (r % 8) * 16 + ((r // 8) % 4) * 4

        for k in range(SLOTS):
            delta = class_token(row) - class_token(col) + ROWS * k
            near = (delta >= 0) & (delta <= 4 * SPAN)
            far = (delta >= 0) & (delta <= 16 * SPAN) & ((row // 8) % 4 == (col // 8) % 4)
            bias = jnp.where(near & far, 1.0, jnp.where(near | far, 0.0, NEG))
            bias_c[:, k * 128 : (k + 1) * 128] = jnp.where(sp >= k, bias, NEG)

        def near_token(r):
            return (r // 32) + (r % 8) * 16 + ((r // 8) % 4) * 4

        delta = near_token(row) - near_token(col)
        own = jnp.where((delta >= 0) & (delta <= SPAN), 0.0, NEG)
        delta = delta + 128
        prev = jnp.where((delta >= 0) & (delta <= SPAN), 0.0, NEG)
        bias_n[0, :, 0:128] = jnp.where(sp >= 1, prev, NEG)
        bias_n[1, :, 0:128] = prev
        bias_n[0, :, 128:256] = own
        bias_n[1, :, 128:256] = own

    def rotate(u, rows):
        swapped = jnp.where(first_half, pltpu.roll(u, 96, 1), pltpu.roll(u, 32, 1))
        return (u * cos_s[rows, :] + swapped * sin_s[rows, :]).astype(BF16)

    def queries():
        local[6].wait()

        for r0 in range(0, ROWS, BIG):
            q = dot(np_v[r0 : r0 + BIG, :], wq_v[...])
            for r in range(BIG // 128):
                rows = slice(r0 + r * 128, r0 + r * 128 + 128)
                for p in range(2):
                    turned = rotate(q[r * 128 : r * 128 + 128, p * 128 : (p + 1) * 128], rows)
                    zero = jnp.zeros_like(turned)
                    q_s[p, r0 // 128 + r, 0:128, :] = jnp.where(first_head, turned, zero)
                    q_s[p, r0 // 128 + r, 128:256, :] = jnp.where(first_head, zero, turned)

    def keys_values(p, first, last):
        weights = jnp.concatenate([w_v[i, p].reshape(D, 128) for i in range(2)], axis=1)

        for rows in (slice(first, last),):
            both = dot(np_v[rows, :], weights)
            kv[0, p, 0, rows, :] = rotate(both[:, 0:128], rows)
            kv[0, p, 1, rows, :] = both[:, 128:256].astype(BF16)

    def near(p, first, last):
        def step(b, _):
            slot = (3 - b) // 3
            before = (b + 3) % 4
            state = [(r, pl.ds(pl.multiple_of(h * 128 + b * 32, 32), 32)) for h in range(2) for r in range(4)]

            def gathered(ref):
                return jnp.concatenate([ref[p, r, at, :] for r, at in state], axis=0)

            def scattered(ref, value):
                for i, (r, at) in enumerate(state):
                    ref[p, r, at, :] = value[i * 32 : (i + 1) * 32]

            def part(r, base):
                return pl.ds(pl.multiple_of(base + r * 128, 32), 32)

            k, v = (
                jnp.concatenate(
                    [kv[slot, p, w, part(r, before * 32), :] for r in range(4)]
                    + [kv[0, p, w, part(r, b * 32), :] for r in range(4)],
                    axis=0,
                )
                for w in range(2)
            )
            o, m, total = update(
                gathered(q_s), k, v, bias_n[jnp.minimum(b, 1)], (gathered(st_o), gathered(st_m), gathered(st_l))
            )
            scattered(st_o, o)
            scattered(st_m, m)
            scattered(st_l, total)
            return 0

        lax.fori_loop(first, last, step, 0, unroll=True)

    def update(q, k, v, bias, state):
        s = dot(q, k, NT) * SCALE2 + jnp.concatenate([bias, bias], axis=0)
        m = jnp.broadcast_to(jnp.max(s, axis=-1, keepdims=True), q.shape)
        if state is not None:
            m = jnp.maximum(m, state[1])
        e = jnp.exp2(s - jnp.concatenate([m] * (s.shape[1] // 128), axis=1))
        total = jnp.broadcast_to(jnp.sum(e, axis=-1, keepdims=True), q.shape)
        o = dot(e.astype(BF16), v)
        if state is not None:
            decay = jnp.exp2(state[1] - m)
            total = state[2] * decay + total
            o = state[0] * decay + o
        return o, m, total

    def far(p, first, last, slots):
        def step(r, _):
            rows = pl.ds(pl.multiple_of(r * 128, 128), 128)
            k, v = (jnp.concatenate([kv[s, p, w, rows, :] for s in slots], axis=0) for w in range(2))
            bias = bias_c[:, slots[0] * 128 : (slots[-1] + 1) * 128]
            state = None if slots[0] == 0 else (st_o[p, r], st_m[p, r], st_l[p, r])
            st_o[p, r], st_m[p, r], st_l[p, r] = update(q_s[p, r], k, v, bias, state)
            return 0

        lax.fori_loop(first, last, step, 0, unroll=True)

    def levels(p):
        for r in range(4):
            rows = slice(r * 128, (r + 1) * 128)
            level = st_m[p, r] * LN2 + jnp.log(st_l[p, r])
            both = jnp.where(lane == 2 * p, level[0:128], level[128:256])
            lw_s[rows, :] = both if p == 0 else jnp.where(lane < 2, lw_s[rows, :], both)

    def finish(p):
        for r in range(4):
            rows = slice(r * 128, (r + 1) * 128)
            o = st_o[p, r] / st_l[p, r]
            att_p[rows, :] = jnp.where(first_head, o[0:128], o[128:256]).astype(BF16)
        att_n[p] = dot(perm[1], att_p[...]).astype(BF16)
        att_all[p, tp] = att_n[p, pl.ds(pl.multiple_of(tp * OUT_ROWS, OUT_ROWS), OUT_ROWS), :]
        for d in (4, 3, 5, 2, 6, 1, 7):
            rows = pl.ds(pl.multiple_of(((tp + d) % NTP) * OUT_ROWS, OUT_ROWS), OUT_ROWS)
            start(att_n.at[p, rows], att_all.at[p, tp], R_A + p * d, t_peer[d], S_A)

    def log_weights():
        levels = jnp.transpose(lw_s[...])[0:8, :]
        high = levels.astype(BF16)
        rest = levels - high.astype(F32)
        mid = rest.astype(BF16)
        low = (rest - mid.astype(F32)).astype(BF16)
        natural = dot(high, perm[0]) + dot(mid, perm[0]) + dot(low, perm[0])
        lw_out[...] = natural[0:4, :]

    def project(d):
        g = (tp + NTP - d) % NTP
        if d == 1:
            arrived(att_all.at[0, 0:7], R_A)
        if d:
            arrived(att_all.at[1, g], R_A + d)
        a = jnp.concatenate([att_all[0, g], att_all[1, g]], axis=1)
        for c in range(2):
            cols = slice(c * 1024, c * 1024 + 1024)
            part = dot(a, wo_v[g, :, cols]).astype(BF16).astype(F32)
            sum_s[:, cols] = part if d == 0 else sum_s[:, cols] + part

    def output():
        local[9].wait()
        total = sum_s[...]
        scale = lax.rsqrt(jnp.mean(total * total, axis=-1, keepdims=True) + EPS)
        out[...] = (total * scale * post[...]).astype(BF16)

    weights_send(0)
    weights_send(1)
    wo_send()
    norm()
    permutation()
    clear()
    permute()
    weights_wait(0)
    relay_send(0)
    weights_wait(1)
    relay_send(1)
    tables()
    relay_step(0, 0)
    relay_step(1, 0)
    biases()
    relay_step(0, 1)
    relay_step(1, 1)
    relay_step(0, 2)
    relay_step(1, 2)
    wo_step(0)
    relay_step(0, 3)
    keys_values(0, 0, AHEAD_ROWS)
    up_send(0)
    keys_values(0, AHEAD_ROWS, ROWS)
    down_send(0)
    relay_step(1, 3)
    keys_values(1, 0, ROWS)
    up_send(1)
    down_send(1)
    queries()
    far(0, 0, 4, (0,))
    near(0, 1, 4)
    up(0, 1)
    far(1, 0, 4, (0,))
    down(0, 0)
    up(1, 1)
    near(1, 1, 4)
    wo_step(1)
    down(1, 0)
    up(0, 2)
    far(0, 0, 2, (1, 2))
    down(0, 4)
    down(1, 4)
    up(1, 2)
    far(1, 0, 2, (1, 2))
    down(0, 3)
    down(1, 3)
    up(0, 3)
    wo_step(2)
    far(0, 3, 4, (3, 4))
    far(1, 3, 4, (3, 4))
    down(0, 2)
    up(1, 3)
    down(1, 2)
    up(0, 4)
    far(0, 0, 3, (3, 4))
    down(0, 1)
    far(0, 2, 4, (1, 2))
    near(0, 0, 1)
    finish(0)
    levels(0)
    up(1, 4)
    far(1, 0, 3, (3, 4))
    down(1, 1)
    far(1, 2, 4, (1, 2))
    near(1, 0, 1)
    finish(1)
    wo_sibling_wait()
    project(0)
    levels(1)
    log_weights()
    project(1)
    project(7)
    project(2)
    project(6)
    project(3)
    project(5)
    project(4)
    output()
    sent(w_v.at[0, 0, 0:4, 0:7], S_WD)
    sent(w_v.at[:, :, 0:7], S_WR)
    sent(wo_v.at[0:7], S_X)
    for k in range(SLOTS - 1):

        @pl.when((sp >= k) & (sp < NSP - 1))
        def _():
            sent(kv.at[k, :, :, 0:AHEAD_ROWS], S_H)

    one_short = (sp == NSP - 1) | ((sp >= 1) & (sp <= 4))

    @pl.when(one_short)
    def _():
        sent(kv.at[0:4, :, :, AHEAD_ROWS:ROWS], S_M)

    @pl.when(jnp.logical_not(one_short))
    def _():
        sent(kv.at[:, :, :, AHEAD_ROWS:ROWS], S_M)

    sent(att_all.at[:, 0:7], S_A)


def hand_over(out_in, lw_in, out, lw_out):
    out[...] = out_in[...]
    lw_out[...] = lw_in[...]


def body(hidden_in, pre_gain, query_proj, key_proj, value_proj, out_proj, post_gain):
    half = np.arange(HEAD_DIM // 2, dtype=np.float32) * np.float32(2.0) / np.float32(HEAD_DIM)
    freq = np.tile(np.power(np.float64(ROPE_BASE), -half.astype(np.float64)).astype(np.float32), 4).reshape(1, 128)
    hbm = pl.BlockSpec(memory_space=pltpu.HBM)
    vmem = pl.BlockSpec(memory_space=pltpu.VMEM)
    results = pl.pallas_call(
        kernel,
        out_shape=(jax.ShapeDtypeStruct((OUT_ROWS, D), BF16), jax.ShapeDtypeStruct((4, ROWS), F32)),
        in_specs=[hbm] * 8,
        out_specs=(vmem, vmem),
        scratch_shapes=[
            pltpu.VMEM((1, D), F32),
            pltpu.VMEM((1, 128), F32),
            pltpu.VMEM((1, D), F32),
            pltpu.VMEM((ROWS, D), BF16),
            pltpu.VMEM((ROWS, D), BF16),
            pltpu.VMEM((D, WIDTH), BF16),
            pltpu.VMEM((2, 2, NZ, NY, D // NSP, 128), BF16),
            pltpu.VMEM((NTP, WIDTH, D), BF16),
            pltpu.VMEM((SLOTS, 2, 2, ROWS, 128), BF16),
            pltpu.VMEM((2, 2, ROWS - AHEAD_ROWS, 128), BF16),
            pltpu.VMEM((2, 4, 256, 128), BF16),
            pltpu.VMEM((2, 4, 256, 128), F32),
            pltpu.VMEM((2, 4, 256, 128), F32),
            pltpu.VMEM((2, 4, 256, 128), F32),
            pltpu.VMEM((ROWS, 128), BF16),
            pltpu.VMEM((2, ROWS, 128), BF16),
            pltpu.VMEM((2, NTP, OUT_ROWS, 128), BF16),
            pltpu.VMEM((ROWS, 128), F32),
            pltpu.VMEM((ROWS, 128), F32),
            pltpu.VMEM((ROWS, 128), F32),
            pltpu.VMEM((128, SLOTS * 128), F32),
            pltpu.VMEM((2, 128, 256), F32),
            pltpu.VMEM((2, ROWS, ROWS), BF16),
            pltpu.VMEM((OUT_ROWS, D), F32),
            pltpu.SemaphoreType.DMA((10,)),
            pltpu.SemaphoreType.DMA((6,)),
            pltpu.SemaphoreType.DMA((R_END,)),
        ],
        compiler_params=pltpu.CompilerParams(
            collective_id=0, has_side_effects=True, vmem_limit_bytes=53 * 1024 * 1024
        ),
        name="layer",
    )(*(
        pltpu.with_memory_space_constraint(a, pltpu.HBM)
        for a in (
            hidden_in, pre_gain.reshape(1, D), jnp.asarray(freq), query_proj, key_proj, value_proj, out_proj,
            post_gain.reshape(1, D),
        )
    ))
    return pl.pallas_call(
        hand_over,
        out_shape=(jax.ShapeDtypeStruct((OUT_ROWS, D), BF16), jax.ShapeDtypeStruct((4, ROWS), F32)),
        in_specs=[vmem, vmem],
        out_specs=(vmem, vmem),
        compiler_params=pltpu.CompilerParams(vmem_limit_bytes=4 * 1024 * 1024),
        name="hand_over",
    )(*results)


def solution(mesh):
    placed = (P("sp", None), P(), P(None, "tp"), P("sp", "tp"), P("sp", "tp"), P("tp", None), P())
    return jax.shard_map(
        body,
        mesh=mesh,
        in_specs=placed,
        out_specs=(P(("sp", "tp"), None), P("tp", "sp")),
        check_vma=False,
    )
```
